256 devices in a mesh: st: 64 (over z, y, core), tp: 4 (over x).
Axes of the slice: x: 4, y: 4, z: 8, core: 2. Of those that a mesh axis runs over, the one named last changes fastest.
Arguments:
- tokens: bfloat16 [24576, 2048], P('st', 'tp'), may hold values from -6 to 6
- cotangent: bfloat16 [24576, 1024], P('st', 'tp'), may hold values from -48 to 48
- mix_query: bfloat16 [24576, 1024], P('st', 'tp'), may hold values from -6 to 6
- mix_key: bfloat16 [24576, 1024], P('st', 'tp'), may hold values from -6 to 6
- mix_value: bfloat16 [24576, 1024], P('st', 'tp'), may hold values from -24 to 24
- beta_pre: float32 [8, 24576], P('tp', 'st'), may hold values from -9 to 9
- decay_pre: float32 [8, 24576], P('tp', 'st'), may hold values from -8 to 6
- decay_rate: float32 [8], P('tp'), may hold values from 0.001 to 0.06
- passages: bfloat16 [1024, 64, 2048], P('st'), may hold values from -16 to 16
- passage_ids: int32 [384, 4], P('st'), may hold values from 0 to 1023, as said below
- query_weight: bfloat16 [2048, 1024], P(None, 'tp'), may hold values from -0.125 to 0.125
- key_weight: bfloat16 [2048, 1024], P(None, 'tp'), may hold values from -0.125 to 0.125
- value_weight: bfloat16 [2048, 1024], P(None, 'tp'), may hold values from -0.125 to 0.125
- gate_weight: bfloat16 [4, 2048], P('tp'), may hold values from -0.125 to 0.125
Outputs:
- token_grad: bfloat16 [24576, 2048], P('st', 'tp')
- passage_grad: bfloat16 [1024, 64, 2048], P('st', None, 'tp')
- key_weight_grad: float32 [2048, 1024], P('st', 'tp')
The draws below stay inside these ranges and needn't reach their ends.
Inputs may be any that keep to these rules, and one draw needn't show every extreme that they name: Passage p is stored on index p // 16 of st. The rows of passage_ids read by one index of st name at most 1 passages stored on any one index of st, and exactly 1 on some.
All inputs are finite; a program needn't handle non-finite values.
Results may differ from the reference program's by a relative error of at most 0.012.
The reference program's roundings to bfloat16 on the way count: a program that leaves them out, or rounds other values in their place, can miss the bound.
Values may be sent and summed in bfloat16 or wider, within the bound.
A program may use at most 128 MiB of HBM per device.

```python
import math
import jax
import jax.numpy as jnp
from jax import lax

D = 2048
HEADS = 4
HEAD = 256
MIX_HEADS = 8
MIX_DIM = 128
SPAN = 64
BLOCK = 64
PER_BLOCK = 4
PROWS = 64
TOK_DEV = 384
PASS_DEV = 16
TOKENS = 24576
BLOCKS = 384
REQ_DEV = 24
CAP = 1
PASSAGES = 1024
N_ST = 64


def draw_passage_ids(key, part):
    slot_count = N_ST * CAP
    shift_table = jax.random.randint(jax.random.fold_in(key, 9001), (N_ST,), 0, PASS_DEV)

    def per_reader(reader_idx):
        keys_split = jax.random.split(jax.random.fold_in(key, reader_idx), 4)
        rank_score = jax.random.permutation(keys_split[0], slot_count).astype(jnp.int32)
        slot_owner = jnp.arange(slot_count, dtype=jnp.int32) // CAP
        forced = (slot_owner == (reader_idx - 1) % N_ST) | (slot_owner == (reader_idx + N_ST // 2) % N_ST)
        rank_score = rank_score + forced.astype(jnp.int32) * (2 * slot_count)
        _, chosen = lax.top_k(rank_score, REQ_DEV)
        chosen = chosen.astype(jnp.int32)[jax.random.permutation(keys_split[1], REQ_DEV)]
        owner_ids = chosen // CAP
        first_draw = jax.random.randint(keys_split[2], (REQ_DEV,), 0, PASS_DEV)
        second_draw = jax.random.randint(keys_split[3], (REQ_DEV,), 0, PASS_DEV)
        local_ids = (jnp.minimum(first_draw, second_draw) + shift_table[owner_ids]) % PASS_DEV
        return (owner_ids * PASS_DEV + local_ids).astype(jnp.int32)
    every_id = jax.vmap(per_reader)(jnp.arange(N_ST, dtype=jnp.int32))
    return every_id.reshape(BLOCKS, PER_BLOCK)


def draw_decay_pre(key, part):
    keys_split = jax.random.split(key, 3)
    noise_part = 0.7 * jax.random.normal(keys_split[0], (MIX_HEADS, TOKENS), jnp.float32)
    slow_part = jax.random.uniform(keys_split[1], (MIX_HEADS, TOKENS // SPAN), jnp.float32, -1.2, 1.2)
    device_part = jax.random.uniform(keys_split[2], (MIX_HEADS, N_ST), jnp.float32, -1.0, 1.0)
    values_out = noise_part + jnp.repeat(slow_part, SPAN, axis=1) + jnp.repeat(device_part, TOK_DEV, axis=1)
    return jnp.clip(values_out, -8.0, 6.0)


def spiked(array, rng, source, target, parts, factor):
    owner, partner = [(jnp.arange(array.shape[dim]) // (array.shape[dim] // parts)).reshape([-1 if axis == dim else 1 for axis in range(array.ndim)]) for dim in (source, target)]
    chosen = jax.random.permutation(rng, parts)[partner]
    strong = (owner == chosen) | (owner == (partner + parts // 2) % parts)
    return jnp.where(strong, factor * array, array)


def level_of(key, extent, cuts, low, largest):
    def one(axis_at, blocks):
        draws = jax.random.uniform(jax.random.fold_in(jax.random.fold_in(key, 6), axis_at), (blocks,), jnp.float32, low / len(cuts), largest / len(cuts))
        return jnp.repeat(jnp.exp(draws), extent[axis_at] // blocks).reshape((-1,) + (1,) * (len(extent) - axis_at - 1))

    level = one(*cuts[0])
    for cut in cuts[1:]:
        level = level * one(*cut)
    return level


def scatter_about(rng, shape, scale, reach, pieces=(), kind=jnp.bfloat16):
    loudness = level_of(rng, shape, pieces, -0.22, 0.18) if pieces else 1.0
    values = jax.random.normal(rng, shape, jnp.float32) * scale * loudness
    return jnp.minimum(jnp.maximum(values, -reach), reach).astype(kind)


def noise_with(rng, extent, deviation, most, cuts, heavy, kind=jnp.bfloat16):
    entries = deviation * jax.random.normal(rng, extent, jnp.float32)
    if cuts:
        entries = entries * level_of(rng, extent, cuts, -0.22, 0.18)
    return jnp.clip(spiked(entries, jax.random.fold_in(rng, 3), *heavy), -most, most).astype(kind)


def setup_inputs(seed: int = 0) -> dict:
    streams_of = jax.random.split(jax.random.key(seed), 15)
    tokens = scatter_about(streams_of[0], (TOKENS, D), 1.0, 6.0, ((0, 64), (1, 4)))
    cotangent = scatter_about(streams_of[1], (TOKENS, HEADS * HEAD), 8.0, 48.0, ((0, 64), (1, 4)))
    mix_query = scatter_about(streams_of[2], (TOKENS, MIX_HEADS * MIX_DIM), 1.0, 6.0, ((0, 64), (1, 4)))
    mix_key = scatter_about(streams_of[3], (TOKENS, MIX_HEADS * MIX_DIM), 1.0, 6.0, ((0, 64), (1, 4)))
    mix_value = scatter_about(streams_of[4], (TOKENS, MIX_HEADS * MIX_DIM), 4.0, 24.0, ((0, 64), (1, 4)))
    beta_pre = scatter_about(streams_of[5], (MIX_HEADS, TOKENS), 1.5, 9.0, ((0, 4), (1, 64)), jnp.float32)
    decay_pre = draw_decay_pre(jax.random.fold_in(streams_of[14], 71), 0)
    decay_rate = jnp.clip(jnp.exp(math.log(0.06) - 4.0943445 * jax.random.uniform(streams_of[7], (MIX_HEADS,), jnp.float32) ** level_of(streams_of[7], (MIX_HEADS,), ((0, 4),), -0.2, 0.2)), 0.001, 0.06)
    passages = noise_with(streams_of[8], (PASSAGES, PROWS, D), 1.0, 16.0, ((0, 64),), (0, 2, 64, 4.0))
    passage_ids = draw_passage_ids(jax.random.fold_in(streams_of[14], 71), 0)
    query_weight = scatter_about(streams_of[10], (D, HEADS * HEAD), D ** -0.5, 0.125, ((1, 4),))
    key_weight = scatter_about(streams_of[11], (D, HEADS * HEAD), D ** -0.5, 0.125, ((1, 4),))
    value_weight = scatter_about(streams_of[12], (D, HEADS * HEAD), D ** -0.5, 0.125, ((1, 4),))
    gate_weight = scatter_about(streams_of[13], (HEADS, D), D ** -0.5, 0.125, ((0, 4),))
    return dict(tokens=tokens, cotangent=cotangent, mix_query=mix_query, mix_key=mix_key, mix_value=mix_value, beta_pre=beta_pre, decay_pre=decay_pre, decay_rate=decay_rate, passages=passages, passage_ids=passage_ids, query_weight=query_weight, key_weight=key_weight, value_weight=value_weight, gate_weight=gate_weight)


NORM_FLOOR = 1.0
SCORE_GAIN = 4.0
HIGHEST = lax.Precision.HIGHEST

def to_low(value):
    return lax.optimization_barrier(value.astype(jnp.bfloat16))

def neumann_inverse(strict_part):
    span_size = strict_part.shape[-1]
    unit_eye = jnp.eye(span_size, dtype=jnp.float32)
    running = unit_eye - strict_part
    power_term = strict_part
    for _ in range(span_size.bit_length() - 2):
        power_term = jnp.einsum('...ij,...jk->...ik', power_term, power_term, precision=HIGHEST)
        running = jnp.einsum('...ij,...jk->...ik', running, unit_eye + power_term, precision=HIGHEST)
    return running

def delta_mixer(queries, keys_in, values_in, strength, log_decay):
    heads_n, length, key_dim = queries.shape
    blocks_n = length // SPAN

    def to_blocks(tensor):
        return tensor.reshape(heads_n, blocks_n, SPAN, *tensor.shape[2:])
    queries, keys_in, values_in = (to_blocks(queries), to_blocks(keys_in), to_blocks(values_in))
    strength, log_decay = (to_blocks(strength), to_blocks(log_decay))
    cumulative = jnp.cumsum(log_decay, axis=-1)
    position = jnp.arange(SPAN)
    inclusive = position[:, None] >= position[None, :]
    strictly = position[:, None] > position[None, :]
    spread = jnp.where(inclusive, cumulative[..., :, None] - cumulative[..., None, :], -jnp.inf)
    decay_map = jnp.exp(spread)
    key_gram = jnp.einsum('hncd,hnmd->hncm', keys_in, keys_in, precision=HIGHEST)
    strict_part = jnp.where(strictly, strength[..., :, None] * key_gram * decay_map, 0.0)
    inverse = neumann_inverse(strict_part)
    fresh_vals = jnp.einsum('hncm,hnme->hnce', inverse, values_in * strength[..., None], precision=HIGHEST)
    correction = jnp.einsum('hncm,hnmd->hncd', inverse, keys_in * (strength * jnp.exp(cumulative))[..., None], precision=HIGHEST)
    attend_map = jnp.where(inclusive, jnp.einsum('hncd,hnmd->hncm', queries, keys_in, precision=HIGHEST) * decay_map, 0.0)
    query_dec = queries * jnp.exp(cumulative)[..., None]
    key_dec = keys_in * jnp.exp(cumulative[..., -1:] - cumulative)[..., None]
    carry_decay = jnp.exp(cumulative[..., -1])

    def advance(memory_state, inputs):
        fresh_blk, correct_blk, attend_blk, query_blk, key_blk, decay_blk = inputs
        new_values = fresh_blk - jnp.einsum('hcd,hde->hce', correct_blk, memory_state, precision=HIGHEST)
        output = jnp.einsum('hcd,hde->hce', query_blk, memory_state, precision=HIGHEST) + jnp.einsum('hcm,hme->hce', attend_blk, new_values, precision=HIGHEST)
        memory_state = memory_state * decay_blk[:, None, None] + jnp.einsum('hcd,hce->hde', key_blk, new_values, precision=HIGHEST)
        return (memory_state, output)
    stacked = tuple((jnp.moveaxis(tensor, 1, 0) for tensor in (fresh_vals, correction, attend_map, query_dec, key_dec, carry_decay)))
    initial = jnp.zeros((heads_n, key_dim, values_in.shape[-1]), jnp.float32)
    _, outputs = lax.scan(advance, initial, stacked)
    return jnp.transpose(outputs, (1, 0, 2, 3)).reshape(heads_n, length, -1)

def mixer_output(query_raw, key_raw, value_raw, beta_raw, decay_raw, rate_vals):
    length = query_raw.shape[0]
    heads_n = beta_raw.shape[0]

    def heads_first(matrix):
        return jnp.transpose(matrix.astype(jnp.float32).reshape(length, heads_n, -1), (1, 0, 2))
    queries = heads_first(query_raw)
    keys_in = heads_first(key_raw)
    values_in = heads_first(value_raw)
    queries = queries * lax.rsqrt(lax.optimization_barrier(jnp.sum(queries * queries, axis=-1, keepdims=True)) + NORM_FLOOR) * queries.shape[-1] ** (-0.5)
    keys_in = keys_in * lax.rsqrt(lax.optimization_barrier(jnp.sum(keys_in * keys_in, axis=-1, keepdims=True)) + NORM_FLOOR)
    strength = jax.nn.sigmoid(beta_raw)
    log_decay = -rate_vals[:, None] * jax.nn.softplus(decay_raw)
    mixer_out = delta_mixer(queries, keys_in, values_in, strength, log_decay)
    return jnp.transpose(mixer_out, (1, 0, 2)).reshape(length, -1)

def request_slots(id_rows, pass_count):
    owners = id_rows // pass_count
    local_idx = id_rows % pass_count
    req_count = id_rows.shape[-1]
    req_order = jnp.arange(req_count, dtype=jnp.int32)
    earlier = (owners[..., :, None] == owners[..., None, :]) & (req_order[None, :] < req_order[:, None])
    ranks = lax.optimization_barrier(jnp.sum(earlier.astype(jnp.int32), axis=-1, dtype=jnp.int32))
    return (owners, local_idx, ranks)

def reference(tokens, cotangent, mix_query, mix_key, mix_value, beta_pre, decay_pre, decay_rate, passages, passage_ids, query_weight, key_weight, value_weight, gate_weight):
    score_scale = SCORE_GAIN * HEAD ** (-0.5)
    every_id = passage_ids.reshape(N_ST, REQ_DEV)
    query_heads = query_weight.astype(jnp.float32).reshape(D, HEADS, HEAD)
    key_heads = key_weight.astype(jnp.float32).reshape(D, HEADS, HEAD)
    value_heads = value_weight.astype(jnp.float32).reshape(D, HEADS, HEAD)
    gate_float = gate_weight.astype(jnp.float32)
    blocks_n = TOK_DEV // BLOCK

    def reader(reader_idx):
        first_row = reader_idx * TOK_DEV
        tok_block = lax.dynamic_slice_in_dim(tokens, first_row, TOK_DEV, 0)
        query_low = to_low(jnp.dot(tok_block, query_weight, preferred_element_type=jnp.float32))
        query_float = query_low.astype(jnp.float32).reshape(TOK_DEV, HEADS, HEAD)
        query_scale = lax.rsqrt(lax.optimization_barrier(jnp.mean(query_float * query_float, axis=-1, keepdims=True)) + NORM_FLOOR)
        query_hat = to_low(query_float * query_scale)
        gate_open = jax.nn.sigmoid(jnp.dot(tok_block, gate_weight.T, preferred_element_type=jnp.float32))
        row_block = passages[every_id[reader_idx]].reshape(REQ_DEV * PROWS, D)
        key_low = to_low(jnp.dot(row_block, key_weight, preferred_element_type=jnp.float32))
        key_float = key_low.astype(jnp.float32).reshape(REQ_DEV * PROWS, HEADS, HEAD)
        key_scale = lax.rsqrt(lax.optimization_barrier(jnp.mean(key_float * key_float, axis=-1, keepdims=True)) + NORM_FLOOR)
        key_hat = to_low(key_float * key_scale)
        value_low = to_low(jnp.dot(row_block, value_weight, preferred_element_type=jnp.float32))
        key_blocks = key_hat.astype(jnp.float32).reshape(blocks_n, PER_BLOCK * PROWS, HEADS, HEAD)
        value_blocks = value_low.astype(jnp.float32).reshape(blocks_n, PER_BLOCK * PROWS, HEADS, HEAD)
        query_blocks = query_hat.astype(jnp.float32).reshape(blocks_n, BLOCK, HEADS, HEAD)
        scores = jnp.einsum('bihd,bjhd->bhij', query_blocks, key_blocks) * score_scale
        exp_scores = jnp.exp(scores)
        attn_probs = exp_scores / lax.optimization_barrier(jnp.sum(exp_scores, axis=-1, keepdims=True))
        probs_low = to_low(attn_probs).astype(jnp.float32)
        retrieved = jnp.einsum('bhij,bjhd->bihd', probs_low, value_blocks).reshape(TOK_DEV, HEADS, HEAD)
        mixer_out = mixer_output(lax.dynamic_slice_in_dim(mix_query, first_row, TOK_DEV, 0), lax.dynamic_slice_in_dim(mix_key, first_row, TOK_DEV, 0), lax.dynamic_slice_in_dim(mix_value, first_row, TOK_DEV, 0), lax.dynamic_slice_in_dim(beta_pre, first_row, TOK_DEV, 1), lax.dynamic_slice_in_dim(decay_pre, first_row, TOK_DEV, 1), decay_rate).reshape(TOK_DEV, HEADS, HEAD)
        grad_out = lax.dynamic_slice_in_dim(cotangent, first_row, TOK_DEV, 0).astype(jnp.float32).reshape(TOK_DEV, HEADS, HEAD)
        grad_ret = to_low(gate_open[..., None] * grad_out).astype(jnp.float32)
        gate_grad = lax.optimization_barrier(jnp.sum(grad_out * (retrieved - mixer_out), axis=-1)) * gate_open * (1.0 - gate_open)
        grad_blocks = grad_ret.reshape(blocks_n, BLOCK, HEADS, HEAD)
        grad_probs = jnp.einsum('bihd,bjhd->bhij', grad_blocks, value_blocks)
        score_grad = to_low(attn_probs * (grad_probs - lax.optimization_barrier(jnp.sum(grad_probs * attn_probs, axis=-1, keepdims=True)))).astype(jnp.float32)
        qhat_grad = score_scale * jnp.einsum('bhij,bjhd->bihd', score_grad, key_blocks).reshape(TOK_DEV, HEADS, HEAD)
        khat_grad = to_low(score_scale * jnp.einsum('bhij,bihd->bjhd', score_grad, query_blocks)).astype(jnp.float32).reshape(REQ_DEV, PROWS, HEADS, HEAD)
        value_grad = to_low(jnp.einsum('bhij,bihd->bjhd', probs_low, grad_blocks)).astype(jnp.float32).reshape(REQ_DEV, PROWS, HEADS, HEAD)
        query_grad = to_low(query_scale * qhat_grad - query_scale ** 3 * query_float * lax.optimization_barrier(jnp.mean(query_float * qhat_grad, axis=-1, keepdims=True))).astype(jnp.float32)
        partial_value = jnp.einsum('thd,ehd->the', query_grad, query_heads) + gate_grad[..., None] * gate_float[None]
        token_rows = lax.optimization_barrier(jnp.sum(to_low(partial_value).astype(jnp.float32), axis=1)).astype(jnp.bfloat16)
        return (token_rows, khat_grad, value_grad)
    token_rows, khat_all, value_all = lax.map(reader, jnp.arange(N_ST, dtype=jnp.int32))
    owner_all, local_all, rank_all = request_slots(every_id, PASS_DEV)
    cap_iota = jnp.arange(CAP, dtype=jnp.int32)
    req_iota = jnp.arange(REQ_DEV, dtype=jnp.int32)
    readers = jnp.arange(N_ST, dtype=jnp.int32)[:, None]
    pass_iota = jnp.arange(PASS_DEV, dtype=jnp.int32)

    def owner_step(weight_acc, owner_idx):
        wanted = (owner_all == owner_idx)[:, None, :] & (rank_all[:, None, :] == cap_iota[None, :, None])
        slot_used = jnp.any(wanted, axis=-1)
        slot_local = lax.optimization_barrier(jnp.sum(jnp.where(wanted, local_all[:, None, :], 0), axis=-1, dtype=jnp.int32))
        req_pick = lax.optimization_barrier(jnp.sum(jnp.where(wanted, req_iota[None, None, :], 0), axis=-1, dtype=jnp.int32))
        khat_slots = jnp.where(slot_used[:, :, None, None, None], khat_all[readers, req_pick], 0.0)
        value_slots = jnp.where(slot_used[:, :, None, None, None], value_all[readers, req_pick], 0.0)
        onehot = ((slot_local.reshape(-1)[None, :] == pass_iota[:, None]) & slot_used.reshape(-1)[None, :]).astype(jnp.float32)
        khat_pass = jnp.dot(onehot, khat_slots.reshape(N_ST * CAP, -1), precision=HIGHEST).reshape(PASS_DEV * PROWS, HEADS, HEAD)
        value_pass = jnp.dot(onehot, value_slots.reshape(N_ST * CAP, -1), precision=HIGHEST).reshape(PASS_DEV * PROWS, HEADS, HEAD)
        row_block = lax.dynamic_slice_in_dim(passages, owner_idx * PASS_DEV, PASS_DEV, 0).reshape(PASS_DEV * PROWS, D)
        key_low = to_low(jnp.dot(row_block, key_weight, preferred_element_type=jnp.float32))
        key_float = key_low.astype(jnp.float32).reshape(PASS_DEV * PROWS, HEADS, HEAD)
        key_scale = lax.rsqrt(lax.optimization_barrier(jnp.mean(key_float * key_float, axis=-1, keepdims=True)) + NORM_FLOOR)
        key_grad = to_low(key_scale * khat_pass - key_scale ** 3 * key_float * lax.optimization_barrier(jnp.mean(key_float * khat_pass, axis=-1, keepdims=True)))
        value_grad_low = to_low(value_pass)
        partial_value = jnp.einsum('rhd,ehd->rhe', key_grad.astype(jnp.float32), key_heads) + jnp.einsum('rhd,ehd->rhe', value_grad_low.astype(jnp.float32), value_heads)
        rows_grad = lax.optimization_barrier(jnp.sum(to_low(partial_value).astype(jnp.float32), axis=1)).astype(jnp.bfloat16).reshape(PASS_DEV, PROWS, D)
        weight_acc = weight_acc + jnp.dot(row_block.T, key_grad.reshape(PASS_DEV * PROWS, HEADS * HEAD), preferred_element_type=jnp.float32)
        return (weight_acc, rows_grad)
    weight_grad, store_grad = lax.scan(owner_step, jnp.zeros((D, HEADS * HEAD), jnp.float32), jnp.arange(N_ST, dtype=jnp.int32))
    return (token_rows.reshape(TOKENS, D), store_grad.reshape(PASSAGES, PROWS, D), weight_grad)
```

```python
import functools

import jax
import jax.numpy as jnp
from jax import lax
from jax.experimental import pallas as pl
from jax.experimental.pallas import tpu as pltpu
from jax.sharding import Mesh
from jax.sharding import PartitionSpec as P

SPAN = 64
ST = ("st_0", "st_1", "st_2")
MESH = pl.DeviceIdType.MESH
NZ, NY, NX = 8, 4, 4
VMEM = pltpu.VMEM
F32, BF16 = jnp.float32, jnp.bfloat16

NORM_FLOOR = 1.0
SCORE_GAIN = 4.0
CONTRACT_LAST = (((1,), (1,)), ((), ()))
CONTRACT_FIRST = (((0,), (0,)), ((), ()))


def place():
    return (lax.axis_index("st_0"), lax.axis_index("st_1"), lax.axis_index("st_2"), lax.axis_index("tp"))


def wrap(value, size):
    return lax.rem(value + size, size)


class Copies:
    def __init__(self):
        self.started = []

    def make(self, src, dst, send, recv, where):
        return pltpu.make_async_remote_copy(
            src_ref=src, dst_ref=dst, send_sem=send, recv_sem=recv, device_id=where, device_id_type=MESH
        )

    def start(self, src, dst, send, recv, where):
        copy = self.make(src, dst, send, recv, where)
        copy.start()
        self.started.append(copy)

    def arrived(self, dst, send, recv, where):
        self.make(dst, dst, send, recv, where).wait_recv()

    def finish(self):
        for copy in self.started:
            copy.wait_send()


def greet(peers):
    barrier = pltpu.get_barrier_semaphore()
    for peer in peers:
        pl.semaphore_signal(barrier, inc=1, device_id=peer, device_id_type=MESH)
    pl.semaphore_wait(barrier, len(peers))


def column_peers(z, c):
    me = z * 2 + c
    peers = []
    for step in range(1, 2 * NZ):
        other = wrap(me + step, 2 * NZ)
        peers.append({"st_0": other // 2, "st_2": lax.rem(other, 2)})
    return peers


def gather_kernel(
    pas, wk, wv, tok, wq, gw, cot, tbl,
    kv, qa, ca, tl, klow, qlow, grow,
    toks, xs, xr, ys, yr, zs, zr, ps, pr, ts, tr,
):
    z, y, c, x = place()
    me = z * 2 + c
    up, down = {"st_0": wrap(z + 1, NZ)}, {"st_0": wrap(z - 1, NZ)}
    east, west = {"st_1": wrap(y + 1, NY)}, {"st_1": wrap(y - 1, NY)}
    front, back = {"tp": wrap(x + 1, NX)}, {"tp": wrap(x - 1, NX)}
    partner = {"st_2": 1 - c}
    peers = column_peers(z, c)
    greet(peers + [east, west, front, back])
    copies = Copies()
    half = 192
    zdirs, ydirs, xdirs = (up, down), (east, west), (front, back)

    def rows_of(ref, slot, h):
        return ref.at[slot, pl.ds(h * half, half), :]

    def z_send(k, ref, d, h):
        for way in (0, 1):
            if d == 4 and h != way:
                continue
            owner = wrap(z - (d - 1), NZ) if way == 0 else wrap(z + (d - 1), NZ)
            piece = rows_of(ref, owner * 2 + c, h)
            at = (d - 1) * 2 + h if d < 4 else 6
            copies.start(piece, piece, zs.at[k, way, at], zr.at[k, way, at], zdirs[way])

    def z_take(k, ref, d):
        for h in (0, 1):
            for way in (0, 1):
                if d == 4 and h != way:
                    continue
                owner = wrap(z - d, NZ) if way == 0 else wrap(z + d, NZ)
                piece = rows_of(ref, owner * 2 + c, h)
                at = (d - 1) * 2 + h if d < 4 else 6
                copies.arrived(piece, zs.at[k, way, at], zr.at[k, way, at], zdirs[way])
                if d < 3 or (d == 3 and h == way):
                    nxt = d * 2 + h if d < 3 else 6
                    copies.start(piece, piece, zs.at[k, way, nxt], zr.at[k, way, nxt], zdirs[way])
                to = 2 + way * 7 + at
                copies.start(piece, piece, ps.at[k, to], pr.at[k, to], partner)

    def own_send(k, ref):
        for h in (0, 1):
            z_send(k, ref, 1, h)
        for h in (0, 1):
            piece = rows_of(ref, me, h)
            copies.start(piece, piece, ps.at[k, h], pr.at[k, h], partner)

    def partner_take(k, ref):
        theirs = 1 - c
        for h in (0, 1):
            piece = rows_of(ref, z * 2 + theirs, h)
            copies.arrived(piece, ps.at[k, h], pr.at[k, h], partner)
        for d in (1, 2, 3, 4):
            for h in (0, 1):
                for way in (0, 1):
                    if d == 4 and h != way:
                        continue
                    owner = wrap(z - d, NZ) if way == 0 else wrap(z + d, NZ)
                    to = 2 + way * 7 + ((d - 1) * 2 + h if d < 4 else 6)
                    piece = rows_of(ref, owner * 2 + theirs, h)
                    copies.arrived(piece, ps.at[k, to], pr.at[k, to], partner)

    toks[x] = tok[...]
    for way in (0, 1):
        for h in (0, 1):
            piece = rows_of(toks, x, h)
            copies.start(piece, piece, xs.at[way, h], xr.at[way, h], xdirs[way])
    ca[me] = cot[...]
    own_send(0, ca)

    rows = 256

    def kv_rows(i):
        return kv.at[y, pl.ds(i * rows, rows), :]

    for i in range(4):
        block = pas[pl.ds(i * rows, rows), :]
        low = jnp.dot(block, wk[...], preferred_element_type=F32).astype(BF16)
        wide = low.astype(F32)
        scale = lax.rsqrt(jnp.mean(wide * wide, axis=-1, keepdims=True) + NORM_FLOOR)
        klow[pl.ds(i * rows, rows), :] = low
        kv[y, pl.ds(i * rows, rows), pl.ds(0, 256)] = (wide * scale).astype(BF16)
        kv[y, pl.ds(i * rows, rows), pl.ds(256, 256)] = jnp.dot(
            block, wv[...], preferred_element_type=F32
        ).astype(BF16)
        for way in (0, 1):
            copies.start(kv_rows(i), kv_rows(i), ys.at[way, i], yr.at[way, i], ydirs[way])

    def y_take(i):
        for way in (0, 1):
            owner = wrap(y - 1, NY) if way == 0 else wrap(y + 1, NY)
            piece = kv.at[owner, pl.ds(i * rows, rows), :]
            copies.arrived(piece, ys.at[way, i], yr.at[way, i], ydirs[way])
            if i % 2 == way:
                at = 4 + i // 2
                copies.start(piece, piece, ys.at[way, at], yr.at[way, at], ydirs[way])

    def y_last():
        owner = wrap(y + 2, NY)
        for i in range(4):
            way, at = i % 2, 4 + i // 2
            piece = kv.at[owner, pl.ds(i * rows, rows), :]
            copies.arrived(piece, ys.at[way, at], yr.at[way, at], ydirs[way])

    def x_take():
        for way in (0, 1):
            owner = wrap(x - 1, NX) if way == 0 else wrap(x + 1, NX)
            for h in (0, 1):
                piece = rows_of(toks, owner, h)
                copies.arrived(piece, xs.at[way, h], xr.at[way, h], xdirs[way])
                if h == way:
                    copies.start(piece, piece, xs.at[way, 2], xr.at[way, 2], xdirs[way])

    def x_last():
        owner = wrap(x + 2, NX)
        for way in (0, 1):
            piece = rows_of(toks, owner, way)
            copies.arrived(piece, xs.at[way, 2], xr.at[way, 2], xdirs[way])

    def project(owner):
        block = toks[owner]
        at = pl.ds(pl.multiple_of(owner * 512, 512), 512)
        return (
            jnp.dot(block, wq[at, :], preferred_element_type=F32),
            lax.dot_general(gw[:, at], block, CONTRACT_LAST, preferred_element_type=F32),
        )

    z_take(0, ca, 1)
    y_take(0)
    acc = project(x)
    x_take()
    z_take(0, ca, 2)
    for owner in (wrap(x - 1, NX), wrap(x + 1, NX)):
        more = project(owner)
        acc = (acc[0] + more[0], acc[1] + more[1])
    y_take(1)
    x_last()
    more = project(wrap(x + 2, NX))
    low = (acc[0] + more[0]).astype(BF16)
    gate = jax.nn.sigmoid(acc[1] + more[1])
    wide = low.astype(F32)
    scale = lax.rsqrt(jnp.mean(wide * wide, axis=-1, keepdims=True) + NORM_FLOOR)
    qlow[...] = low
    qa[me] = (wide * scale).astype(BF16)
    own_send(1, qa)
    z_take(0, ca, 3)
    grow[...] = gate[0:8]
    tl[me] = jnp.zeros((8, 128), F32)
    for b in range(6):
        tl[me, b : b + 1, 0:64] = gate[0:1, b * 64 : b * 64 + 64]
    tl[me, 6:7, 0:64] = tbl[...]
    for step, peer in enumerate(peers):
        copies.start(tl.at[me], tl.at[me], ts.at[step], tr.at[step], peer)
    y_take(2)
    z_take(1, qa, 1)
    y_take(3)
    z_take(1, qa, 2)
    z_take(0, ca, 4)
    z_take(1, qa, 3)
    z_take(1, qa, 4)
    for step in range(2 * NZ - 1):
        other = wrap(me - (step + 1), 2 * NZ)
        copies.arrived(tl.at[other], ts.at[step], tr.at[step], peers[step])
    partner_take(0, ca)
    partner_take(1, qa)
    y_last()
    copies.finish()


def score_kernel(tb, kv, qa, ca, tl, eg, tot, own, sent, parts, total, ss, sr, bs, br):
    z, y, c, x = place()
    me = z * 2 + c
    peers = column_peers(z, c)
    greet(peers)
    copies = Copies()
    gain = SCORE_GAIN * 256 ** (-0.5)
    line = lax.broadcasted_iota(jnp.int32, (8, 128), 0)

    def reader(r, carry):
        tile = tl[r]
        stats = jnp.zeros((8, 128), F32)
        for yy in range(NY):
            entry = tb[r, (z * NY + yy) * 2 + c]
            used = entry >= 0
            safe = jnp.maximum(entry, 0)
            b, loc = safe // 64, lax.rem(safe, 16)
            keys_values = kv[yy * 16 + loc]
            scores = gain * lax.dot_general(
                keys_values[:, 0:256], qa[r * 6 + b], CONTRACT_LAST, preferred_element_type=F32
            )
            here = (line == b) & used
            gate = jnp.sum(jnp.where(line == b, tile, 0.0), axis=0, keepdims=True)
            grads = gate[:, 0:64] * lax.dot_general(
                keys_values[:, 256:512], ca[r * 6 + b], CONTRACT_LAST, preferred_element_type=F32
            )
            exps = jnp.exp(scores)
            both = jnp.concatenate([exps, grads], axis=1)
            eg[r * NY + yy] = both
            row = jnp.concatenate(
                [jnp.sum(exps, axis=0, keepdims=True), jnp.sum(exps * grads, axis=0, keepdims=True)], axis=1
            )
            stats = stats + jnp.where(here, row, 0.0)
        sent[r] = stats
        return carry

    lax.fori_loop(0, 2 * NZ, reader, 0)
    for step, peer in enumerate(peers):
        other = wrap(me + step + 1, 2 * NZ)
        copies.start(sent.at[other], parts.at[step], ss.at[step], sr.at[step], peer)
    whole = sent[me]
    for step in range(2 * NZ - 1):
        copies.arrived(parts.at[step], ss.at[step], sr.at[step], peers[step])
        whole = whole + parts[step]
    total[...] = whole
    tot[me] = whole
    own[...] = whole
    for step, peer in enumerate(peers):
        copies.start(total, tot.at[me], bs.at[step], br.at[step], peer)
    for step in range(2 * NZ - 1):
        other = wrap(me - (step + 1), 2 * NZ)
        copies.arrived(tot.at[other], bs.at[step], br.at[step], peers[step])
    copies.finish()


def grads_kernel(tb, kv, qa, ca, tl, eg, tot, kvg, qp, kacc, qacc):
    z, c = lax.axis_index("st_0"), lax.axis_index("st_2")
    gain = SCORE_GAIN * 256 ** (-0.5)
    kacc[...] = jnp.zeros(kacc.shape, F32)
    qacc[...] = jnp.zeros(qacc.shape, F32)

    @pl.loop(0, 2 * NZ)
    def _(r):
        for yy in range(NY):
            entry = tb[r, (z * NY + yy) * 2 + c]

            @pl.when(entry >= 0)
            def _():
                b, loc = entry // 64, lax.rem(entry, 16)
                row = tot[r, pl.ds(b, 1), :]
                gate = tl[r, pl.ds(b, 1), 0:64]
                norm = 1.0 / row[:, 0:64]
                both = eg[r * NY + yy]
                probs = both[:, 0:64] * norm
                slope = (probs * (both[:, 64:128] - row[:, 64:128] * norm)).astype(BF16)
                gated = (probs * gate).astype(BF16)
                at, slot = r * 6 + b, yy * 16 + loc
                key = gain * jnp.dot(slope, qa[at], preferred_element_type=F32)
                value = jnp.dot(gated, ca[at], preferred_element_type=F32)
                kacc[slot, :, 0:256] += key.astype(BF16).astype(F32)
                kacc[slot, :, 256:512] += value.astype(BF16).astype(F32)
                qacc[at] += gain * lax.dot_general(
                    slope, kv[slot, :, 0:256], CONTRACT_FIRST, preferred_element_type=F32
                )

    @pl.loop(0, 64)
    def _(i):
        kvg[i] = kacc[i].astype(BF16)

    @pl.loop(0, 96)
    def _(i):
        qp[i] = qacc[i].astype(BF16)


def return_kernel(kvg, qp, kvs, qg, ybuf, ysum, px, qs, zbuf, ys, yr, zs, zr, ps, pr):
    z, y, c, x = place()
    up, down = {"st_0": wrap(z + 1, NZ)}, {"st_0": wrap(z - 1, NZ)}
    east, west = {"st_1": wrap(y + 1, NY)}, {"st_1": wrap(y - 1, NY)}
    partner = {"st_2": 1 - c}
    greet([up, down, east, west, partner])
    copies = Copies()
    zdirs, ydirs = (up, down), (east, west)
    half = 192
    order = [4, 3, 5, 2, 6, 1, 7, 0]
    for k in order:
        there = wrap(z + k, NZ)
        copies.start(qp.at[there * 2 + 1 - c], px.at[there], ps.at[k], pr.at[k], partner)
    part, sub = 512, 256
    far, beside = wrap(y + 2, NY), (wrap(y + 1, NY), wrap(y - 1, NY))
    for j in (0, 1):
        for way in (0, 1):
            at = pl.ds(way * part + j * sub, sub)
            copies.start(kvg.at[far, at, :], ybuf.at[way, pl.ds(j * sub, sub), :], ys.at[way, j], yr.at[way, j], ydirs[way])
    for way in (0, 1):
        at = pl.ds((1 - way) * part, part)
        copies.start(kvg.at[beside[way], at, :], ysum.at[way, at, :], ys.at[way, 4], yr.at[way, 4], ydirs[way])

    def q_pair(k):
        there = wrap(z + k, NZ)
        copies.arrived(px.at[there], ps.at[k], pr.at[k], partner)
        qs[there] = (qp[there * 2 + c].astype(F32) + px[there].astype(F32)).astype(BF16)

    def y_add(j):
        for way in (0, 1):
            copies.arrived(ybuf.at[way, pl.ds(j * sub, sub), :], ys.at[way, j], yr.at[way, j], ydirs[way])
            at = pl.ds(way * part + j * sub, sub)
            mine = kvg[beside[way], at, :].astype(F32)
            ybuf[way, pl.ds(j * sub, sub), :] = (
                mine + ybuf[way, pl.ds(j * sub, sub), :].astype(F32)
            ).astype(BF16)
            copies.start(
                ybuf.at[way, pl.ds(j * sub, sub), :], ysum.at[way, at, :], ys.at[way, 2 + j], yr.at[way, 2 + j], ydirs[way]
            )

    def z_step(d):
        for way in (0, 1):
            there = wrap(z + d, NZ) if way == 0 else wrap(z - d, NZ)
            if d == 3:
                piece = zbuf.at[way, 0, pl.ds(way * half, half), :]
                copies.arrived(piece, zs.at[way, 3], zr.at[way, 3], zdirs[way])
                at = pl.ds(way * half, half)
                qs[there, at, :] = (
                    qs[there, at, :].astype(F32) + zbuf[way, 0, at, :].astype(F32)
                ).astype(BF16)
            elif d < 3:
                piece = zbuf.at[way, 3 - d]
                copies.arrived(piece, zs.at[way, d], zr.at[way, d], zdirs[way])
                qs[there] = (qs[there].astype(F32) + zbuf[way, 3 - d].astype(F32)).astype(BF16)
            if d == 4:
                at = pl.ds(way * half, half)
                copies.start(qs.at[there, at, :], zbuf.at[way, 0, at, :], zs.at[way, 3], zr.at[way, 3], zdirs[way])
            else:
                copies.start(qs.at[there], zbuf.at[way, 4 - d], zs.at[way, d - 1], zr.at[way, d - 1], zdirs[way])

    q_pair(4)
    z_step(4)
    q_pair(3)
    q_pair(5)
    q_pair(2)
    q_pair(6)
    z_step(3)
    q_pair(1)
    q_pair(7)
    q_pair(0)
    y_add(0)
    z_step(2)
    y_add(1)
    z_step(1)
    grad = qs[z].astype(F32)
    for way in (0, 1):
        copies.arrived(zbuf.at[way, 3], zs.at[way, 0], zr.at[way, 0], zdirs[way])
        grad = grad + zbuf[way, 3].astype(F32)
    qg[...] = grad
    for way in (0, 1):
        at = pl.ds((1 - way) * part, part)
        copies.arrived(ysum.at[way, at, :], ys.at[way, 4], yr.at[way, 4], ydirs[way])
    for way in (0, 1):
        for j in (0, 1):
            at = pl.ds(way * part + j * sub, sub)
            copies.arrived(ysum.at[way, at, :], ys.at[way, 2 + j], yr.at[way, 2 + j], ydirs[way])
    for i in range(4):
        at = pl.ds(i * 256, 256)
        kvs[at, :] = kvg[y, at, :].astype(F32) + ysum[0, at, :].astype(F32) + ysum[1, at, :].astype(F32)
    copies.finish()


def shaped(shape, dtype):
    return jax.ShapeDtypeStruct(shape, dtype)


def dma(*shape):
    return pltpu.SemaphoreType.DMA(shape)


def call(kernel, outs, scratch, collective, smem=0, limit=48, count=0, **extra):
    in_specs = [pl.BlockSpec(memory_space=pltpu.SMEM)] * smem + [pl.BlockSpec(memory_space=VMEM)] * (count - smem)
    params = dict(vmem_limit_bytes=limit * 2**20)
    if collective is not None:
        params.update(collective_id=collective, has_side_effects=True)
    return pl.pallas_call(
        kernel,
        out_shape=outs,
        in_specs=in_specs,
        out_specs=[pl.BlockSpec(memory_space=VMEM)] * len(outs),
        scratch_shapes=scratch,
        compiler_params=pltpu.CompilerParams(**params),
        **extra,
    )


def in_blocks(shard, dim, devices):
    before, after = (shard.shape[:dim], shard.shape[dim + 1 :])
    return jnp.moveaxis(shard.reshape(*before, devices, -1, *after), dim, 0)


def sum_at_owner(shard, axis, dim):
    parts = in_blocks(shard, dim, lax.axis_size(axis))
    arrived = lax.all_to_all(parts, axis, split_axis=0, concat_axis=0, tiled=True)
    return arrived.astype(jnp.float32).sum(axis=0)


def sum_by_axis(shard, axes, dim):
    for axis in axes:
        shard = lax.psum_scatter(shard, axis, scatter_dimension=dim, tiled=True)
    return shard


def neumann_inverse(strict_part):
    span_size = strict_part.shape[-1]
    unit_eye = jnp.eye(span_size, dtype=jnp.float32)
    running = unit_eye - strict_part
    power_term = strict_part
    for _ in range(span_size.bit_length() - 2):
        power_term = jnp.einsum("...ij,...jk->...ik", power_term, power_term)
        running = jnp.einsum("...ij,...jk->...ik", running, unit_eye + power_term)
    return running


def delta_mixer(queries, keys_in, values_in, strength, log_decay):
    heads_n, length, key_dim = queries.shape
    blocks_n = length // SPAN

    def to_blocks(tensor):
        return tensor.reshape(heads_n, blocks_n, SPAN, *tensor.shape[2:])

    queries, keys_in, values_in = (to_blocks(queries), to_blocks(keys_in), to_blocks(values_in))
    strength, log_decay = (to_blocks(strength), to_blocks(log_decay))
    cumulative = jnp.cumsum(log_decay, axis=-1)
    position = jnp.arange(SPAN)
    inclusive = position[:, None] >= position[None, :]
    strictly = position[:, None] > position[None, :]
    spread = jnp.where(inclusive, cumulative[..., :, None] - cumulative[..., None, :], -jnp.inf)
    decay_map = jnp.exp(spread)
    key_gram = jnp.einsum("hncd,hnmd->hncm", keys_in, keys_in)
    strict_part = jnp.where(strictly, strength[..., :, None] * key_gram * decay_map, 0.0)
    inverse = neumann_inverse(strict_part)
    fresh_vals = jnp.einsum("hncm,hnme->hnce", inverse, values_in * strength[..., None])
    correction = jnp.einsum(
        "hncm,hnmd->hncd", inverse, keys_in * (strength * jnp.exp(cumulative))[..., None]
    )
    attend_map = jnp.where(
        inclusive, jnp.einsum("hncd,hnmd->hncm", queries, keys_in) * decay_map, 0.0
    )
    query_dec = queries * jnp.exp(cumulative)[..., None]
    key_dec = keys_in * jnp.exp(cumulative[..., -1:] - cumulative)[..., None]
    carry_decay = jnp.exp(cumulative[..., -1])

    def advance(memory_state, inputs):
        fresh_blk, correct_blk, attend_blk, query_blk, key_blk, decay_blk = inputs
        new_values = fresh_blk - jnp.einsum("hcd,hde->hce", correct_blk, memory_state)
        output = jnp.einsum("hcd,hde->hce", query_blk, memory_state) + jnp.einsum(
            "hcm,hme->hce", attend_blk, new_values
        )
        memory_state = memory_state * decay_blk[:, None, None] + jnp.einsum(
            "hcd,hce->hde", key_blk, new_values
        )
        return (memory_state, output)

    stacked = tuple(
        (
            jnp.moveaxis(tensor, 1, 0)
            for tensor in (fresh_vals, correction, attend_map, query_dec, key_dec, carry_decay)
        )
    )
    initial = jnp.zeros((heads_n, key_dim, values_in.shape[-1]), jnp.float32)
    _, outputs = lax.scan(advance, initial, stacked)
    return jnp.transpose(outputs, (1, 0, 2, 3)).reshape(heads_n, length, -1)


def mixer_output(query_raw, key_raw, value_raw, beta_raw, decay_raw, rate_vals):
    length = query_raw.shape[0]
    heads_n = beta_raw.shape[0]

    def heads_first(matrix):
        return jnp.transpose(matrix.astype(jnp.float32).reshape(length, heads_n, -1), (1, 0, 2))

    queries = heads_first(query_raw)
    keys_in = heads_first(key_raw)
    values_in = heads_first(value_raw)
    queries = (
        queries
        * lax.rsqrt(jnp.sum(queries * queries, axis=-1, keepdims=True) + NORM_FLOOR)
        * queries.shape[-1] ** (-0.5)
    )
    keys_in = keys_in * lax.rsqrt(jnp.sum(keys_in * keys_in, axis=-1, keepdims=True) + NORM_FLOOR)
    strength = jax.nn.sigmoid(beta_raw)
    log_decay = -rate_vals[:, None] * jax.nn.softplus(decay_raw)
    mixer_out = delta_mixer(queries, keys_in, values_in, strength, log_decay)
    return jnp.transpose(mixer_out, (1, 0, 2)).reshape(length, -1)


def body(
    tokens, cotangent, mix_query, mix_key, mix_value, beta_pre, decay_pre, decay_rate,
    passages, passage_ids, query_weight, key_weight, value_weight, gate_weight,
):
    pass_local, span_rows, model_width = passages.shape
    flat_rows = passages.reshape(pass_local * span_rows, model_width)
    ids = passage_ids.reshape(24)
    place_of = jnp.arange(24, dtype=jnp.int32) * 16 + ids % 16
    wanted = (ids // 16)[:, None] == jnp.arange(64, dtype=jnp.int32)[None, :]
    table = jnp.max(jnp.where(wanted, place_of[:, None], -1), axis=0).astype(F32)[None, :]
    gate_rows = jnp.broadcast_to(gate_weight, (16, model_width))
    kv, qa, ca, tl, key_low, query_low, gate_row = call(
        gather_kernel,
        [
            shaped((NY, 1024, 512), BF16), shaped((16, 384, 256), BF16), shaped((16, 384, 256), BF16),
            shaped((16, 8, 128), F32), shaped((1024, 256), BF16), shaped((384, 256), BF16), shaped((8, 384), F32),
        ],
        [
            VMEM((NX, 384, 512), BF16), dma(2, 3), dma(2, 3), dma(2, 6), dma(2, 6), dma(2, 2, 7), dma(2, 2, 7),
            dma(2, 16), dma(2, 16), dma(15), dma(15),
        ],
        1, count=8,
    )(flat_rows, key_weight, value_weight, tokens, query_weight, gate_rows, cotangent, table)
    mixer_out = mixer_output(mix_query, mix_key, mix_value, beta_pre, decay_pre, decay_rate)
    lookup = tl[:, 6, 0:64].astype(jnp.int32)
    kv_one, qa_one, ca_one = kv.reshape(64, 64, 512), qa.reshape(96, 64, 256), ca.reshape(96, 64, 256)
    eg, tot, own = call(
        score_kernel,
        [shaped((64, 64, 128), F32), shaped((16, 8, 128), F32), shaped((8, 128), F32)],
        [
            VMEM((16, 8, 128), F32), VMEM((15, 8, 128), F32), VMEM((8, 128), F32),
            dma(15), dma(15), dma(15), dma(15),
        ],
        2, smem=1, count=5,
    )(lookup, kv_one, qa_one, ca_one, tl)
    kvg, qp = call(
        grads_kernel,
        [shaped((64, 64, 512), BF16), shaped((96, 64, 256), BF16)],
        [VMEM((64, 64, 512), F32), VMEM((96, 64, 256), F32)],
        None, smem=1, count=7,
    )(lookup, kv_one, qa_one, ca_one, tl, eg, tot)
    kvs, qhat_grad = call(
        return_kernel,
        [shaped((1024, 512), F32), shaped((384, 256), F32)],
        [
            VMEM((2, 512, 512), BF16), VMEM((2, 1024, 512), BF16), VMEM((NZ, 384, 256), BF16),
            VMEM((NZ, 384, 256), BF16), VMEM((2, 4, 384, 256), BF16),
            dma(2, 5), dma(2, 5), dma(2, 4), dma(2, 4), dma(8), dma(8),
        ],
        3, count=2,
    )(kvg.reshape(NY, 1024, 512), qp.reshape(16, 384, 256))

    query_float = query_low.astype(F32)
    query_scale = lax.rsqrt(jnp.mean(query_float * query_float, axis=-1, keepdims=True) + NORM_FLOOR)
    key_float = key_low.astype(F32)
    key_scale = lax.rsqrt(jnp.mean(key_float * key_float, axis=-1, keepdims=True) + NORM_FLOOR)
    gate_open = gate_row[0]
    dots = (own[0:6, 64:128] / own[0:6, 0:64]).reshape(384)
    grad_out = cotangent.astype(F32)
    gate_grad = (1.0 - gate_open) * (dots - gate_open * jnp.sum(grad_out * mixer_out, axis=-1))
    query_grad = (
        query_scale * qhat_grad
        - query_scale**3 * query_float * jnp.mean(query_float * qhat_grad, axis=-1, keepdims=True)
    ).astype(BF16)
    token_term = (
        lax.dot_general(query_grad, query_weight, CONTRACT_LAST, preferred_element_type=F32)
        + gate_grad[:, None] * gate_weight[0].astype(F32)[None, :]
    )
    token_grad = sum_at_owner(token_term.astype(BF16), "tp", 1).astype(BF16)
    key_hat_grad, value_grad = kvs[:, 0:256], kvs[:, 256:512]
    key_grad = (
        key_scale * key_hat_grad
        - key_scale**3 * key_float * jnp.mean(key_float * key_hat_grad, axis=-1, keepdims=True)
    ).astype(BF16)
    value_grad_low = value_grad.astype(BF16)
    row_term = lax.dot_general(
        key_grad, key_weight, CONTRACT_LAST, preferred_element_type=F32
    ) + lax.dot_general(value_grad_low, value_weight, CONTRACT_LAST, preferred_element_type=F32)
    passage_grad = sum_at_owner(
        row_term.reshape(pass_local, span_rows, model_width).astype(BF16), "tp", 2
    ).astype(BF16)
    weight_term = lax.dot_general(flat_rows, key_grad, CONTRACT_FIRST, preferred_element_type=F32)
    key_weight_grad = sum_by_axis(weight_term, ST, 0)
    return (token_grad, passage_grad, key_weight_grad)


def solution(mesh):
    torus = Mesh(mesh.devices.reshape(8, 4, 2, mesh.shape["tp"]), ("st_0", "st_1", "st_2", "tp"))
    return jax.shard_map(
        body,
        mesh=torus,
        in_specs=(
            P(ST, "tp"),
            P(ST, "tp"),
            P(ST, "tp"),
            P(ST, "tp"),
            P(ST, "tp"),
            P("tp", ST),
            P("tp", ST),
            P("tp"),
            P(ST, None, None),
            P(ST, None),
            P(None, "tp"),
            P(None, "tp"),
            P(None, "tp"),
            P("tp", None),
        ),
        out_specs=(P(ST, "tp"), P(ST, None, "tp"), P(ST, "tp")),
        check_vma=False,
    )
```

```python
import functools

import jax
import jax.numpy as jnp
from jax import lax
from jax.experimental import pallas as pl
from jax.experimental.pallas import tpu as pltpu
from jax.sharding import Mesh
from jax.sharding import PartitionSpec as P

SPAN = 64
ST = ("st_0", "st_1", "st_2")
MESH = pl.DeviceIdType.MESH
NZ, NY, NX = 8, 4, 4
VMEM = pltpu.VMEM
F32, BF16 = jnp.float32, jnp.bfloat16

NORM_FLOOR = 1.0
SCORE_GAIN = 4.0
CONTRACT_LAST = (((1,), (1,)), ((), ()))
CONTRACT_FIRST = (((0,), (0,)), ((), ()))


def place():
    return (lax.axis_index("st_0"), lax.axis_index("st_1"), lax.axis_index("st_2"), lax.axis_index("tp"))


def wrap(value, size):
    return lax.rem(value + size, size)


class Copies:
    def __init__(self):
        self.started = []

    def make(self, src, dst, send, recv, where):
        return pltpu.make_async_remote_copy(
            src_ref=src, dst_ref=dst, send_sem=send, recv_sem=recv, device_id=where, device_id_type=MESH
        )

    def start(self, src, dst, send, recv, where):
        copy = self.make(src, dst, send, recv, where)
        copy.start()
        self.started.append(copy)

    def arrived(self, dst, send, recv, where):
        self.make(dst, dst, send, recv, where).wait_recv()

    def finish(self):
        for copy in self.started:
            copy.wait_send()


def greet(peers):
    barrier = pltpu.get_barrier_semaphore()
    for peer in peers:
        pl.semaphore_signal(barrier, inc=1, device_id=peer, device_id_type=MESH)
    pl.semaphore_wait(barrier, len(peers))


def column_peers(z, c):
    me = z * 2 + c
    peers = []
    for step in range(1, 2 * NZ):
        other = wrap(me + step, 2 * NZ)
        peers.append({"st_0": other // 2, "st_2": lax.rem(other, 2)})
    return peers


def columns_of(rows):
    return jnp.transpose(rows)


def mixer_rows(mx):
    strength = jax.nn.sigmoid(mx[0:8])
    pre = mx[8:16]
    log_decay = -mx[16:17] * (jnp.maximum(pre, 0.0) + jnp.log1p(jnp.exp(-jnp.abs(pre))))
    lane = lax.broadcasted_iota(jnp.int32, (8, 128), 1)
    inner = lax.rem(lane, SPAN)
    total = log_decay
    for shift in (1, 2, 4, 8, 16, 32):
        total = total + jnp.where(inner >= shift, pltpu.roll(total, shift, axis=1), 0.0)
    ends = [
        jnp.sum(jnp.where(lane == at, total, 0.0), axis=1, keepdims=True) for at in (SPAN - 1, 2 * SPAN - 1)
    ]
    last = jnp.where(lane < SPAN, ends[0], ends[1])
    grown = jnp.exp(total)
    stacked = jnp.concatenate([strength, total, strength * grown, grown, jnp.exp(last - total)], axis=0)
    return total, ends, stacked


def low_dot(a, b, dims=(((1,), (0,)), ((), ()))):
    return lax.dot_general(a.astype(BF16), b.astype(BF16), dims, preferred_element_type=F32)


def mixer_prepare(b, mq, mk, mv, total, cols, fresh, corr, att, qdec, kdec):
    at = slice(b * SPAN, (b + 1) * SPAN)

    def both(ref):
        return jnp.concatenate([ref[at, 0:128], ref[at, 128:256]], axis=0).astype(F32)

    def unit(value):
        return value * lax.rsqrt(jnp.sum(value * value, axis=-1, keepdims=True) + NORM_FLOOR)

    def column(k):
        return cols[:, k * 8 + b : k * 8 + b + 1]

    queries, keys, values = unit(both(mq)) * 128 ** (-0.5), unit(both(mk)), both(mv)
    row, col = lax.broadcasted_iota(jnp.int32, (128, 128), 0), lax.broadcasted_iota(jnp.int32, (128, 128), 1)
    same = (row // SPAN) == (col // SPAN)
    spread = jnp.where(same & (row >= col), column(1) - total[b : b + 1, :], -1e30)
    decay = jnp.exp(spread)
    strict = jnp.where(same & (row > col), column(0) * low_dot(keys, keys, CONTRACT_LAST) * decay, 0.0)
    inverse = jnp.where(row == col, 1.0, 0.0) - strict
    power = strict
    for _ in range(SPAN.bit_length() - 2):
        power = low_dot(power, power)
        inverse = inverse + low_dot(inverse, power)
    fresh[b] = low_dot(inverse, values * column(0))
    corr[b] = low_dot(inverse, keys * column(2)).astype(BF16)
    att[b] = (low_dot(queries, keys, CONTRACT_LAST) * decay).astype(BF16)
    qdec[b] = (queries * column(3)).astype(BF16)
    kdec[b] = (keys * column(4)).astype(BF16)


def mixer_advance(b, state, cot, ends, fresh, corr, att, qdec, kdec, sums):
    heads = [slice(0, 64), slice(64, 128)]
    new = jnp.concatenate(
        [fresh[b, h, :] - low_dot(corr[b, h, :], state[i]) for i, h in enumerate(heads)], axis=0
    )
    out = jnp.concatenate([low_dot(qdec[b, h, :], state[i]) for i, h in enumerate(heads)], axis=0)
    out = out + low_dot(att[b], new)
    state = [
        jnp.exp(ends[i][b : b + 1, :]) * state[i] + low_dot(kdec[b, h, :], new[h], CONTRACT_FIRST)
        for i, h in enumerate(heads)
    ]
    at = slice(b * SPAN, (b + 1) * SPAN)
    grads = jnp.concatenate([cot[at, 0:128], cot[at, 128:256]], axis=0).astype(F32)
    lane = lax.broadcasted_iota(jnp.int32, (128, 128), 1)
    sums = jnp.where(lane == b, jnp.sum(grads * out, axis=-1, keepdims=True), sums)
    return state, sums


def gather_kernel(
    pas, wk, wv, tok, wq, gw, cot, tbl, mq, mk, mv, mx,
    kv, qa, ca, tl, klow, qlow, gown, wall, gall, md,
    toks, relay, fresh, corr, att, qdec, kdec,
    xs, xr, ys, yr, zs, zr, ps, pr, ts, tr, ws, wr, vs, vr, gs, gr,
):
    z, y, c, x = place()
    me = z * 2 + c
    up, down = {"st_0": wrap(z + 1, NZ)}, {"st_0": wrap(z - 1, NZ)}
    east, west = {"st_1": wrap(y + 1, NY)}, {"st_1": wrap(y - 1, NY)}
    front, back = {"tp": wrap(x + 1, NX)}, {"tp": wrap(x - 1, NX)}
    partner = {"st_2": 1 - c}
    peers = column_peers(z, c)
    across = {"tp": wrap(x + 2, NX)}
    greet(peers + [east, west, front, back, across])
    copies = Copies()
    half = 192
    zdirs, ydirs, xdirs = (up, down), (east, west), (front, back)

    def rows_of(ref, slot, h):
        return ref.at[slot, pl.ds(h * half, half), :]

    def z_send(k, ref, d, h):
        for way in (0, 1):
            if d == 4 and h != way:
                continue
            owner = wrap(z - (d - 1), NZ) if way == 0 else wrap(z + (d - 1), NZ)
            piece = rows_of(ref, owner * 2 + c, h)
            at = (d - 1) * 2 + h if d < 4 else 6
            copies.start(piece, piece, zs.at[k, way, at], zr.at[k, way, at], zdirs[way])

    def z_take(k, ref, d):
        for h in (0, 1):
            for way in (0, 1):
                if d == 4 and h != way:
                    continue
                owner = wrap(z - d, NZ) if way == 0 else wrap(z + d, NZ)
                piece = rows_of(ref, owner * 2 + c, h)
                at = (d - 1) * 2 + h if d < 4 else 6
                copies.arrived(piece, zs.at[k, way, at], zr.at[k, way, at], zdirs[way])
                if d < 3 or (d == 3 and h == way):
                    nxt = d * 2 + h if d < 3 else 6
                    copies.start(piece, piece, zs.at[k, way, nxt], zr.at[k, way, nxt], zdirs[way])
                to = 2 + way * 7 + at
                copies.start(piece, piece, ps.at[k, to], pr.at[k, to], partner)

    def own_send(k, ref):
        for h in (0, 1):
            z_send(k, ref, 1, h)
        for h in (0, 1):
            piece = rows_of(ref, me, h)
            copies.start(piece, piece, ps.at[k, h], pr.at[k, h], partner)

    def partner_take(k, ref):
        theirs = 1 - c
        for h in (0, 1):
            piece = rows_of(ref, z * 2 + theirs, h)
            copies.arrived(piece, ps.at[k, h], pr.at[k, h], partner)
        for d in (1, 2, 3, 4):
            for h in (0, 1):
                for way in (0, 1):
                    if d == 4 and h != way:
                        continue
                    owner = wrap(z - d, NZ) if way == 0 else wrap(z + d, NZ)
                    to = 2 + way * 7 + ((d - 1) * 2 + h if d < 4 else 6)
                    piece = rows_of(ref, owner * 2 + theirs, h)
                    copies.arrived(piece, ps.at[k, to], pr.at[k, to], partner)

    toks[x] = tok[...]
    for way in (0, 1):
        for h in (0, 1):
            piece = rows_of(toks, x, h)
            copies.start(piece, piece, xs.at[way, h], xr.at[way, h], xdirs[way])
    ca[me] = cot[...]
    own_send(0, ca)

    rows = 256

    def kv_rows(i):
        return kv.at[y, pl.ds(i * rows, rows), :]

    for i in range(4):
        block = pas[pl.ds(i * rows, rows), :]
        low = jnp.dot(block, wk[...], preferred_element_type=F32).astype(BF16)
        wide = low.astype(F32)
        scale = lax.rsqrt(jnp.mean(wide * wide, axis=-1, keepdims=True) + NORM_FLOOR)
        klow[pl.ds(i * rows, rows), :] = low
        kv[y, pl.ds(i * rows, rows), pl.ds(0, 256)] = (wide * scale).astype(BF16)
        kv[y, pl.ds(i * rows, rows), pl.ds(256, 256)] = jnp.dot(
            block, wv[...], preferred_element_type=F32
        ).astype(BF16)
        for way in (0, 1):
            copies.start(kv_rows(i), kv_rows(i), ys.at[way, i], yr.at[way, i], ydirs[way])

    def y_take(i):
        for way in (0, 1):
            owner = wrap(y - 1, NY) if way == 0 else wrap(y + 1, NY)
            piece = kv.at[owner, pl.ds(i * rows, rows), :]
            copies.arrived(piece, ys.at[way, i], yr.at[way, i], ydirs[way])
            if i % 2 == way:
                at = 4 + i // 2
                copies.start(piece, piece, ys.at[way, at], yr.at[way, at], ydirs[way])

    def y_last():
        owner = wrap(y + 2, NY)
        for i in range(4):
            way, at = i % 2, 4 + i // 2
            piece = kv.at[owner, pl.ds(i * rows, rows), :]
            copies.arrived(piece, ys.at[way, at], yr.at[way, at], ydirs[way])

    def x_take():
        for way in (0, 1):
            owner = wrap(x - 1, NX) if way == 0 else wrap(x + 1, NX)
            for h in (0, 1):
                piece = rows_of(toks, owner, h)
                copies.arrived(piece, xs.at[way, h], xr.at[way, h], xdirs[way])
                if h == way:
                    copies.start(piece, piece, xs.at[way, 2], xr.at[way, 2], xdirs[way])

    def x_last():
        owner = wrap(x + 2, NX)
        for way in (0, 1):
            piece = rows_of(toks, owner, way)
            copies.arrived(piece, xs.at[way, 2], xr.at[way, 2], xdirs[way])

    def project(owner):
        block = toks[owner]
        at = pl.ds(pl.multiple_of(owner * 512, 512), 512)
        return (
            jnp.dot(block, wq[at, :], preferred_element_type=F32),
            lax.dot_general(gw[:, at], block, CONTRACT_LAST, preferred_element_type=F32),
        )

    weights = (wk, wv, wq)
    via, behind = {"tp": wrap(x + 1 - 2 * c, NX)}, wrap(x - 1 + 2 * c, NX)

    def w_rows(owner):
        return pl.ds(pl.multiple_of(owner * 512 + c * 256, 256), 256)

    mine = pl.ds(pl.multiple_of(c * 256, 256), 256)

    def w_send():
        for i, ref in enumerate(weights):
            copies.start(ref.at[w_rows(wrap(x + 2, NX)), :], relay.at[i], ws.at[6 + i], wr.at[6 + i], via)
        for way in (0, 1):
            to = wrap(x + 1 - 2 * way, NX)
            for i, ref in enumerate(weights):
                copies.start(
                    ref.at[w_rows(to), :], wall.at[i, x, mine, :], ws.at[way * 3 + i], wr.at[way * 3 + i], xdirs[way]
                )
        for step, peer in enumerate((front, across, back)):
            at = pl.ds(pl.multiple_of(wrap(x + 1 + step, NX) * 512, 512), 512)
            copies.start(gw.at[:, at], gall.at[x], gs.at[step], gr.at[step], peer)
        own = pl.ds(pl.multiple_of(x * 512, 512), 512)
        for i, ref in enumerate(weights):
            wall[i, x] = ref[own, :]
        gall[x] = gw[:, own]

    def w_forward():
        for i in range(3):
            copies.arrived(relay.at[i], ws.at[6 + i], wr.at[6 + i], via)
            copies.start(relay.at[i], wall.at[i, behind, mine, :], ws.at[9 + i], wr.at[9 + i], via)

    def w_share(n, owner, first):
        for i in range(3):
            piece = wall.at[i, owner, mine, :]
            copies.arrived(piece, ws.at[first + i], wr.at[first + i], via)
            copies.start(piece, piece, vs.at[n * 3 + i], vr.at[n * 3 + i], partner)

    def w_last():
        theirs = pl.ds(pl.multiple_of((1 - c) * 256, 256), 256)
        for n, owner in enumerate((wrap(x - 1, NX), wrap(x + 1, NX), wrap(x + 2, NX))):
            for i in range(3):
                copies.arrived(wall.at[i, owner, theirs, :], vs.at[n * 3 + i], vr.at[n * 3 + i], partner)
        for step, peer in enumerate((front, across, back)):
            copies.arrived(gall.at[wrap(x - 1 - step, NX)], gs.at[step], gr.at[step], peer)

    total, ends, stacked = mixer_rows(mx[...])
    cols = columns_of(stacked)
    work = (fresh, corr, att, qdec, kdec)

    def prepare(b):
        mixer_prepare(b, mq, mk, mv, total, cols, *work)

    z_take(0, ca, 1)
    prepare(0)
    y_take(0)
    acc = project(x)
    x_take()
    w_send()
    z_take(0, ca, 2)
    for owner in (wrap(x - 1, NX), wrap(x + 1, NX)):
        more = project(owner)
        acc = (acc[0] + more[0], acc[1] + more[1])
    prepare(1)
    y_take(1)
    x_last()
    more = project(wrap(x + 2, NX))
    low = (acc[0] + more[0]).astype(BF16)
    gate = jax.nn.sigmoid(acc[1] + more[1])
    wide = low.astype(F32)
    scale = lax.rsqrt(jnp.mean(wide * wide, axis=-1, keepdims=True) + NORM_FLOOR)
    qlow[...] = low
    qa[me] = (wide * scale).astype(BF16)
    own_send(1, qa)
    z_take(0, ca, 3)
    tl[me] = jnp.zeros((8, 128), F32)
    for b in range(6):
        tl[me, b : b + 1, 0:64] = gate[0:1, b * 64 : b * 64 + 64]
    tl[me, 6:7, 0:64] = tbl[...]
    for step, peer in enumerate(peers):
        copies.start(tl.at[me], tl.at[me], ts.at[step], tr.at[step], peer)
    gown[...] = tl[me]
    y_take(2)
    prepare(2)
    z_take(1, qa, 1)
    w_forward()
    prepare(3)
    y_take(3)
    z_take(1, qa, 2)
    prepare(4)
    w_share(0, wrap(x - 1, NX), 0)
    w_share(1, wrap(x + 1, NX), 3)
    z_take(0, ca, 4)
    prepare(5)
    z_take(1, qa, 3)
    w_share(2, wrap(x + 2, NX), 9)
    state = [jnp.zeros((128, 128), F32), jnp.zeros((128, 128), F32)]
    sums = jnp.zeros((128, 128), F32)
    for b in range(6):
        state, sums = mixer_advance(b, state, cot, ends, *work, sums)
    turned = jnp.transpose(sums)[0:8]
    md[...] = turned[:, 0:64] + turned[:, 64:128]
    z_take(1, qa, 4)
    w_last()
    for step in range(2 * NZ - 1):
        other = wrap(me - (step + 1), 2 * NZ)
        copies.arrived(tl.at[other], ts.at[step], tr.at[step], peers[step])
    partner_take(0, ca)
    partner_take(1, qa)
    y_last()
    copies.finish()


def score_kernel(tb, kv, qa, ca, tl, eg, tot, own, sent, parts, total, ss, sr, bs, br):
    z, y, c, x = place()
    me = z * 2 + c
    peers = column_peers(z, c)
    greet(peers)
    copies = Copies()
    gain = SCORE_GAIN * 256 ** (-0.5)
    line = lax.broadcasted_iota(jnp.int32, (8, 128), 0)

    def reader(r, carry):
        tile = tl[r]
        stats = jnp.zeros((8, 128), F32)
        for yy in range(NY):
            entry = tb[r, (z * NY + yy) * 2 + c]
            used = entry >= 0
            safe = jnp.maximum(entry, 0)
            b, loc = safe // 64, lax.rem(safe, 16)
            keys_values = kv[yy * 16 + loc]
            scores = gain * lax.dot_general(
                keys_values[:, 0:256], qa[r * 6 + b], CONTRACT_LAST, preferred_element_type=F32
            )
            here = (line == b) & used
            gate = jnp.sum(jnp.where(line == b, tile, 0.0), axis=0, keepdims=True)
            grads = gate[:, 0:64] * lax.dot_general(
                keys_values[:, 256:512], ca[r * 6 + b], CONTRACT_LAST, preferred_element_type=F32
            )
            exps = jnp.exp(scores)
            both = jnp.concatenate([exps, grads], axis=1)
            eg[r * NY + yy] = both
            row = jnp.concatenate(
                [jnp.sum(exps, axis=0, keepdims=True), jnp.sum(exps * grads, axis=0, keepdims=True)], axis=1
            )
            stats = stats + jnp.where(here, row, 0.0)
        sent[r] = stats
        return carry

    lax.fori_loop(0, 2 * NZ, reader, 0)
    for step, peer in enumerate(peers):
        other = wrap(me + step + 1, 2 * NZ)
        copies.start(sent.at[other], parts.at[step], ss.at[step], sr.at[step], peer)
    whole = sent[me]
    for step in range(2 * NZ - 1):
        copies.arrived(parts.at[step], ss.at[step], sr.at[step], peers[step])
        whole = whole + parts[step]
    total[...] = whole
    tot[me] = whole
    own[...] = whole
    for step, peer in enumerate(peers):
        copies.start(total, tot.at[me], bs.at[step], br.at[step], peer)
    for step in range(2 * NZ - 1):
        other = wrap(me - (step + 1), 2 * NZ)
        copies.arrived(tot.at[other], bs.at[step], br.at[step], peers[step])
    copies.finish()


def grads_kernel(tb, kv, qa, ca, tl, eg, tot, kvg, qp, kacc, qacc):
    z, c = lax.axis_index("st_0"), lax.axis_index("st_2")
    gain = SCORE_GAIN * 256 ** (-0.5)
    kacc[...] = jnp.zeros(kacc.shape, F32)
    qacc[...] = jnp.zeros(qacc.shape, F32)

    @pl.loop(0, 2 * NZ)
    def _(r):
        for yy in range(NY):
            entry = tb[r, (z * NY + yy) * 2 + c]

            @pl.when(entry >= 0)
            def _():
                b, loc = entry // 64, lax.rem(entry, 16)
                row = tot[r, pl.ds(b, 1), :]
                gate = tl[r, pl.ds(b, 1), 0:64]
                norm = 1.0 / row[:, 0:64]
                both = eg[r * NY + yy]
                probs = both[:, 0:64] * norm
                slope = (probs * (both[:, 64:128] - row[:, 64:128] * norm)).astype(BF16)
                gated = (probs * gate).astype(BF16)
                at, slot = r * 6 + b, yy * 16 + loc
                key = gain * jnp.dot(slope, qa[at], preferred_element_type=F32)
                value = jnp.dot(gated, ca[at], preferred_element_type=F32)
                kacc[0, slot] += key.astype(BF16).astype(F32)
                kacc[1, slot] += value.astype(BF16).astype(F32)
                qacc[at] += gain * lax.dot_general(
                    slope, kv[slot, :, 0:256], CONTRACT_FIRST, preferred_element_type=F32
                )

    @pl.loop(0, 64)
    def _(i):
        kvg[0, i] = kacc[0, i].astype(BF16)
        kvg[1, i] = kacc[1, i].astype(BF16)

    @pl.loop(0, 96)
    def _(i):
        qp[i] = qacc[i].astype(BF16)


def finish_kernel(
    kvg, qp, klow, pas, qlow, wall, gall, own, md, gown,
    tgrad, pgrad, wgrad,
    ybuf, ysum, px, qs, zbuf, xall, pacc, xq, ggx, whalf, wget, wz, wbuf, wsum, wlast,
    ys, yr, zs, zr, ps, pr, xs, xr, qxs, qxr, gs, gr, us, ur, vs, vr, ls, lr,
):
    z, y, c, x = place()
    up, down = {"st_0": wrap(z + 1, NZ)}, {"st_0": wrap(z - 1, NZ)}
    east, west = {"st_1": wrap(y + 1, NY)}, {"st_1": wrap(y - 1, NY)}
    front, back, across = {"tp": wrap(x + 1, NX)}, {"tp": wrap(x - 1, NX)}, {"tp": wrap(x + 2, NX)}
    partner = {"st_2": 1 - c}
    spot = y * 2 + c
    plane = []
    for step in range(1, 8):
        other = wrap(spot + step, 8)
        plane.append({"st_1": other // 2, "st_2": lax.rem(other, 2)})
    greet([up, down, front, back, across] + plane)
    copies = Copies()
    zdirs, ydirs, xdirs = (up, down), (east, west), (front, back)

    for k in (4, 3, 5, 2, 6, 1, 7, 0):
        there = wrap(z + k, NZ)
        copies.start(qp.at[there * 2 + 1 - c], px.at[there], ps.at[k], pr.at[k], partner)

    far, beside = wrap(y + 2, NY), (wrap(y + 1, NY), wrap(y - 1, NY))

    def y_rows(j, part):
        return j // 2, pl.ds((j % 2) * 512 + part * 256, 256)

    def y_open(j):
        for way in (0, 1):
            p, at = y_rows(j, way)
            copies.start(kvg.at[p, far, at, :], ybuf.at[way, j], ys.at[0, way, j], yr.at[0, way, j], ydirs[way])
        for way in (0, 1):
            p, at = y_rows(j, 1 - way)
            copies.start(
                kvg.at[p, beside[way], at, :], ysum.at[way, p, at, :], ys.at[1, way, j], yr.at[1, way, j], ydirs[way]
            )

    def y_add(j):
        for way in (0, 1):
            p, at = y_rows(j, way)
            copies.arrived(ybuf.at[way, j], ys.at[0, way, j], yr.at[0, way, j], ydirs[way])
            ybuf[way, j] = (kvg[p, beside[way], at, :].astype(F32) + ybuf[way, j].astype(F32)).astype(BF16)
            copies.start(ybuf.at[way, j], ysum.at[way, p, at, :], ys.at[2, way, j], yr.at[2, way, j], ydirs[way])
        if j < 3:
            y_open(j + 1)

    def x_pieces(j, h):
        return j // 2, pl.ds((j % 2) * 512 + h * 256, 256)

    def y_done(j):
        for way in (0, 1):
            p, at = y_rows(j, 1 - way)
            copies.arrived(ysum.at[way, p, at, :], ys.at[1, way, j], yr.at[1, way, j], ydirs[way])
            p, at = y_rows(j, way)
            copies.arrived(ysum.at[way, p, at, :], ys.at[2, way, j], yr.at[2, way, j], ydirs[way])
        for h in (0, 1):
            p, at = x_pieces(j, h)
            grad = kvg[p, y, at, :].astype(F32) + ysum[0, p, at, :].astype(F32) + ysum[1, p, at, :].astype(F32)
            if p == 0:
                wide = klow[at, :].astype(F32)
                scale = lax.rsqrt(jnp.mean(wide * wide, axis=-1, keepdims=True) + NORM_FLOOR)
                inner = jnp.mean(wide * grad, axis=-1, keepdims=True)
                grad = scale * grad - (scale * scale * scale * inner) * wide
            xall[x, p, at, :] = grad.astype(BF16)
            for way in (0, 1):
                piece = xall.at[x, p, at, :]
                copies.start(piece, piece, xs.at[j, way, h], xr.at[j, way, h], xdirs[way])

    def x_take(j):
        for way in (0, 1):
            owner = wrap(x - 1 + 2 * way, NX)
            for h in (0, 1):
                p, at = x_pieces(j, h)
                piece = xall.at[owner, p, at, :]
                copies.arrived(piece, xs.at[j, way, h], xr.at[j, way, h], xdirs[way])
                if h == way:
                    copies.start(piece, piece, xs.at[j, way, 2], xr.at[j, way, 2], xdirs[way])

    def x_last(j):
        owner = wrap(x + 2, NX)
        for way in (0, 1):
            p, at = x_pieces(j, way)
            copies.arrived(xall.at[owner, p, at, :], xs.at[j, way, 2], xr.at[j, way, 2], xdirs[way])
        p = j // 2

        @pl.loop(0, 4)
        def _(i):
            at = pl.ds(pl.multiple_of((j % 2) * 512 + i * 128, 128), 128)
            term = lax.dot_general(xall[0, p, at, :], wall[p, 0], CONTRACT_LAST, preferred_element_type=F32)
            for h in range(1, NX):
                term += lax.dot_general(xall[h, p, at, :], wall[p, h], CONTRACT_LAST, preferred_element_type=F32)
            if p == 0:
                pacc[at, :] = term
            else:
                pgrad[at, :] = (pacc[at, :] + term).astype(BF16)

    def ring_step(d, value, slots, send, recv, half):
        for way in (0, 1):
            there = wrap(z + d, NZ) if way == 0 else wrap(z - d, NZ)
            at = pl.ds(way * half, half)
            if d == 3:
                copies.arrived(slots.at[way, 0, at, :], send.at[way, 3], recv.at[way, 3], zdirs[way])
                value[there, at, :] = (value[there, at, :].astype(F32) + slots[way, 0, at, :].astype(F32)).astype(BF16)
            elif d < 3:
                copies.arrived(slots.at[way, 3 - d], send.at[way, d], recv.at[way, d], zdirs[way])
                value[there] = (value[there].astype(F32) + slots[way, 3 - d].astype(F32)).astype(BF16)
            if d == 4:
                copies.start(value.at[there, at, :], slots.at[way, 0, at, :], send.at[way, 3], recv.at[way, 3], zdirs[way])
            else:
                copies.start(value.at[there], slots.at[way, 4 - d], send.at[way, d - 1], recv.at[way, d - 1], zdirs[way])

    def ring_last(value, slots, send, recv):
        result = value[z].astype(F32)
        for way in (0, 1):
            copies.arrived(slots.at[way, 3], send.at[way, 0], recv.at[way, 0], zdirs[way])
            result = result + slots[way, 3].astype(F32)
        return result

    def q_pair(k):
        there = wrap(z + k, NZ)
        copies.arrived(px.at[there], ps.at[k], pr.at[k], partner)
        qs[there] = (qp[there * 2 + c].astype(F32) + px[there].astype(F32)).astype(BF16)

    def q_step(d):
        ring_step(d, qs, zbuf, zs, zr, 192)

    def q_done():
        grad = ring_last(qs, zbuf, zs, zr)
        wide = qlow[...].astype(F32)
        scale = lax.rsqrt(jnp.mean(wide * wide, axis=-1, keepdims=True) + NORM_FLOOR)
        inner = jnp.mean(wide * grad, axis=-1, keepdims=True)
        xq[x] = (scale * grad - (scale * scale * scale * inner) * wide).astype(BF16)
        for way in (0, 1):
            for h in (0, 1):
                piece = xq.at[x, pl.ds(h * 192, 192), :]
                copies.start(piece, piece, qxs.at[way, h], qxr.at[way, h], xdirs[way])

    def gates():
        gate = gown[0:6, 0:64]
        dots = own[0:6, 64:128] / own[0:6, 0:64]
        ggx[x] = jnp.zeros((8, 128), F32)
        ggx[x, 0:6, 0:64] = (1.0 - gate) * (dots - gate * md[0:6, :])
        for step, peer in enumerate((front, across, back)):
            copies.start(ggx.at[x], ggx.at[x], gs.at[step], gr.at[step], peer)

    def q_take():
        for way in (0, 1):
            owner = wrap(x - 1 + 2 * way, NX)
            for h in (0, 1):
                piece = xq.at[owner, pl.ds(h * 192, 192), :]
                copies.arrived(piece, qxs.at[way, h], qxr.at[way, h], xdirs[way])
                if h == way:
                    copies.start(piece, piece, qxs.at[way, 2], qxr.at[way, 2], xdirs[way])

    def q_last():
        owner = wrap(x + 2, NX)
        for way in (0, 1):
            copies.arrived(xq.at[owner, pl.ds(way * 192, 192), :], qxs.at[way, 2], qxr.at[way, 2], xdirs[way])
        for step, peer in enumerate((front, across, back)):
            copies.arrived(ggx.at[wrap(x - 1 - step, NX)], gs.at[step], gr.at[step], peer)
        blank = [jnp.zeros((4, 64), F32)]
        slope = jnp.concatenate(
            [gall[h, 0:1, :].astype(F32) for h in range(NX)] + [jnp.zeros((4, 512), F32)], axis=0
        )
        for b in range(6):
            at = pl.ds(b * 64, 64)
            rows = jnp.concatenate([ggx[h, b : b + 1, 0:64] for h in range(NX)] + blank, axis=0)
            term = lax.dot_general(
                rows, slope, CONTRACT_FIRST, preferred_element_type=F32, precision=lax.Precision.HIGHEST
            )
            for h in range(NX):
                term += lax.dot_general(xq[h, at, :], wall[2, h], CONTRACT_LAST, preferred_element_type=F32)
            tgrad[at, :] = term.astype(BF16)

    keep = pl.ds(pl.multiple_of(c * 128, 128), 128)
    give = pl.ds(pl.multiple_of((1 - c) * 128, 128), 128)

    def w_tile(k):
        there = wrap(z + k, NZ)
        at = pl.ds(pl.multiple_of(there * 256, 256), 256)
        wsum[there] = lax.dot_general(
            pas[:, at], xall[x, 0], CONTRACT_FIRST, preferred_element_type=F32
        )
        whalf[there] = wsum[there, :, give]
        copies.start(whalf.at[there], wget.at[there], us.at[k], ur.at[k], partner)

    def w_pair(k):
        there = wrap(z + k, NZ)
        copies.arrived(wget.at[there], us.at[k], ur.at[k], partner)
        wz[there] = (wsum[there, :, keep] + wget[there]).astype(BF16)

    def w_step(d):
        ring_step(d, wz, wbuf, vs, vr, 128)

    def w_done():
        wsum[z, :, 0:128] = ring_last(wz, wbuf, vs, vr)
        for step, peer in enumerate(plane):
            other = wrap(spot + step + 1, 8)
            piece = wsum.at[z, pl.ds(pl.multiple_of(other * 32, 32), 32), pl.ds(0, 128)]
            copies.start(piece, wlast.at[spot], ls.at[step], lr.at[step], peer)
        wlast[spot] = wsum[z, pl.ds(pl.multiple_of(spot * 32, 32), 32), 0:128]

    def w_last():
        for step, peer in enumerate(plane):
            copies.arrived(wlast.at[wrap(spot - step - 1, 8)], ls.at[step], lr.at[step], peer)
        for k in (0, 1):
            wgrad[:, k * 128 : k * 128 + 128] = wlast[k] + wlast[2 + k] + wlast[4 + k] + wlast[6 + k]

    y_open(0)
    q_pair(4)
    q_step(4)
    for k in (3, 5):
        q_pair(k)
    y_add(0)
    q_step(3)
    for k in (2, 6, 1, 7, 0):
        q_pair(k)
    gates()
    y_done(0)
    q_step(2)
    y_add(1)
    q_step(1)
    x_take(0)
    y_done(1)
    for k in (4, 3, 5):
        w_tile(k)
    y_add(2)
    q_done()
    for k in (2, 6, 1, 7, 0):
        w_tile(k)
    x_take(1)
    y_done(2)
    w_pair(4)
    w_step(4)
    y_add(3)
    x_last(0)
    w_pair(3)
    w_pair(5)
    w_step(3)
    q_take()
    for k in (2, 6, 1, 7, 0):
        w_pair(k)
    w_step(2)
    x_take(2)
    x_last(1)
    y_done(3)
    w_step(1)
    q_last()
    w_done()
    x_take(3)
    x_last(2)
    w_last()
    x_last(3)
    copies.finish()


def shaped(shape, dtype):
    return jax.ShapeDtypeStruct(shape, dtype)


def dma(*shape):
    return pltpu.SemaphoreType.DMA(shape)


def call(kernel, outs, scratch, collective, smem=0, limit=48, count=0, **extra):
    in_specs = [pl.BlockSpec(memory_space=pltpu.SMEM)] * smem + [pl.BlockSpec(memory_space=VMEM)] * (count - smem)
    params = dict(vmem_limit_bytes=limit * 2**20)
    if collective is not None:
        params.update(collective_id=collective, has_side_effects=True)
    return pl.pallas_call(
        kernel,
        out_shape=outs,
        in_specs=in_specs,
        out_specs=[pl.BlockSpec(memory_space=VMEM)] * len(outs),
        scratch_shapes=scratch,
        compiler_params=pltpu.CompilerParams(**params),
        **extra,
    )


def body(
    tokens, cotangent, mix_query, mix_key, mix_value, beta_pre, decay_pre, decay_rate,
    passages, passage_ids, query_weight, key_weight, value_weight, gate_weight,
):
    pass_local, span_rows, model_width = passages.shape
    flat_rows = passages.reshape(pass_local * span_rows, model_width)
    ids = passage_ids.reshape(24)
    place_of = jnp.arange(24, dtype=jnp.int32) * 16 + ids % 16
    wanted = (ids // 16)[:, None] == jnp.arange(64, dtype=jnp.int32)[None, :]
    table = jnp.max(jnp.where(wanted, place_of[:, None], -1), axis=0).astype(F32)[None, :]
    gate_rows = jnp.broadcast_to(gate_weight, (16, model_width))

    def by_block(rows):
        return jnp.pad(rows.reshape(2, 6, 64).transpose(1, 0, 2).reshape(6, 128), ((0, 2), (0, 0)))

    rates = jnp.broadcast_to(jnp.repeat(decay_rate, 64)[None, :], (8, 128))
    scalars = jnp.concatenate([by_block(beta_pre), by_block(decay_pre), rates], axis=0)
    kv, qa, ca, tl, key_low, query_low, gown, wall, gall, md = call(
        gather_kernel,
        [
            shaped((NY, 1024, 512), BF16), shaped((16, 384, 256), BF16), shaped((16, 384, 256), BF16),
            shaped((16, 8, 128), F32), shaped((1024, 256), BF16), shaped((384, 256), BF16), shaped((8, 128), F32),
            shaped((3, NX, 512, 256), BF16), shaped((NX, 16, 512), BF16), shaped((8, 64), F32),
        ],
        [
            VMEM((NX, 384, 512), BF16), VMEM((3, 256, 256), BF16), VMEM((6, 128, 128), F32),
            VMEM((6, 128, 128), BF16), VMEM((6, 128, 128), BF16), VMEM((6, 128, 128), BF16), VMEM((6, 128, 128), BF16),
            dma(2, 3), dma(2, 3), dma(2, 6), dma(2, 6), dma(2, 2, 7), dma(2, 2, 7),
            dma(2, 16), dma(2, 16), dma(15), dma(15), dma(12), dma(12), dma(9), dma(9), dma(3), dma(3),
        ],
        1, count=12,
    )(
        flat_rows, key_weight, value_weight, tokens, query_weight, gate_rows, cotangent, table,
        mix_query, mix_key, mix_value, scalars,
    )
    lookup = tl[:, 6, 0:64].astype(jnp.int32)
    kv_one, qa_one, ca_one = kv.reshape(64, 64, 512), qa.reshape(96, 64, 256), ca.reshape(96, 64, 256)
    eg, tot, own = call(
        score_kernel,
        [shaped((64, 64, 128), F32), shaped((16, 8, 128), F32), shaped((8, 128), F32)],
        [
            VMEM((16, 8, 128), F32), VMEM((15, 8, 128), F32), VMEM((8, 128), F32),
            dma(15), dma(15), dma(15), dma(15),
        ],
        2, smem=1, count=5,
    )(lookup, kv_one, qa_one, ca_one, tl)
    kvg, qp = call(
        grads_kernel,
        [shaped((2, 64, 64, 256), BF16), shaped((96, 64, 256), BF16)],
        [VMEM((2, 64, 64, 256), F32), VMEM((96, 64, 256), F32)],
        None, smem=1, count=7,
    )(lookup, kv_one, qa_one, ca_one, tl, eg, tot)
    token_grad, passage_grad, key_weight_grad = call(
        finish_kernel,
        [shaped((384, 512), BF16), shaped((1024, 512), BF16), shaped((32, 256), F32)],
        [
            VMEM((2, 4, 256, 256), BF16), VMEM((2, 2, 1024, 256), BF16), VMEM((NZ, 384, 256), BF16),
            VMEM((NZ, 384, 256), BF16), VMEM((2, 4, 384, 256), BF16), VMEM((NX, 2, 1024, 256), BF16),
            VMEM((1024, 512), F32), VMEM((NX, 384, 256), BF16), VMEM((NX, 8, 128), F32),
            VMEM((NZ, 256, 128), F32), VMEM((NZ, 256, 128), F32), VMEM((NZ, 256, 128), BF16),
            VMEM((2, 4, 256, 128), BF16), VMEM((NZ, 256, 256), F32), VMEM((8, 32, 128), F32),
            dma(3, 2, 4), dma(3, 2, 4), dma(2, 4), dma(2, 4), dma(8), dma(8), dma(4, 2, 3), dma(4, 2, 3),
            dma(2, 3), dma(2, 3), dma(3), dma(3), dma(8), dma(8), dma(2, 4), dma(2, 4), dma(7), dma(7),
        ],
        3, count=10,
    )(
        kvg.reshape(2, NY, 1024, 256), qp.reshape(16, 384, 256), key_low, flat_rows, query_low,
        wall, gall, own, md, gown,
    )
    return (token_grad, passage_grad.reshape(pass_local, span_rows, 512), key_weight_grad)


def solution(mesh):
    torus = Mesh(mesh.devices.reshape(8, 4, 2, mesh.shape["tp"]), ("st_0", "st_1", "st_2", "tp"))
    return jax.shard_map(
        body,
        mesh=torus,
        in_specs=(
            P(ST, "tp"),
            P(ST, "tp"),
            P(ST, "tp"),
            P(ST, "tp"),
            P(ST, "tp"),
            P("tp", ST),
            P("tp", ST),
            P("tp"),
            P(ST, None, None),
            P(ST, None),
            P(None, "tp"),
            P(None, "tp"),
            P(None, "tp"),
            P("tp", None),
        ),
        out_specs=(P(ST, "tp"), P(ST, None, "tp"), P(ST, "tp")),
        check_vma=False,
    )
```

```python
import functools

import jax
import jax.numpy as jnp
from jax import lax
from jax.experimental import pallas as pl
from jax.experimental.pallas import tpu as pltpu
from jax.sharding import Mesh
from jax.sharding import PartitionSpec as P

SPAN = 64
ST = ("st_0", "st_1", "st_2")
MESH = pl.DeviceIdType.MESH
NZ, NY, NX = 8, 4, 4
VMEM = pltpu.VMEM
F32, BF16 = jnp.float32, jnp.bfloat16
LIMITS = (20, 6, 18, 24)

NORM_FLOOR = 1.0
SCORE_GAIN = 4.0
CONTRACT_LAST = (((1,), (1,)), ((), ()))
CONTRACT_FIRST = (((0,), (0,)), ((), ()))


def place():
    return (lax.axis_index("st_0"), lax.axis_index("st_1"), lax.axis_index("st_2"), lax.axis_index("tp"))


def wrap(value, size):
    return lax.rem(value + size, size)


class Copies:
    def __init__(self):
        self.started = []

    def make(self, src, dst, send, recv, where):
        return pltpu.make_async_remote_copy(
            src_ref=src, dst_ref=dst, send_sem=send, recv_sem=recv, device_id=where, device_id_type=MESH
        )

    def start(self, src, dst, send, recv, where):
        copy = self.make(src, dst, send, recv, where)
        copy.start()
        self.started.append(copy)

    def arrived(self, dst, send, recv, where):
        self.make(dst, dst, send, recv, where).wait_recv()

    def finish(self):
        for copy in self.started:
            copy.wait_send()


def greet(peers):
    barrier = pltpu.get_barrier_semaphore()
    for peer in peers:
        pl.semaphore_signal(barrier, inc=1, device_id=peer, device_id_type=MESH)
    pl.semaphore_wait(barrier, len(peers))


def column_peers(z, c):
    me = z * 2 + c
    peers = []
    for step in range(1, 2 * NZ):
        other = wrap(me + step, 2 * NZ)
        peers.append({"st_0": other // 2, "st_2": lax.rem(other, 2)})
    return peers


def columns_of(rows):
    return jnp.transpose(rows)


def mixer_rows(mx):
    strength = jax.nn.sigmoid(mx[0:8])
    pre = mx[8:16]
    log_decay = -mx[16:17] * (jnp.maximum(pre, 0.0) + jnp.log1p(jnp.exp(-jnp.abs(pre))))
    lane = lax.broadcasted_iota(jnp.int32, (8, 128), 1)
    inner = lax.rem(lane, SPAN)
    total = log_decay
    for shift in (1, 2, 4, 8, 16, 32):
        total = total + jnp.where(inner >= shift, pltpu.roll(total, shift, axis=1), 0.0)
    ends = [
        jnp.sum(jnp.where(lane == at, total, 0.0), axis=1, keepdims=True) for at in (SPAN - 1, 2 * SPAN - 1)
    ]
    last = jnp.where(lane < SPAN, ends[0], ends[1])
    grown = jnp.exp(total)
    stacked = jnp.concatenate([strength, total, strength * grown, grown, jnp.exp(last - total)], axis=0)
    return total, ends, stacked


def low_dot(a, b, dims=(((1,), (0,)), ((), ()))):
    return lax.dot_general(a.astype(BF16), b.astype(BF16), dims, preferred_element_type=F32)


def mixer_prepare(b, mq, mk, mv, total, cols, fresh, corr, att, qdec, kdec):
    at = slice(b * SPAN, (b + 1) * SPAN)

    def both(ref):
        return jnp.concatenate([ref[at, 0:128], ref[at, 128:256]], axis=0).astype(F32)

    def unit(value):
        return value * lax.rsqrt(jnp.sum(value * value, axis=-1, keepdims=True) + NORM_FLOOR)

    def column(k):
        return cols[:, k * 8 + b : k * 8 + b + 1]

    queries, keys, values = unit(both(mq)) * 128 ** (-0.5), unit(both(mk)), both(mv)
    row, col = lax.broadcasted_iota(jnp.int32, (128, 128), 0), lax.broadcasted_iota(jnp.int32, (128, 128), 1)
    same = (row // SPAN) == (col // SPAN)
    spread = jnp.where(same & (row >= col), column(1) - total[b : b + 1, :], -1e30)
    decay = jnp.exp(spread)
    strict = jnp.where(same & (row > col), column(0) * low_dot(keys, keys, CONTRACT_LAST) * decay, 0.0)
    inverse = jnp.where(row == col, 1.0, 0.0) - strict
    power = strict
    for _ in range(SPAN.bit_length() - 2):
        power = low_dot(power, power)
        inverse = inverse + low_dot(inverse, power)
    fresh[b] = low_dot(inverse, values * column(0))
    corr[b] = low_dot(inverse, keys * column(2)).astype(BF16)
    att[b] = (low_dot(queries, keys, CONTRACT_LAST) * decay).astype(BF16)
    qdec[b] = (queries * column(3)).astype(BF16)
    kdec[b] = (keys * column(4)).astype(BF16)


def mixer_advance(b, state, cot, ends, fresh, corr, att, qdec, kdec, sums):
    heads = [slice(0, 64), slice(64, 128)]
    new = jnp.concatenate(
        [fresh[b, h, :] - low_dot(corr[b, h, :], state[i]) for i, h in enumerate(heads)], axis=0
    )
    out = jnp.concatenate([low_dot(qdec[b, h, :], state[i]) for i, h in enumerate(heads)], axis=0)
    out = out + low_dot(att[b], new)
    state = [
        jnp.exp(ends[i][b : b + 1, :]) * state[i] + low_dot(kdec[b, h, :], new[h], CONTRACT_FIRST)
        for i, h in enumerate(heads)
    ]
    at = slice(b * SPAN, (b + 1) * SPAN)
    grads = jnp.concatenate([cot[at, 0:128], cot[at, 128:256]], axis=0).astype(F32)
    lane = lax.broadcasted_iota(jnp.int32, (128, 128), 1)
    sums = jnp.where(lane == b, jnp.sum(grads * out, axis=-1, keepdims=True), sums)
    return state, sums


def gather_kernel(
    pas_in, wk_in, wv_in, tok_in, wq_in, gw_in, cot_in, mq_in, mk_in, mv_in, ids_in, beta_in, pre_in, rate_in,
    kv, qa, ca, tl, tb, klow, qlow, gown, wall, gall, md,
    pas, wk, wv, wq, mq, mk, mv, gw_row, ids, beta, pre, rate, gw, mx,
    toks, relay, fresh, corr, att, qdec, kdec,
    ins, hs, hr, xs, xr, ys, yr, zs, zr, ps, pr, ts, tr, ws, wr, vs, vr, gs, gr,
):
    z, y, c, x = place()
    me = z * 2 + c
    up, down = {"st_0": wrap(z + 1, NZ)}, {"st_0": wrap(z - 1, NZ)}
    east, west = {"st_1": wrap(y + 1, NY)}, {"st_1": wrap(y - 1, NY)}
    front, back = {"tp": wrap(x + 1, NX)}, {"tp": wrap(x - 1, NX)}
    partner = {"st_2": 1 - c}
    peers = column_peers(z, c)
    across = {"tp": wrap(x + 2, NX)}
    reads = {}

    def fetch(name, src, dst):
        reads[name] = pltpu.make_async_copy(src, dst, ins.at[len(reads)])
        reads[name].start()

    fetch("tok", tok_in, toks.at[x])
    fetch("cot", cot_in, ca.at[me])
    fetch("wk", wk_in, wk)
    fetch("wv", wv_in, wv)
    for i in range(4):
        fetch(f"pas{i}", pas_in.at[pl.ds(i * 256, 256), :], pas.at[pl.ds(i * 256, 256), :])
    fetch("wq", wq_in, wq)
    for name, src, dst in (
        ("gw", gw_in, gw_row), ("ids", ids_in, ids), ("beta", beta_in, beta), ("pre", pre_in, pre),
        ("rate", rate_in, rate), ("mq", mq_in, mq), ("mk", mk_in, mk), ("mv", mv_in, mv),
    ):
        fetch(name, src, dst)
    greet(peers + [east, west, front, back, across])
    copies = Copies()
    half = 192
    zdirs, ydirs, xdirs = (up, down), (east, west), (front, back)

    def rows_of(ref, slot, h):
        return ref.at[slot, pl.ds(h * half, half), :]

    def z_send(k, ref, d, h):
        for way in (0, 1):
            if d == 4 and h != way:
                continue
            owner = wrap(z - (d - 1), NZ) if way == 0 else wrap(z + (d - 1), NZ)
            piece = rows_of(ref, owner * 2 + c, h)
            at = (d - 1) * 2 + h if d < 4 else 6
            copies.start(piece, piece, zs.at[k, way, at], zr.at[k, way, at], zdirs[way])

    def z_take(k, ref, d):
        for h in (0, 1):
            for way in (0, 1):
                if d == 4 and h != way:
                    continue
                owner = wrap(z - d, NZ) if way == 0 else wrap(z + d, NZ)
                piece = rows_of(ref, owner * 2 + c, h)
                at = (d - 1) * 2 + h if d < 4 else 6
                copies.arrived(piece, zs.at[k, way, at], zr.at[k, way, at], zdirs[way])
                if d < 3 or (d == 3 and h == way):
                    nxt = d * 2 + h if d < 3 else 6
                    copies.start(piece, piece, zs.at[k, way, nxt], zr.at[k, way, nxt], zdirs[way])
                to = 2 + way * 7 + at
                copies.start(piece, piece, ps.at[k, to], pr.at[k, to], partner)

    def own_send(k, ref):
        for h in (0, 1):
            z_send(k, ref, 1, h)
        for h in (0, 1):
            piece = rows_of(ref, me, h)
            copies.start(piece, piece, ps.at[k, h], pr.at[k, h], partner)

    def partner_take(k, ref):
        theirs = 1 - c
        for h in (0, 1):
            piece = rows_of(ref, z * 2 + theirs, h)
            copies.arrived(piece, ps.at[k, h], pr.at[k, h], partner)
        for d in (1, 2, 3, 4):
            for h in (0, 1):
                for way in (0, 1):
                    if d == 4 and h != way:
                        continue
                    owner = wrap(z - d, NZ) if way == 0 else wrap(z + d, NZ)
                    to = 2 + way * 7 + ((d - 1) * 2 + h if d < 4 else 6)
                    piece = rows_of(ref, owner * 2 + theirs, h)
                    copies.arrived(piece, ps.at[k, to], pr.at[k, to], partner)

    reads["tok"].wait()
    for way in (0, 1):
        for h in (0, 1):
            piece = rows_of(toks, x, h)
            copies.start(piece, piece, xs.at[way, h], xr.at[way, h], xdirs[way])
    reads["cot"].wait()
    own_send(0, ca)

    rows = 256

    def kv_rows(i):
        return kv.at[y, pl.ds(i * rows, rows), :]

    reads["wk"].wait()
    reads["wv"].wait()
    for i in range(4):
        reads[f"pas{i}"].wait()
        block = pas[pl.ds(i * rows, rows), :]
        low = jnp.dot(block, wk[...], preferred_element_type=F32).astype(BF16)
        wide = low.astype(F32)
        scale = lax.rsqrt(jnp.mean(wide * wide, axis=-1, keepdims=True) + NORM_FLOOR)
        klow[pl.ds(i * rows, rows), :] = low
        kv[y, pl.ds(i * rows, rows), pl.ds(0, 256)] = (wide * scale).astype(BF16)
        kv[y, pl.ds(i * rows, rows), pl.ds(256, 256)] = jnp.dot(
            block, wv[...], preferred_element_type=F32
        ).astype(BF16)
        for way in (0, 1):
            copies.start(kv_rows(i), kv_rows(i), ys.at[way, i], yr.at[way, i], ydirs[way])

    def y_take(i):
        for way in (0, 1):
            owner = wrap(y - 1, NY) if way == 0 else wrap(y + 1, NY)
            piece = kv.at[owner, pl.ds(i * rows, rows), :]
            copies.arrived(piece, ys.at[way, i], yr.at[way, i], ydirs[way])
            if i % 2 == way:
                at = 4 + i // 2
                copies.start(piece, piece, ys.at[way, at], yr.at[way, at], ydirs[way])

    def y_last():
        owner = wrap(y + 2, NY)
        for i in range(4):
            way, at = i % 2, 4 + i // 2
            piece = kv.at[owner, pl.ds(i * rows, rows), :]
            copies.arrived(piece, ys.at[way, at], yr.at[way, at], ydirs[way])

    def x_take():
        for way in (0, 1):
            owner = wrap(x - 1, NX) if way == 0 else wrap(x + 1, NX)
            for h in (0, 1):
                piece = rows_of(toks, owner, h)
                copies.arrived(piece, xs.at[way, h], xr.at[way, h], xdirs[way])
                if h == way:
                    copies.start(piece, piece, xs.at[way, 2], xr.at[way, 2], xdirs[way])

    def x_last():
        owner = wrap(x + 2, NX)
        for way in (0, 1):
            piece = rows_of(toks, owner, way)
            copies.arrived(piece, xs.at[way, 2], xr.at[way, 2], xdirs[way])

    def project(owner):
        block = toks[owner]
        at = pl.ds(pl.multiple_of(owner * 512, 512), 512)
        return (
            jnp.dot(block, wq[at, :], preferred_element_type=F32),
            lax.dot_general(gw[:, at], block, CONTRACT_LAST, preferred_element_type=F32),
        )

    weights = (wk, wv, wq)
    via, behind = {"tp": wrap(x + 1 - 2 * c, NX)}, wrap(x - 1 + 2 * c, NX)

    def w_rows(owner):
        return pl.ds(pl.multiple_of(owner * 512 + c * 256, 256), 256)

    mine = pl.ds(pl.multiple_of(c * 256, 256), 256)

    def w_send():
        for i, ref in enumerate(weights):
            copies.start(ref.at[w_rows(wrap(x + 2, NX)), :], relay.at[i], ws.at[6 + i], wr.at[6 + i], via)
        for way in (0, 1):
            to = wrap(x + 1 - 2 * way, NX)
            for i, ref in enumerate(weights):
                copies.start(
                    ref.at[w_rows(to), :], wall.at[i, x, mine, :], ws.at[way * 3 + i], wr.at[way * 3 + i], xdirs[way]
                )
        for step, peer in enumerate((front, across, back)):
            at = pl.ds(pl.multiple_of(wrap(x + 1 + step, NX) * 512, 512), 512)
            copies.start(gw.at[:, at], gall.at[x], gs.at[step], gr.at[step], peer)
        own = pl.ds(pl.multiple_of(x * 512, 512), 512)
        for i, ref in enumerate(weights):
            wall[i, x] = ref[own, :]
        gall[x] = gw[:, own]

    def w_forward():
        for i in range(3):
            copies.arrived(relay.at[i], ws.at[6 + i], wr.at[6 + i], via)
            copies.start(relay.at[i], wall.at[i, behind, mine, :], ws.at[9 + i], wr.at[9 + i], via)

    def w_share(n, owner, first):
        for i in range(3):
            piece = wall.at[i, owner, mine, :]
            copies.arrived(piece, ws.at[first + i], wr.at[first + i], via)
            copies.start(piece, piece, vs.at[n * 3 + i], vr.at[n * 3 + i], partner)

    def w_last():
        theirs = pl.ds(pl.multiple_of((1 - c) * 256, 256), 256)
        for n, owner in enumerate((wrap(x - 1, NX), wrap(x + 1, NX), wrap(x + 2, NX))):
            for i in range(3):
                copies.arrived(wall.at[i, owner, theirs, :], vs.at[n * 3 + i], vr.at[n * 3 + i], partner)
        for step, peer in enumerate((front, across, back)):
            copies.arrived(gall.at[wrap(x - 1 - step, NX)], gs.at[step], gr.at[step], peer)

    for name in ("wq", "gw", "ids", "beta", "pre", "rate", "mq", "mk", "mv"):
        reads[name].wait()
    gw[...] = jnp.broadcast_to(gw_row[...].astype(F32), (16, 2048)).astype(BF16)
    lanes = lax.broadcasted_iota(jnp.int32, (1, 128), 1)
    row = jnp.full((1, 128), -1, jnp.int32)
    for b in range(6):
        for p in range(4):
            each = jnp.broadcast_to(ids[b : b + 1, p : p + 1], (1, 128))
            row = jnp.where(lanes == each // 16, (b * 4 + p) * 16 + lax.rem(each, 16), row)
    tb[me] = row
    mx[...] = jnp.zeros((24, 128), F32)
    for b in range(6):
        for h in range(2):
            mx[b : b + 1, h * 64 : h * 64 + 64] = beta[h : h + 1, b * 64 : b * 64 + 64]
            mx[8 + b : 9 + b, h * 64 : h * 64 + 64] = pre[h : h + 1, b * 64 : b * 64 + 64]
    for h in range(2):
        mx[16:17, h * 64 : h * 64 + 64] = jnp.broadcast_to(rate[0:1, h : h + 1], (1, 64))
    total, ends, stacked = mixer_rows(mx[...])
    cols = columns_of(stacked)
    work = (fresh, corr, att, qdec, kdec)

    def prepare(b):
        mixer_prepare(b, mq, mk, mv, total, cols, *work)

    z_take(0, ca, 1)
    prepare(0)
    y_take(0)
    acc = project(x)
    x_take()
    w_send()
    z_take(0, ca, 2)
    for owner in (wrap(x - 1, NX), wrap(x + 1, NX)):
        more = project(owner)
        acc = (acc[0] + more[0], acc[1] + more[1])
    prepare(1)
    y_take(1)
    x_last()
    more = project(wrap(x + 2, NX))
    low = (acc[0] + more[0]).astype(BF16)
    gate = jax.nn.sigmoid(acc[1] + more[1])
    wide = low.astype(F32)
    scale = lax.rsqrt(jnp.mean(wide * wide, axis=-1, keepdims=True) + NORM_FLOOR)
    qlow[...] = low
    qa[me] = (wide * scale).astype(BF16)
    own_send(1, qa)
    z_take(0, ca, 3)
    tl[me] = jnp.zeros((8, 128), F32)
    for b in range(6):
        tl[me, b : b + 1, 0:64] = gate[0:1, b * 64 : b * 64 + 64]
    for step, peer in enumerate(peers):
        copies.start(tl.at[me], tl.at[me], ts.at[step], tr.at[step], peer)
        copies.start(tb.at[me], tb.at[me], hs.at[step], hr.at[step], peer)
    gown[...] = tl[me]
    y_take(2)
    prepare(2)
    z_take(1, qa, 1)
    w_forward()
    prepare(3)
    y_take(3)
    z_take(1, qa, 2)
    prepare(4)
    w_share(0, wrap(x - 1, NX), 0)
    w_share(1, wrap(x + 1, NX), 3)
    z_take(0, ca, 4)
    prepare(5)
    z_take(1, qa, 3)
    w_share(2, wrap(x + 2, NX), 9)
    state = [jnp.zeros((128, 128), F32), jnp.zeros((128, 128), F32)]
    sums = jnp.zeros((128, 128), F32)
    for b in range(6):
        state, sums = mixer_advance(b, state, ca.at[me], ends, *work, sums)
    turned = jnp.transpose(sums)[0:8]
    md[...] = turned[:, 0:64] + turned[:, 64:128]
    z_take(1, qa, 4)
    w_last()
    for step in range(2 * NZ - 1):
        other = wrap(me - (step + 1), 2 * NZ)
        copies.arrived(tl.at[other], ts.at[step], tr.at[step], peers[step])
        copies.arrived(tb.at[other], hs.at[step], hr.at[step], peers[step])
    partner_take(0, ca)
    partner_take(1, qa)
    y_last()
    copies.finish()


def score_kernel(tb, kv, qa, ca, tl, eg, tot, own, sent, parts, total, ss, sr, bs, br):
    z, y, c, x = place()
    me = z * 2 + c
    peers = column_peers(z, c)
    greet(peers)
    copies = Copies()
    gain = SCORE_GAIN * 256 ** (-0.5)
    line = lax.broadcasted_iota(jnp.int32, (8, 128), 0)

    def reader(r, carry):
        tile = tl[r]
        stats = jnp.zeros((8, 128), F32)
        for yy in range(NY):
            entry = tb[r, 0, (z * NY + yy) * 2 + c]
            used = entry >= 0
            safe = jnp.maximum(entry, 0)
            b, loc = safe // 64, lax.rem(safe, 16)
            keys_values = kv[yy * 16 + loc]
            scores = gain * lax.dot_general(
                keys_values[:, 0:256], qa[r * 6 + b], CONTRACT_LAST, preferred_element_type=F32
            )
            here = (line == b) & used
            gate = jnp.sum(jnp.where(line == b, tile, 0.0), axis=0, keepdims=True)
            grads = gate[:, 0:64] * lax.dot_general(
                keys_values[:, 256:512], ca[r * 6 + b], CONTRACT_LAST, preferred_element_type=F32
            )
            exps = jnp.exp(scores)
            both = jnp.concatenate([exps, grads], axis=1)
            eg[r * NY + yy] = both
            row = jnp.concatenate(
                [jnp.sum(exps, axis=0, keepdims=True), jnp.sum(exps * grads, axis=0, keepdims=True)], axis=1
            )
            stats = stats + jnp.where(here, row, 0.0)
        sent[r] = stats
        return carry

    lax.fori_loop(0, 2 * NZ, reader, 0)
    for step, peer in enumerate(peers):
        other = wrap(me + step + 1, 2 * NZ)
        copies.start(sent.at[other], parts.at[step], ss.at[step], sr.at[step], peer)
    whole = sent[me]
    for step in range(2 * NZ - 1):
        copies.arrived(parts.at[step], ss.at[step], sr.at[step], peers[step])
        whole = whole + parts[step]
    total[...] = whole
    tot[me] = whole
    own[...] = whole
    for step, peer in enumerate(peers):
        copies.start(total, tot.at[me], bs.at[step], br.at[step], peer)
    for step in range(2 * NZ - 1):
        other = wrap(me - (step + 1), 2 * NZ)
        copies.arrived(tot.at[other], bs.at[step], br.at[step], peers[step])
    copies.finish()


def grads_kernel(tb, kv, qa, ca, tl, eg, tot, kvg, qp, kacc, qacc):
    z, c = lax.axis_index("st_0"), lax.axis_index("st_2")
    gain = SCORE_GAIN * 256 ** (-0.5)
    kacc[...] = jnp.zeros(kacc.shape, F32)
    qacc[...] = jnp.zeros(qacc.shape, F32)

    @pl.loop(0, 2 * NZ)
    def _(r):
        for yy in range(NY):
            entry = tb[r, 0, (z * NY + yy) * 2 + c]

            @pl.when(entry >= 0)
            def _():
                b, loc = entry // 64, lax.rem(entry, 16)
                row = tot[r, pl.ds(b, 1), :]
                gate = tl[r, pl.ds(b, 1), 0:64]
                norm = 1.0 / row[:, 0:64]
                both = eg[r * NY + yy]
                probs = both[:, 0:64] * norm
                slope = (probs * (both[:, 64:128] - row[:, 64:128] * norm)).astype(BF16)
                gated = (probs * gate).astype(BF16)
                at, slot = r * 6 + b, yy * 16 + loc
                key = gain * jnp.dot(slope, qa[at], preferred_element_type=F32)
                value = jnp.dot(gated, ca[at], preferred_element_type=F32)
                kacc[0, slot] += key.astype(BF16).astype(F32)
                kacc[1, slot] += value.astype(BF16).astype(F32)
                qacc[at] += gain * lax.dot_general(
                    slope, kv[slot, :, 0:256], CONTRACT_FIRST, preferred_element_type=F32
                )

    @pl.loop(0, 64)
    def _(i):
        kvg[0, i] = kacc[0, i].astype(BF16)
        kvg[1, i] = kacc[1, i].astype(BF16)

    @pl.loop(0, 96)
    def _(i):
        qp[i] = qacc[i].astype(BF16)


def finish_kernel(
    kvg, qp, klow, pas, qlow, wall, gall, own, md, gown,
    tgrad, pgrad, wgrad,
    ybuf, ysum, px, qs, zbuf, xall, pacc, xq, ggx, whalf, wget, wz, wbuf, wsum, wlast,
    ys, yr, zs, zr, ps, pr, xs, xr, qxs, qxr, gs, gr, us, ur, vs, vr, ls, lr,
):
    z, y, c, x = place()
    up, down = {"st_0": wrap(z + 1, NZ)}, {"st_0": wrap(z - 1, NZ)}
    east, west = {"st_1": wrap(y + 1, NY)}, {"st_1": wrap(y - 1, NY)}
    front, back, across = {"tp": wrap(x + 1, NX)}, {"tp": wrap(x - 1, NX)}, {"tp": wrap(x + 2, NX)}
    partner = {"st_2": 1 - c}
    spot = y * 2 + c
    plane = []
    for step in range(1, 8):
        other = wrap(spot + step, 8)
        plane.append({"st_1": other // 2, "st_2": lax.rem(other, 2)})
    greet([up, down, front, back, across] + plane)
    copies = Copies()
    zdirs, ydirs, xdirs = (up, down), (east, west), (front, back)

    for k in (4, 3, 5, 2, 6, 1, 7, 0):
        there = wrap(z + k, NZ)
        copies.start(qp.at[there * 2 + 1 - c], px.at[there], ps.at[k], pr.at[k], partner)

    far, beside = wrap(y + 2, NY), (wrap(y + 1, NY), wrap(y - 1, NY))

    def y_rows(j, part):
        return j // 2, pl.ds((j % 2) * 512 + part * 256, 256)

    def y_open(j):
        for way in (0, 1):
            p, at = y_rows(j, way)
            copies.start(kvg.at[p, far, at, :], ybuf.at[way, j], ys.at[0, way, j], yr.at[0, way, j], ydirs[way])
        for way in (0, 1):
            p, at = y_rows(j, 1 - way)
            copies.start(
                kvg.at[p, beside[way], at, :], ysum.at[way, p, at, :], ys.at[1, way, j], yr.at[1, way, j], ydirs[way]
            )

    def y_add(j):
        for way in (0, 1):
            p, at = y_rows(j, way)
            copies.arrived(ybuf.at[way, j], ys.at[0, way, j], yr.at[0, way, j], ydirs[way])
            ybuf[way, j] = (kvg[p, beside[way], at, :].astype(F32) + ybuf[way, j].astype(F32)).astype(BF16)
            copies.start(ybuf.at[way, j], ysum.at[way, p, at, :], ys.at[2, way, j], yr.at[2, way, j], ydirs[way])
        if j < 3:
            y_open(j + 1)

    def x_pieces(j, h):
        return j // 2, pl.ds((j % 2) * 512 + h * 256, 256)

    def y_done(j):
        for way in (0, 1):
            p, at = y_rows(j, 1 - way)
            copies.arrived(ysum.at[way, p, at, :], ys.at[1, way, j], yr.at[1, way, j], ydirs[way])
            p, at = y_rows(j, way)
            copies.arrived(ysum.at[way, p, at, :], ys.at[2, way, j], yr.at[2, way, j], ydirs[way])
        for h in (0, 1):
            p, at = x_pieces(j, h)
            grad = kvg[p, y, at, :].astype(F32) + ysum[0, p, at, :].astype(F32) + ysum[1, p, at, :].astype(F32)
            if p == 0:
                wide = klow[at, :].astype(F32)
                scale = lax.rsqrt(jnp.mean(wide * wide, axis=-1, keepdims=True) + NORM_FLOOR)
                inner = jnp.mean(wide * grad, axis=-1, keepdims=True)
                grad = scale * grad - (scale * scale * scale * inner) * wide
            xall[x, p, at, :] = grad.astype(BF16)
            for way in (0, 1):
                piece = xall.at[x, p, at, :]
                copies.start(piece, piece, xs.at[j, way, h], xr.at[j, way, h], xdirs[way])

    def x_take(j):
        for way in (0, 1):
            owner = wrap(x - 1 + 2 * way, NX)
            for h in (0, 1):
                p, at = x_pieces(j, h)
                piece = xall.at[owner, p, at, :]
                copies.arrived(piece, xs.at[j, way, h], xr.at[j, way, h], xdirs[way])
                if h == way:
                    copies.start(piece, piece, xs.at[j, way, 2], xr.at[j, way, 2], xdirs[way])

    def x_last(j):
        owner = wrap(x + 2, NX)
        for way in (0, 1):
            p, at = x_pieces(j, way)
            copies.arrived(xall.at[owner, p, at, :], xs.at[j, way, 2], xr.at[j, way, 2], xdirs[way])
        p = j // 2

        @pl.loop(0, 4)
        def _(i):
            at = pl.ds(pl.multiple_of((j % 2) * 512 + i * 128, 128), 128)
            term = lax.dot_general(xall[0, p, at, :], wall[p, 0], CONTRACT_LAST, preferred_element_type=F32)
            for h in range(1, NX):
                term += lax.dot_general(xall[h, p, at, :], wall[p, h], CONTRACT_LAST, preferred_element_type=F32)
            if p == 0:
                pacc[at, :] = term
            else:
                pgrad[at, :] = (pacc[at, :] + term).astype(BF16)

    def ring_step(d, value, slots, send, recv, half):
        for way in (0, 1):
            there = wrap(z + d, NZ) if way == 0 else wrap(z - d, NZ)
            at = pl.ds(way * half, half)
            if d == 3:
                copies.arrived(slots.at[way, 0, at, :], send.at[way, 3], recv.at[way, 3], zdirs[way])
                value[there, at, :] = (value[there, at, :].astype(F32) + slots[way, 0, at, :].astype(F32)).astype(BF16)
            elif d < 3:
                copies.arrived(slots.at[way, 3 - d], send.at[way, d], recv.at[way, d], zdirs[way])
                value[there] = (value[there].astype(F32) + slots[way, 3 - d].astype(F32)).astype(BF16)
            if d == 4:
                copies.start(value.at[there, at, :], slots.at[way, 0, at, :], send.at[way, 3], recv.at[way, 3], zdirs[way])
            else:
                copies.start(value.at[there], slots.at[way, 4 - d], send.at[way, d - 1], recv.at[way, d - 1], zdirs[way])

    def ring_last(value, slots, send, recv):
        result = value[z].astype(F32)
        for way in (0, 1):
            copies.arrived(slots.at[way, 3], send.at[way, 0], recv.at[way, 0], zdirs[way])
            result = result + slots[way, 3].astype(F32)
        return result

    def q_pair(k):
        there = wrap(z + k, NZ)
        copies.arrived(px.at[there], ps.at[k], pr.at[k], partner)
        qs[there] = (qp[there * 2 + c].astype(F32) + px[there].astype(F32)).astype(BF16)

    def q_step(d):
        ring_step(d, qs, zbuf, zs, zr, 192)

    def q_done():
        grad = ring_last(qs, zbuf, zs, zr)
        wide = qlow[...].astype(F32)
        scale = lax.rsqrt(jnp.mean(wide * wide, axis=-1, keepdims=True) + NORM_FLOOR)
        inner = jnp.mean(wide * grad, axis=-1, keepdims=True)
        xq[x] = (scale * grad - (scale * scale * scale * inner) * wide).astype(BF16)
        for way in (0, 1):
            for h in (0, 1):
                piece = xq.at[x, pl.ds(h * 192, 192), :]
                copies.start(piece, piece, qxs.at[way, h], qxr.at[way, h], xdirs[way])

    def gates():
        gate = gown[0:6, 0:64]
        dots = own[0:6, 64:128] / own[0:6, 0:64]
        ggx[x] = jnp.zeros((8, 128), F32)
        ggx[x, 0:6, 0:64] = (1.0 - gate) * (dots - gate * md[0:6, :])
        for step, peer in enumerate((front, across, back)):
            copies.start(ggx.at[x], ggx.at[x], gs.at[step], gr.at[step], peer)

    def q_take():
        for way in (0, 1):
            owner = wrap(x - 1 + 2 * way, NX)
            for h in (0, 1):
                piece = xq.at[owner, pl.ds(h * 192, 192), :]
                copies.arrived(piece, qxs.at[way, h], qxr.at[way, h], xdirs[way])
                if h == way:
                    copies.start(piece, piece, qxs.at[way, 2], qxr.at[way, 2], xdirs[way])

    def q_last():
        owner = wrap(x + 2, NX)
        for way in (0, 1):
            copies.arrived(xq.at[owner, pl.ds(way * 192, 192), :], qxs.at[way, 2], qxr.at[way, 2], xdirs[way])
        for step, peer in enumerate((front, across, back)):
            copies.arrived(ggx.at[wrap(x - 1 - step, NX)], gs.at[step], gr.at[step], peer)
        blank = [jnp.zeros((4, 64), F32)]
        slope = jnp.concatenate(
            [gall[h, 0:1, :].astype(F32) for h in range(NX)] + [jnp.zeros((4, 512), F32)], axis=0
        )
        for b in range(6):
            at = pl.ds(b * 64, 64)
            rows = jnp.concatenate([ggx[h, b : b + 1, 0:64] for h in range(NX)] + blank, axis=0)
            term = lax.dot_general(
                rows, slope, CONTRACT_FIRST, preferred_element_type=F32, precision=lax.Precision.HIGHEST
            )
            for h in range(NX):
                term += lax.dot_general(xq[h, at, :], wall[2, h], CONTRACT_LAST, preferred_element_type=F32)
            tgrad[at, :] = term.astype(BF16)

    keep = pl.ds(pl.multiple_of(c * 128, 128), 128)
    give = pl.ds(pl.multiple_of((1 - c) * 128, 128), 128)

    def w_tile(k):
        there = wrap(z + k, NZ)
        at = pl.ds(pl.multiple_of(there * 256, 256), 256)
        wsum[there] = lax.dot_general(
            pas[:, at], xall[x, 0], CONTRACT_FIRST, preferred_element_type=F32
        )
        whalf[there] = wsum[there, :, give]
        copies.start(whalf.at[there], wget.at[there], us.at[k], ur.at[k], partner)

    def w_pair(k):
        there = wrap(z + k, NZ)
        copies.arrived(wget.at[there], us.at[k], ur.at[k], partner)
        wz[there] = (wsum[there, :, keep] + wget[there]).astype(BF16)

    def w_step(d):
        ring_step(d, wz, wbuf, vs, vr, 128)

    def w_done():
        wsum[z, :, 0:128] = ring_last(wz, wbuf, vs, vr)
        for step, peer in enumerate(plane):
            other = wrap(spot + step + 1, 8)
            piece = wsum.at[z, pl.ds(pl.multiple_of(other * 32, 32), 32), pl.ds(0, 128)]
            copies.start(piece, wlast.at[spot], ls.at[step], lr.at[step], peer)
        wlast[spot] = wsum[z, pl.ds(pl.multiple_of(spot * 32, 32), 32), 0:128]

    def w_last():
        for step, peer in enumerate(plane):
            copies.arrived(wlast.at[wrap(spot - step - 1, 8)], ls.at[step], lr.at[step], peer)
        for k in (0, 1):
            wgrad[:, k * 128 : k * 128 + 128] = wlast[k] + wlast[2 + k] + wlast[4 + k] + wlast[6 + k]

    y_open(0)
    q_pair(4)
    q_step(4)
    for k in (3, 5):
        q_pair(k)
    y_add(0)
    q_step(3)
    for k in (2, 6, 1, 7, 0):
        q_pair(k)
    gates()
    y_done(0)
    q_step(2)
    y_add(1)
    q_step(1)
    x_take(0)
    y_done(1)
    for k in (4, 3, 5):
        w_tile(k)
    y_add(2)
    q_done()
    for k in (2, 6, 1, 7, 0):
        w_tile(k)
    x_take(1)
    y_done(2)
    w_pair(4)
    w_step(4)
    y_add(3)
    x_last(0)
    w_pair(3)
    w_pair(5)
    w_step(3)
    q_take()
    for k in (2, 6, 1, 7, 0):
        w_pair(k)
    w_step(2)
    x_take(2)
    x_last(1)
    y_done(3)
    w_step(1)
    q_last()
    w_done()
    x_take(3)
    x_last(2)
    w_last()
    x_last(3)
    copies.finish()


def shaped(shape, dtype):
    return jax.ShapeDtypeStruct(shape, dtype)


def dma(*shape):
    return pltpu.SemaphoreType.DMA(shape)


def call(kernel, outs, scratch, collective, smem=0, limit=48, count=0, space=VMEM, **extra):
    in_specs = [pl.BlockSpec(memory_space=pltpu.SMEM)] * smem + [pl.BlockSpec(memory_space=space)] * (count - smem)
    params = dict(vmem_limit_bytes=limit * 2**20)
    if collective is not None:
        params.update(collective_id=collective, has_side_effects=True)
    return pl.pallas_call(
        kernel,
        out_shape=outs,
        in_specs=in_specs,
        out_specs=[pl.BlockSpec(memory_space=VMEM)] * len(outs),
        scratch_shapes=scratch,
        compiler_params=pltpu.CompilerParams(**params),
        **extra,
    )


def body(
    tokens, cotangent, mix_query, mix_key, mix_value, beta_pre, decay_pre, decay_rate,
    passages, passage_ids, query_weight, key_weight, value_weight, gate_weight,
):
    pass_local, span_rows, model_width = passages.shape
    flat_rows = passages.reshape(pass_local * span_rows, model_width)
    kv, qa, ca, tl, lookup, key_low, query_low, gown, wall, gall, md = call(
        gather_kernel,
        [
            shaped((NY, 1024, 512), BF16), shaped((16, 384, 256), BF16), shaped((16, 384, 256), BF16),
            shaped((16, 8, 128), F32), shaped((16, 1, 128), jnp.int32), shaped((1024, 256), BF16), shaped((384, 256), BF16), shaped((8, 128), F32),
            shaped((3, NX, 512, 256), BF16), shaped((NX, 16, 512), BF16), shaped((8, 64), F32),
        ],
        [
            VMEM((1024, 2048), BF16), VMEM((2048, 256), BF16), VMEM((2048, 256), BF16), VMEM((2048, 256), BF16),
            VMEM((384, 256), BF16), VMEM((384, 256), BF16), VMEM((384, 256), BF16), VMEM((1, 2048), BF16),
            VMEM((6, 4), jnp.int32), VMEM((2, 384), F32), VMEM((2, 384), F32), VMEM((1, 2), F32),
            VMEM((16, 2048), BF16), VMEM((24, 128), F32),
            VMEM((NX, 384, 512), BF16), VMEM((3, 256, 256), BF16), VMEM((6, 128, 128), F32),
            VMEM((6, 128, 128), BF16), VMEM((6, 128, 128), BF16), VMEM((6, 128, 128), BF16), VMEM((6, 128, 128), BF16),
            dma(17), dma(15), dma(15), dma(2, 3), dma(2, 3), dma(2, 6), dma(2, 6), dma(2, 2, 7), dma(2, 2, 7),
            dma(2, 16), dma(2, 16), dma(15), dma(15), dma(12), dma(12), dma(9), dma(9), dma(3), dma(3),
        ],
        1, count=14, limit=LIMITS[0], space=pltpu.HBM,
    )(*[pltpu.with_memory_space_constraint(a, pltpu.HBM) for a in (
        flat_rows, key_weight, value_weight, tokens, query_weight, gate_weight, cotangent,
        mix_query, mix_key, mix_value, passage_ids, beta_pre, decay_pre, decay_rate[None, :],
    )])
    kv_one, qa_one, ca_one = kv.reshape(64, 64, 512), qa.reshape(96, 64, 256), ca.reshape(96, 64, 256)
    eg, tot, own = call(
        score_kernel,
        [shaped((64, 64, 128), F32), shaped((16, 8, 128), F32), shaped((8, 128), F32)],
        [
            VMEM((16, 8, 128), F32), VMEM((15, 8, 128), F32), VMEM((8, 128), F32),
            dma(15), dma(15), dma(15), dma(15),
        ],
        2, smem=1, count=5, limit=LIMITS[1],
    )(lookup, kv_one, qa_one, ca_one, tl)
    kvg, qp = call(
        grads_kernel,
        [shaped((2, 64, 64, 256), BF16), shaped((96, 64, 256), BF16)],
        [VMEM((2, 64, 64, 256), F32), VMEM((96, 64, 256), F32)],
        None, smem=1, count=7, limit=LIMITS[2],
    )(lookup, kv_one, qa_one, ca_one, tl, eg, tot)
    token_grad, passage_grad, key_weight_grad = call(
        finish_kernel,
        [shaped((384, 512), BF16), shaped((1024, 512), BF16), shaped((32, 256), F32)],
        [
            VMEM((2, 4, 256, 256), BF16), VMEM((2, 2, 1024, 256), BF16), VMEM((NZ, 384, 256), BF16),
            VMEM((NZ, 384, 256), BF16), VMEM((2, 4, 384, 256), BF16), VMEM((NX, 2, 1024, 256), BF16),
            VMEM((1024, 512), F32), VMEM((NX, 384, 256), BF16), VMEM((NX, 8, 128), F32),
            VMEM((NZ, 256, 128), F32), VMEM((NZ, 256, 128), F32), VMEM((NZ, 256, 128), BF16),
            VMEM((2, 4, 256, 128), BF16), VMEM((NZ, 256, 256), F32), VMEM((8, 32, 128), F32),
            dma(3, 2, 4), dma(3, 2, 4), dma(2, 4), dma(2, 4), dma(8), dma(8), dma(4, 2, 3), dma(4, 2, 3),
            dma(2, 3), dma(2, 3), dma(3), dma(3), dma(8), dma(8), dma(2, 4), dma(2, 4), dma(7), dma(7),
        ],
        3, count=10, limit=LIMITS[3],
    )(
        kvg.reshape(2, NY, 1024, 256), qp.reshape(16, 384, 256), key_low, flat_rows, query_low,
        wall, gall, own, md, gown,
    )
    return (token_grad, passage_grad.reshape(pass_local, span_rows, 512), key_weight_grad)


def solution(mesh):
    torus = Mesh(mesh.devices.reshape(8, 4, 2, mesh.shape["tp"]), ("st_0", "st_1", "st_2", "tp"))
    return jax.shard_map(
        body,
        mesh=torus,
        in_specs=(
            P(ST, "tp"),
            P(ST, "tp"),
            P(ST, "tp"),
            P(ST, "tp"),
            P(ST, "tp"),
            P("tp", ST),
            P("tp", ST),
            P("tp"),
            P(ST, None, None),
            P(ST, None),
            P(None, "tp"),
            P(None, "tp"),
            P(None, "tp"),
            P("tp", None),
        ),
        out_specs=(P(ST, "tp"), P(ST, None, "tp"), P(ST, "tp")),
        check_vma=False,
    )
```

```python
import functools

import jax
import jax.numpy as jnp
from jax import lax
from jax.experimental import pallas as pl
from jax.experimental.pallas import tpu as pltpu
from jax.sharding import Mesh
from jax.sharding import PartitionSpec as P

SPAN = 64
ST = ("st_0", "st_1", "st_2")
MESH = pl.DeviceIdType.MESH
NZ, NY, NX = 8, 4, 4
VMEM = pltpu.VMEM
F32, BF16 = jnp.float32, jnp.bfloat16
LIMITS = (22, 18, 24)

NORM_FLOOR = 1.0
SCORE_GAIN = 4.0
CONTRACT_LAST = (((1,), (1,)), ((), ()))
CONTRACT_FIRST = (((0,), (0,)), ((), ()))


def place():
    return (lax.axis_index("st_0"), lax.axis_index("st_1"), lax.axis_index("st_2"), lax.axis_index("tp"))


def wrap(value, size):
    return lax.rem(value + size, size)


class Copies:
    def __init__(self):
        self.started = []

    def make(self, src, dst, send, recv, where):
        return pltpu.make_async_remote_copy(
            src_ref=src, dst_ref=dst, send_sem=send, recv_sem=recv, device_id=where, device_id_type=MESH
        )

    def start(self, src, dst, send, recv, where):
        copy = self.make(src, dst, send, recv, where)
        copy.start()
        self.started.append(copy)

    def arrived(self, dst, send, recv, where):
        self.make(dst, dst, send, recv, where).wait_recv()

    def finish(self):
        for copy in self.started:
            copy.wait_send()


def greet(peers):
    barrier = pltpu.get_barrier_semaphore()
    for peer in peers:
        pl.semaphore_signal(barrier, inc=1, device_id=peer, device_id_type=MESH)
    pl.semaphore_wait(barrier, len(peers))


def column_peers(z, c):
    me = z * 2 + c
    peers = []
    for step in range(1, 2 * NZ):
        other = wrap(me + step, 2 * NZ)
        peers.append({"st_0": other // 2, "st_2": lax.rem(other, 2)})
    return peers


def columns_of(rows):
    return jnp.transpose(rows)


def mixer_rows(mx):
    strength = jax.nn.sigmoid(mx[0:8])
    pre = mx[8:16]
    log_decay = -mx[16:17] * (jnp.maximum(pre, 0.0) + jnp.log1p(jnp.exp(-jnp.abs(pre))))
    lane = lax.broadcasted_iota(jnp.int32, (8, 128), 1)
    inner = lax.rem(lane, SPAN)
    total = log_decay
    for shift in (1, 2, 4, 8, 16, 32):
        total = total + jnp.where(inner >= shift, pltpu.roll(total, shift, axis=1), 0.0)
    ends = [
        jnp.sum(jnp.where(lane == at, total, 0.0), axis=1, keepdims=True) for at in (SPAN - 1, 2 * SPAN - 1)
    ]
    last = jnp.where(lane < SPAN, ends[0], ends[1])
    grown = jnp.exp(total)
    stacked = jnp.concatenate([strength, total, strength * grown, grown, jnp.exp(last - total)], axis=0)
    return total, ends, stacked


def low_dot(a, b, dims=(((1,), (0,)), ((), ()))):
    return lax.dot_general(a.astype(BF16), b.astype(BF16), dims, preferred_element_type=F32)


def mixer_prepare(b, mq, mk, mv, total, cols, fresh, corr, att, qdec, kdec):
    at = slice(b * SPAN, (b + 1) * SPAN)

    def both(ref):
        return jnp.concatenate([ref[at, 0:128], ref[at, 128:256]], axis=0).astype(F32)

    def unit(value):
        return value * lax.rsqrt(jnp.sum(value * value, axis=-1, keepdims=True) + NORM_FLOOR)

    def column(k):
        return cols[:, k * 8 + b : k * 8 + b + 1]

    queries, keys, values = unit(both(mq)) * 128 ** (-0.5), unit(both(mk)), both(mv)
    row, col = lax.broadcasted_iota(jnp.int32, (128, 128), 0), lax.broadcasted_iota(jnp.int32, (128, 128), 1)
    same = (row // SPAN) == (col // SPAN)
    spread = jnp.where(same & (row >= col), column(1) - total[b : b + 1, :], -1e30)
    decay = jnp.exp(spread)
    strict = jnp.where(same & (row > col), column(0) * low_dot(keys, keys, CONTRACT_LAST) * decay, 0.0)
    inverse = jnp.where(row == col, 1.0, 0.0) - strict
    power = strict
    for _ in range(SPAN.bit_length() - 2):
        power = low_dot(power, power)
        inverse = inverse + low_dot(inverse, power)
    fresh[b] = low_dot(inverse, values * column(0))
    corr[b] = low_dot(inverse, keys * column(2)).astype(BF16)
    att[b] = (low_dot(queries, keys, CONTRACT_LAST) * decay).astype(BF16)
    qdec[b] = (queries * column(3)).astype(BF16)
    kdec[b] = (keys * column(4)).astype(BF16)


def mixer_advance(b, state, grads, ends, fresh, corr, att, qdec, kdec, sums):
    heads = [slice(0, 64), slice(64, 128)]
    new = jnp.concatenate(
        [fresh[b, h, :] - low_dot(corr[b, h, :], state[i]) for i, h in enumerate(heads)], axis=0
    )
    out = jnp.concatenate([low_dot(qdec[b, h, :], state[i]) for i, h in enumerate(heads)], axis=0)
    out = out + low_dot(att[b], new)
    state = [
        jnp.exp(ends[i][b : b + 1, :]) * state[i] + low_dot(kdec[b, h, :], new[h], CONTRACT_FIRST)
        for i, h in enumerate(heads)
    ]
    grads = jnp.concatenate([grads[:, 0:128], grads[:, 128:256]], axis=0).astype(F32)
    lane = lax.broadcasted_iota(jnp.int32, (128, 128), 1)
    sums = jnp.where(lane == b, jnp.sum(grads * out, axis=-1, keepdims=True), sums)
    return state, sums


def gather_kernel(
    pas_in, wk_in, wv_in, tok_in, wq_in, gw_in, cot_in, mq_in, mk_in, mv_in, ids_in, beta_in, pre_in, rate_in,
    kv, qa, ca, tl, tb, klow, qlow, gown, wall, gall, md, eg, tot, own,
    tbs, sent, parts, total, ss, sr, bs, br,
    pas, wk, wv, wq, mq, mk, mv, gw_row, ids, beta, pre, rate, gw, mx,
    toks, relay, fresh, corr, att, qdec, kdec,
    ins, hs, hr, xs, xr, ys, yr, zs, zr, ps, pr, ts, tr, ws, wr, vs, vr, gs, gr,
):
    z, y, c, x = place()
    me = z * 2 + c
    up, down = {"st_0": wrap(z + 1, NZ)}, {"st_0": wrap(z - 1, NZ)}
    east, west = {"st_1": wrap(y + 1, NY)}, {"st_1": wrap(y - 1, NY)}
    front, back = {"tp": wrap(x + 1, NX)}, {"tp": wrap(x - 1, NX)}
    partner = {"st_2": 1 - c}
    peers = column_peers(z, c)
    across = {"tp": wrap(x + 2, NX)}
    reads = {}

    def fetch(name, src, dst):
        reads[name] = pltpu.make_async_copy(src, dst, ins.at[len(reads)])
        reads[name].start()

    fetch("tok", tok_in, toks.at[x])
    fetch("cot", cot_in, ca.at[pl.ds(me * 6, 6)])
    fetch("wk", wk_in, wk)
    fetch("wv", wv_in, wv)
    for i in range(4):
        fetch(f"pas{i}", pas_in.at[pl.ds(i * 256, 256), :], pas.at[pl.ds(i * 256, 256), :])
    fetch("wq", wq_in, wq)
    for name, src, dst in (
        ("gw", gw_in, gw_row), ("ids", ids_in, ids), ("beta", beta_in, beta), ("pre", pre_in, pre),
        ("rate", rate_in, rate), ("mq", mq_in, mq), ("mk", mk_in, mk), ("mv", mv_in, mv),
    ):
        fetch(name, src, dst)
    greet(peers + [east, west, front, back, across])
    copies = Copies()
    half = 192
    zdirs, ydirs, xdirs = (up, down), (east, west), (front, back)

    def token_rows(slot, h):
        return toks.at[slot, pl.ds(h * half, half), :]

    def rows_of(ref, slot, h):
        return ref.at[pl.ds(slot * 6 + h * 3, 3)]

    def z_send(k, ref, d, h):
        for way in (0, 1):
            if d == 4 and h != way:
                continue
            owner = wrap(z - (d - 1), NZ) if way == 0 else wrap(z + (d - 1), NZ)
            piece = rows_of(ref, owner * 2 + c, h)
            at = (d - 1) * 2 + h if d < 4 else 6
            copies.start(piece, piece, zs.at[k, way, at], zr.at[k, way, at], zdirs[way])

    def z_take(k, ref, d):
        for h in (0, 1):
            for way in (0, 1):
                if d == 4 and h != way:
                    continue
                owner = wrap(z - d, NZ) if way == 0 else wrap(z + d, NZ)
                piece = rows_of(ref, owner * 2 + c, h)
                at = (d - 1) * 2 + h if d < 4 else 6
                copies.arrived(piece, zs.at[k, way, at], zr.at[k, way, at], zdirs[way])
                if d < 3 or (d == 3 and h == way):
                    nxt = d * 2 + h if d < 3 else 6
                    copies.start(piece, piece, zs.at[k, way, nxt], zr.at[k, way, nxt], zdirs[way])
                to = 2 + way * 7 + at
                copies.start(piece, piece, ps.at[k, to], pr.at[k, to], partner)

    def own_send(k, ref):
        for h in (0, 1):
            z_send(k, ref, 1, h)
        for h in (0, 1):
            piece = rows_of(ref, me, h)
            copies.start(piece, piece, ps.at[k, h], pr.at[k, h], partner)

    def partner_take(k, ref):
        theirs = 1 - c
        for h in (0, 1):
            piece = rows_of(ref, z * 2 + theirs, h)
            copies.arrived(piece, ps.at[k, h], pr.at[k, h], partner)
        for d in (1, 2, 3, 4):
            for h in (0, 1):
                for way in (0, 1):
                    if d == 4 and h != way:
                        continue
                    owner = wrap(z - d, NZ) if way == 0 else wrap(z + d, NZ)
                    to = 2 + way * 7 + ((d - 1) * 2 + h if d < 4 else 6)
                    piece = rows_of(ref, owner * 2 + theirs, h)
                    copies.arrived(piece, ps.at[k, to], pr.at[k, to], partner)

    reads["tok"].wait()
    for way, h in ((0, 0), (1, 1), (0, 1), (1, 0)):
        piece = token_rows(x, h)
        copies.start(piece, piece, xs.at[way, h], xr.at[way, h], xdirs[way])
    reads["cot"].wait()
    own_send(0, ca)

    rows = 256

    def kv_rows(i):
        return kv.at[pl.ds(y * 16 + i * 4, 4)]

    reads["wk"].wait()
    reads["wv"].wait()
    for i in range(4):
        reads[f"pas{i}"].wait()
        block = pas[pl.ds(i * rows, rows), :]
        low = jnp.dot(block, wk[...], preferred_element_type=F32).astype(BF16)
        wide = low.astype(F32)
        scale = lax.rsqrt(jnp.mean(wide * wide, axis=-1, keepdims=True) + NORM_FLOOR)
        klow[pl.ds(i * rows, rows), :] = low
        kv[pl.ds(y * 16 + i * 4, 4), :, 0:256] = (wide * scale).astype(BF16).reshape(4, 64, 256)
        value = jnp.dot(block, wv[...], preferred_element_type=F32)
        kv[pl.ds(y * 16 + i * 4, 4), :, 256:512] = value.astype(BF16).reshape(4, 64, 256)
        for way in (0, 1):
            copies.start(kv_rows(i), kv_rows(i), ys.at[way, i], yr.at[way, i], ydirs[way])

    def y_take(i):
        for way in (0, 1):
            owner = wrap(y - 1, NY) if way == 0 else wrap(y + 1, NY)
            piece = kv.at[pl.ds(owner * 16 + i * 4, 4)]
            copies.arrived(piece, ys.at[way, i], yr.at[way, i], ydirs[way])
            if i % 2 == way:
                at = 4 + i // 2
                copies.start(piece, piece, ys.at[way, at], yr.at[way, at], ydirs[way])

    def y_last():
        owner = wrap(y + 2, NY)
        for i in range(4):
            way, at = i % 2, 4 + i // 2
            piece = kv.at[pl.ds(owner * 16 + i * 4, 4)]
            copies.arrived(piece, ys.at[way, at], yr.at[way, at], ydirs[way])

    def x_take(first):
        for way in (0, 1):
            owner = wrap(x - 1, NX) if way == 0 else wrap(x + 1, NX)
            h = way if first else 1 - way
            piece = token_rows(owner, h)
            copies.arrived(piece, xs.at[way, h], xr.at[way, h], xdirs[way])
            if first:
                copies.start(piece, piece, xs.at[way, 2], xr.at[way, 2], xdirs[way])

    def x_last():
        owner = wrap(x + 2, NX)
        for way in (0, 1):
            piece = token_rows(owner, way)
            copies.arrived(piece, xs.at[way, 2], xr.at[way, 2], xdirs[way])

    def project(owner):
        block = toks[owner]
        at = pl.ds(pl.multiple_of(owner * 512, 512), 512)
        return (
            jnp.dot(block, wq[at, :], preferred_element_type=F32),
            lax.dot_general(gw[:, at], block, CONTRACT_LAST, preferred_element_type=F32),
        )

    weights = (wk, wv, wq)
    via, behind = {"tp": wrap(x + 1 - 2 * c, NX)}, wrap(x - 1 + 2 * c, NX)

    def w_rows(owner):
        return pl.ds(pl.multiple_of(owner * 512 + c * 256, 256), 256)

    mine = pl.ds(pl.multiple_of(c * 256, 256), 256)

    def w_send():
        for i, ref in enumerate(weights):
            copies.start(ref.at[w_rows(wrap(x + 2, NX)), :], relay.at[i], ws.at[6 + i], wr.at[6 + i], via)
        for way in (0, 1):
            to = wrap(x + 1 - 2 * way, NX)
            for i, ref in enumerate(weights):
                copies.start(
                    ref.at[w_rows(to), :], wall.at[i, x, mine, :], ws.at[way * 3 + i], wr.at[way * 3 + i], xdirs[way]
                )
        for step, peer in enumerate((front, across, back)):
            at = pl.ds(pl.multiple_of(wrap(x + 1 + step, NX) * 512, 512), 512)
            copies.start(gw.at[:, at], gall.at[x], gs.at[step], gr.at[step], peer)
        own = pl.ds(pl.multiple_of(x * 512, 512), 512)
        for i, ref in enumerate(weights):
            wall[i, x] = ref[own, :]
        gall[x] = gw[:, own]

    def w_forward():
        for i in range(3):
            copies.arrived(relay.at[i], ws.at[6 + i], wr.at[6 + i], via)
            copies.start(relay.at[i], wall.at[i, behind, mine, :], ws.at[9 + i], wr.at[9 + i], via)

    def w_share(n, owner, first):
        for i in range(3):
            piece = wall.at[i, owner, mine, :]
            copies.arrived(piece, ws.at[first + i], wr.at[first + i], via)
            copies.start(piece, piece, vs.at[n * 3 + i], vr.at[n * 3 + i], partner)

    def w_last():
        theirs = pl.ds(pl.multiple_of((1 - c) * 256, 256), 256)
        for n, owner in enumerate((wrap(x - 1, NX), wrap(x + 1, NX), wrap(x + 2, NX))):
            for i in range(3):
                copies.arrived(wall.at[i, owner, theirs, :], vs.at[n * 3 + i], vr.at[n * 3 + i], partner)
        for step, peer in enumerate((front, across, back)):
            copies.arrived(gall.at[wrap(x - 1 - step, NX)], gs.at[step], gr.at[step], peer)

    for name in ("wq", "gw", "ids", "beta", "pre", "rate", "mq", "mk", "mv"):
        reads[name].wait()
    gw[...] = jnp.broadcast_to(gw_row[...].astype(F32), (16, 2048)).astype(BF16)
    lanes = lax.broadcasted_iota(jnp.int32, (1, 128), 1)
    row = jnp.full((1, 128), -1, jnp.int32)
    for b in range(6):
        for p in range(4):
            each = jnp.broadcast_to(ids[p : p + 1, b : b + 1], (1, 128))
            row = jnp.where(lanes == each // 16, (b * 4 + p) * 16 + lax.rem(each, 16), row)
    tb[me] = row
    for step, peer in enumerate(peers):
        copies.start(tb.at[me], tb.at[me], hs.at[step], hr.at[step], peer)
    mx[...] = jnp.zeros((24, 128), F32)
    for b in range(6):
        for h in range(2):
            mx[b : b + 1, h * 64 : h * 64 + 64] = beta[h : h + 1, b * 64 : b * 64 + 64]
            mx[8 + b : 9 + b, h * 64 : h * 64 + 64] = pre[h : h + 1, b * 64 : b * 64 + 64]
    for h in range(2):
        mx[16:17, h * 64 : h * 64 + 64] = jnp.broadcast_to(rate[0:1, h : h + 1], (1, 64))
    decays, ends, stacked = mixer_rows(mx[...])
    cols = columns_of(stacked)
    work = (fresh, corr, att, qdec, kdec)

    def prepare(b):
        mixer_prepare(b, mq, mk, mv, decays, cols, *work)

    z_take(0, ca, 1)
    x_take(True)
    w_send()
    acc = project(x)
    prepare(0)
    y_take(0)
    z_take(0, ca, 2)
    x_take(False)
    for owner in (wrap(x - 1, NX), wrap(x + 1, NX)):
        more = project(owner)
        acc = (acc[0] + more[0], acc[1] + more[1])
    prepare(1)
    x_last()
    more = project(wrap(x + 2, NX))
    low = (acc[0] + more[0]).astype(BF16)
    gate = jax.nn.sigmoid(acc[1] + more[1])
    wide = low.astype(F32)
    scale = lax.rsqrt(jnp.mean(wide * wide, axis=-1, keepdims=True) + NORM_FLOOR)
    qlow[...] = low
    qa[pl.ds(me * 6, 6)] = (wide * scale).astype(BF16).reshape(6, 64, 256)
    own_send(1, qa)
    z_take(0, ca, 3)
    y_take(1)
    tl[me] = jnp.zeros((8, 128), F32)
    for b in range(6):
        tl[me, b : b + 1, 0:64] = gate[0:1, b * 64 : b * 64 + 64]
    gown[...] = tl[me]
    y_take(2)
    prepare(2)
    z_take(1, qa, 1)
    z_take(0, ca, 4)
    prepare(3)
    w_forward()
    y_take(3)
    z_take(1, qa, 2)
    for step, peer in enumerate(peers):
        copies.start(tl.at[me], tl.at[me], ts.at[step], tr.at[step], peer)
    w_share(0, wrap(x - 1, NX), 0)
    w_share(1, wrap(x + 1, NX), 3)
    prepare(4)
    z_take(1, qa, 3)
    w_share(2, wrap(x + 2, NX), 9)
    prepare(5)
    state = [jnp.zeros((128, 128), F32), jnp.zeros((128, 128), F32)]
    sums = jnp.zeros((128, 128), F32)
    for b in range(6):
        state, sums = mixer_advance(b, state, ca[me * 6 + b], ends, *work, sums)
    turned = jnp.transpose(sums)[0:8]
    md[...] = turned[:, 0:64] + turned[:, 64:128]
    w_last()
    z_take(1, qa, 4)
    for step in range(2 * NZ - 1):
        other = wrap(me - (step + 1), 2 * NZ)
        copies.arrived(tl.at[other], ts.at[step], tr.at[step], peers[step])
        copies.arrived(tb.at[other], hs.at[step], hr.at[step], peers[step])
    table = pltpu.make_async_copy(tb, tbs, ins.at[17])
    table.start()
    partner_take(0, ca)
    partner_take(1, qa)
    y_last()
    table.wait()

    gain = SCORE_GAIN * 256 ** (-0.5)
    line = lax.broadcasted_iota(jnp.int32, (8, 128), 0)

    def reader(r):
        tile = tl[r]
        stats = jnp.zeros((8, 128), F32)
        for yy in range(NY):
            entry = tbs[r, 0, (z * NY + yy) * 2 + c]
            used = entry >= 0
            safe = jnp.maximum(entry, 0)
            b, loc = safe // 64, lax.rem(safe, 16)
            keys_values = kv[yy * 16 + loc]
            scores = gain * lax.dot_general(
                keys_values[:, 0:256], qa[r * 6 + b], CONTRACT_LAST, preferred_element_type=F32
            )
            here = (line == b) & used
            gate = jnp.sum(jnp.where(line == b, tile, 0.0), axis=0, keepdims=True)
            grads = gate[:, 0:64] * lax.dot_general(
                keys_values[:, 256:512], ca[r * 6 + b], CONTRACT_LAST, preferred_element_type=F32
            )
            exps = jnp.exp(scores)
            both = jnp.concatenate([exps, grads], axis=1)
            eg[r * NY + yy] = both
            row = jnp.concatenate(
                [jnp.sum(exps, axis=0, keepdims=True), jnp.sum(exps * grads, axis=0, keepdims=True)], axis=1
            )
            stats = stats + jnp.where(here, row, 0.0)
        sent[r] = stats

    def outward(i, carry):
        near = (i + 1) // 2
        step = NZ + near - 2 * near * lax.rem(i, 2) - 1
        r = wrap(me + step + 1, 2 * NZ)
        reader(r)
        copies.make(
            sent.at[r], parts.at[step], ss.at[step], sr.at[step], {"st_0": r // 2, "st_2": lax.rem(r, 2)}
        ).start()
        return carry

    lax.fori_loop(0, 2 * NZ - 1, outward, 0)
    reader(me)
    whole = sent[me]
    for step in range(2 * NZ - 1):
        copies.arrived(parts.at[step], ss.at[step], sr.at[step], peers[step])
        whole = whole + parts[step]
    total[...] = whole
    tot[me] = whole
    own[...] = whole
    for step, peer in enumerate(peers):
        copies.start(total, tot.at[me], bs.at[step], br.at[step], peer)
    for step in range(2 * NZ - 1):
        other = wrap(me - (step + 1), 2 * NZ)
        copies.arrived(tot.at[other], bs.at[step], br.at[step], peers[step])
        copies.make(sent.at[0], parts.at[step], ss.at[step], sr.at[step], peers[step]).wait_send()
    copies.finish()


def grads_kernel(tb, kv, qa, ca, tl, eg, tot, kvg, qp, kacc, qacc):
    z, c = lax.axis_index("st_0"), lax.axis_index("st_2")
    gain = SCORE_GAIN * 256 ** (-0.5)
    kacc[...] = jnp.zeros(kacc.shape, F32)
    qacc[...] = jnp.zeros(qacc.shape, F32)

    @pl.loop(0, 2 * NZ)
    def _(r):
        for yy in range(NY):
            entry = tb[r, 0, (z * NY + yy) * 2 + c]

            @pl.when(entry >= 0)
            def _():
                b, loc = entry // 64, lax.rem(entry, 16)
                row = tot[r, pl.ds(b, 1), :]
                gate = tl[r, pl.ds(b, 1), 0:64]
                norm = 1.0 / row[:, 0:64]
                both = eg[r * NY + yy]
                probs = both[:, 0:64] * norm
                slope = (probs * (both[:, 64:128] - row[:, 64:128] * norm)).astype(BF16)
                gated = (probs * gate).astype(BF16)
                at, slot = r * 6 + b, yy * 16 + loc
                key = gain * jnp.dot(slope, qa[at], preferred_element_type=F32)
                value = jnp.dot(gated, ca[at], preferred_element_type=F32)
                kacc[0, slot] += key.astype(BF16).astype(F32)
                kacc[1, slot] += value.astype(BF16).astype(F32)
                qacc[at] += gain * lax.dot_general(
                    slope, kv[slot, :, 0:256], CONTRACT_FIRST, preferred_element_type=F32
                )

    @pl.loop(0, 64)
    def _(i):
        kvg[0, i] = kacc[0, i].astype(BF16)
        kvg[1, i] = kacc[1, i].astype(BF16)

    @pl.loop(0, 96)
    def _(i):
        qp[i] = qacc[i].astype(BF16)


def finish_kernel(
    kvg, qp, klow, pas, qlow, wall, gall, own, md, gown,
    tgrad, pgrad, wgrad,
    ybuf, ysum, px, qs, zbuf, xall, pacc, xq, ggx, whalf, wget, wz, wbuf, wsum, wlast,
    ys, yr, zs, zr, ps, pr, xs, xr, qxs, qxr, gs, gr, us, ur, vs, vr, ls, lr,
):
    z, y, c, x = place()
    up, down = {"st_0": wrap(z + 1, NZ)}, {"st_0": wrap(z - 1, NZ)}
    east, west = {"st_1": wrap(y + 1, NY)}, {"st_1": wrap(y - 1, NY)}
    front, back, across = {"tp": wrap(x + 1, NX)}, {"tp": wrap(x - 1, NX)}, {"tp": wrap(x + 2, NX)}
    partner = {"st_2": 1 - c}
    spot = y * 2 + c
    plane = []
    for step in range(1, 8):
        other = wrap(spot + step, 8)
        plane.append({"st_1": other // 2, "st_2": lax.rem(other, 2)})
    greet([up, down, front, back, across] + plane)
    copies = Copies()
    zdirs, ydirs, xdirs = (up, down), (east, west), (front, back)

    far, beside = wrap(y + 2, NY), (wrap(y + 1, NY), wrap(y - 1, NY))

    def y_rows(j, part):
        return j // 4, pl.ds((j % 4) * 256 + part * 128, 128)

    def y_far(j):
        for way in (0, 1):
            p, at = y_rows(j, way)
            copies.start(kvg.at[p, far, at, :], ybuf.at[way, j], ys.at[0, way, j], yr.at[0, way, j], ydirs[way])

    def y_near(j):
        for way in (0, 1):
            p, at = y_rows(j, 1 - way)
            copies.start(
                kvg.at[p, beside[way], at, :], ysum.at[way, p, at, :], ys.at[1, way, j], yr.at[1, way, j], ydirs[way]
            )

    def y_add(j):
        for way in (0, 1):
            p, at = y_rows(j, way)
            copies.arrived(ybuf.at[way, j], ys.at[0, way, j], yr.at[0, way, j], ydirs[way])
            ybuf[way, j] = (kvg[p, beside[way], at, :].astype(F32) + ybuf[way, j].astype(F32)).astype(BF16)
            copies.start(ybuf.at[way, j], ysum.at[way, p, at, :], ys.at[2, way, j], yr.at[2, way, j], ydirs[way])
        if j + 1 < 8:
            y_near(j + 1)
        if j + 2 < 8:
            y_far(j + 2)

    def x_pieces(j, h):
        return j // 4, pl.ds((j % 4) * 256 + h * 128, 128)

    def y_done(j):
        for way in (0, 1):
            p, at = y_rows(j, 1 - way)
            copies.arrived(ysum.at[way, p, at, :], ys.at[1, way, j], yr.at[1, way, j], ydirs[way])
            p, at = y_rows(j, way)
            copies.arrived(ysum.at[way, p, at, :], ys.at[2, way, j], yr.at[2, way, j], ydirs[way])
        for h in (0, 1):
            p, at = x_pieces(j, h)
            grad = kvg[p, y, at, :].astype(F32) + ysum[0, p, at, :].astype(F32) + ysum[1, p, at, :].astype(F32)
            if p == 0:
                wide = klow[at, :].astype(F32)
                scale = lax.rsqrt(jnp.mean(wide * wide, axis=-1, keepdims=True) + NORM_FLOOR)
                inner = jnp.mean(wide * grad, axis=-1, keepdims=True)
                grad = scale * grad - (scale * scale * scale * inner) * wide
            xall[x, p, at, :] = grad.astype(BF16)
            for way in (0, 1):
                piece = xall.at[x, p, at, :]
                copies.start(piece, piece, xs.at[j, way, h], xr.at[j, way, h], xdirs[way])

    def x_take(j):
        for way in (0, 1):
            owner = wrap(x - 1 + 2 * way, NX)
            for h in (0, 1):
                p, at = x_pieces(j, h)
                piece = xall.at[owner, p, at, :]
                copies.arrived(piece, xs.at[j, way, h], xr.at[j, way, h], xdirs[way])
                if h == way:
                    copies.start(piece, piece, xs.at[j, way, 2], xr.at[j, way, 2], xdirs[way])

    def x_last(j):
        owner = wrap(x + 2, NX)
        for way in (0, 1):
            p, at = x_pieces(j, way)
            copies.arrived(xall.at[owner, p, at, :], xs.at[j, way, 2], xr.at[j, way, 2], xdirs[way])
        p = j // 4

        @pl.loop(0, 2)
        def _(i):
            at = pl.ds(pl.multiple_of((j % 4) * 256 + i * 128, 128), 128)
            term = lax.dot_general(xall[0, p, at, :], wall[p, 0], CONTRACT_LAST, preferred_element_type=F32)
            for h in range(1, NX):
                term += lax.dot_general(xall[h, p, at, :], wall[p, h], CONTRACT_LAST, preferred_element_type=F32)
            if p == 0:
                pacc[at, :] = term
            else:
                pgrad[at, :] = (pacc[at, :] + term).astype(BF16)

    def ring_step(d, value, slots, send, recv, half):
        for way in (0, 1):
            there = wrap(z + d, NZ) if way == 0 else wrap(z - d, NZ)
            at = pl.ds(way * half, half)
            if d == 3:
                copies.arrived(slots.at[way, 0, at, :], send.at[way, 3], recv.at[way, 3], zdirs[way])
                value[there, at, :] = (value[there, at, :].astype(F32) + slots[way, 0, at, :].astype(F32)).astype(BF16)
            elif d < 3:
                copies.arrived(slots.at[way, 3 - d], send.at[way, d], recv.at[way, d], zdirs[way])
                value[there] = (value[there].astype(F32) + slots[way, 3 - d].astype(F32)).astype(BF16)
            if d == 4:
                copies.start(value.at[there, at, :], slots.at[way, 0, at, :], send.at[way, 3], recv.at[way, 3], zdirs[way])
            else:
                copies.start(value.at[there], slots.at[way, 4 - d], send.at[way, d - 1], recv.at[way, d - 1], zdirs[way])

    def ring_last(value, slots, send, recv):
        result = value[z].astype(F32)
        for way in (0, 1):
            copies.arrived(slots.at[way, 3], send.at[way, 0], recv.at[way, 0], zdirs[way])
            result = result + slots[way, 3].astype(F32)
        return result

    def q_pair(k):
        there = wrap(z + k, NZ)
        copies.arrived(px.at[there], ps.at[k], pr.at[k], partner)
        qs[there] = (qp[there * 2 + c].astype(F32) + px[there].astype(F32)).astype(BF16)

    def q_step(d):
        ring_step(d, qs, zbuf, zs, zr, 192)

    def q_done():
        grad = ring_last(qs, zbuf, zs, zr)
        wide = qlow[...].astype(F32)
        scale = lax.rsqrt(jnp.mean(wide * wide, axis=-1, keepdims=True) + NORM_FLOOR)
        inner = jnp.mean(wide * grad, axis=-1, keepdims=True)
        xq[x] = (scale * grad - (scale * scale * scale * inner) * wide).astype(BF16)
        for way in (0, 1):
            for h in (0, 1):
                piece = xq.at[x, pl.ds(h * 192, 192), :]
                copies.start(piece, piece, qxs.at[way, h], qxr.at[way, h], xdirs[way])

    def gates():
        gate = gown[0:6, 0:64]
        dots = own[0:6, 64:128] / own[0:6, 0:64]
        ggx[x] = jnp.zeros((8, 128), F32)
        ggx[x, 0:6, 0:64] = (1.0 - gate) * (dots - gate * md[0:6, :])
        for step, peer in enumerate((front, across, back)):
            copies.start(ggx.at[x], ggx.at[x], gs.at[step], gr.at[step], peer)

    def q_take():
        for way in (0, 1):
            owner = wrap(x - 1 + 2 * way, NX)
            for h in (0, 1):
                piece = xq.at[owner, pl.ds(h * 192, 192), :]
                copies.arrived(piece, qxs.at[way, h], qxr.at[way, h], xdirs[way])
                if h == way:
                    copies.start(piece, piece, qxs.at[way, 2], qxr.at[way, 2], xdirs[way])

    def q_last():
        owner = wrap(x + 2, NX)
        for way in (0, 1):
            copies.arrived(xq.at[owner, pl.ds(way * 192, 192), :], qxs.at[way, 2], qxr.at[way, 2], xdirs[way])
        for step, peer in enumerate((front, across, back)):
            copies.arrived(ggx.at[wrap(x - 1 - step, NX)], gs.at[step], gr.at[step], peer)
        blank = [jnp.zeros((4, 64), F32)]
        slope = jnp.concatenate(
            [gall[h, 0:1, :].astype(F32) for h in range(NX)] + [jnp.zeros((4, 512), F32)], axis=0
        )
        for b in range(6):
            at = pl.ds(b * 64, 64)
            rows = jnp.concatenate([ggx[h, b : b + 1, 0:64] for h in range(NX)] + blank, axis=0)
            term = lax.dot_general(
                rows, slope, CONTRACT_FIRST, preferred_element_type=F32, precision=lax.Precision.HIGHEST
            )
            for h in range(NX):
                term += lax.dot_general(xq[h, at, :], wall[2, h], CONTRACT_LAST, preferred_element_type=F32)
            tgrad[at, :] = term.astype(BF16)

    keep = pl.ds(pl.multiple_of(c * 128, 128), 128)
    give = pl.ds(pl.multiple_of((1 - c) * 128, 128), 128)

    def w_tile(k):
        there = wrap(z + k, NZ)
        at = pl.ds(pl.multiple_of(there * 256, 256), 256)
        wsum[there] = lax.dot_general(
            pas[:, at], xall[x, 0], CONTRACT_FIRST, preferred_element_type=F32
        )
        whalf[there] = wsum[there, :, give]
        copies.start(whalf.at[there], wget.at[there], us.at[k], ur.at[k], partner)

    def w_pair(k):
        there = wrap(z + k, NZ)
        copies.arrived(wget.at[there], us.at[k], ur.at[k], partner)
        wz[there] = (wsum[there, :, keep] + wget[there]).astype(BF16)

    def w_step(d):
        ring_step(d, wz, wbuf, vs, vr, 128)

    def w_done():
        wsum[z, :, 0:128] = ring_last(wz, wbuf, vs, vr)
        for step, peer in enumerate(plane):
            other = wrap(spot + step + 1, 8)
            piece = wsum.at[z, pl.ds(pl.multiple_of(other * 32, 32), 32), pl.ds(0, 128)]
            copies.start(piece, wlast.at[spot], ls.at[step], lr.at[step], peer)
        wlast[spot] = wsum[z, pl.ds(pl.multiple_of(spot * 32, 32), 32), 0:128]

    def w_last():
        for step, peer in enumerate(plane):
            copies.arrived(wlast.at[wrap(spot - step - 1, 8)], ls.at[step], lr.at[step], peer)
        for k in (0, 1):
            wgrad[:, k * 128 : k * 128 + 128] = wlast[k] + wlast[2 + k] + wlast[4 + k] + wlast[6 + k]

    y_far(0)
    y_near(0)
    y_far(1)
    for k in (4, 3, 5, 2, 6, 1, 7, 0):
        there = wrap(z + k, NZ)
        copies.start(qp.at[there * 2 + 1 - c], px.at[there], ps.at[k], pr.at[k], partner)
    q_pair(4)
    q_step(4)
    q_pair(3)
    q_pair(5)
    y_add(0)
    for k in (2, 6, 1, 7, 0):
        q_pair(k)
    gates()
    y_add(1)
    q_step(3)
    y_done(0)
    y_add(2)
    y_done(1)
    q_step(2)
    x_take(0)
    y_add(3)
    y_done(2)
    x_take(1)
    x_last(0)
    y_add(4)
    y_done(3)
    q_step(1)
    for k in (4, 3, 5):
        w_tile(k)
    x_take(2)
    x_last(1)
    y_add(5)
    y_done(4)
    x_take(3)
    for k in (2, 6, 1, 7, 0):
        w_tile(k)
    y_add(6)
    q_done()
    y_done(5)
    w_pair(4)
    w_step(4)
    x_last(2)
    y_add(7)
    y_done(6)
    x_take(4)
    w_pair(3)
    w_pair(5)
    w_step(3)
    y_done(7)
    x_last(3)
    x_take(5)
    for k in (2, 6, 1, 7, 0):
        w_pair(k)
    w_step(2)
    q_take()
    x_last(4)
    x_take(6)
    w_step(1)
    x_last(5)
    x_take(7)
    w_done()
    q_last()
    x_last(6)
    w_last()
    x_last(7)
    copies.finish()


def shaped(shape, dtype):
    return jax.ShapeDtypeStruct(shape, dtype)


def dma(*shape):
    return pltpu.SemaphoreType.DMA(shape)


def call(kernel, outs, scratch, collective, smem=0, limit=48, count=0, space=VMEM, **extra):
    in_specs = [pl.BlockSpec(memory_space=pltpu.SMEM)] * smem + [pl.BlockSpec(memory_space=space)] * (count - smem)
    params = dict(vmem_limit_bytes=limit * 2**20)
    if collective is not None:
        params.update(collective_id=collective, has_side_effects=True)
    return pl.pallas_call(
        kernel,
        out_shape=outs,
        in_specs=in_specs,
        out_specs=[pl.BlockSpec(memory_space=VMEM)] * len(outs),
        scratch_shapes=scratch,
        compiler_params=pltpu.CompilerParams(**params),
        **extra,
    )


def body(
    tokens, cotangent, mix_query, mix_key, mix_value, beta_pre, decay_pre, decay_rate,
    passages, passage_ids, query_weight, key_weight, value_weight, gate_weight,
):
    pass_local, span_rows, model_width = passages.shape
    flat_rows = passages.reshape(pass_local * span_rows, model_width)
    kv, qa, ca, tl, lookup, key_low, query_low, gown, wall, gall, md, eg, tot, own = call(
        gather_kernel,
        [
            shaped((64, 64, 512), BF16), shaped((96, 64, 256), BF16), shaped((96, 64, 256), BF16),
            shaped((16, 8, 128), F32), shaped((16, 1, 128), jnp.int32), shaped((1024, 256), BF16), shaped((384, 256), BF16), shaped((8, 128), F32),
            shaped((3, NX, 512, 256), BF16), shaped((NX, 16, 512), BF16), shaped((8, 64), F32),
            shaped((64, 64, 128), F32), shaped((16, 8, 128), F32), shaped((8, 128), F32),
        ],
        [
            pltpu.SMEM((16, 1, 128), jnp.int32), VMEM((16, 8, 128), F32), VMEM((15, 8, 128), F32), VMEM((8, 128), F32),
            dma(15), dma(15), dma(15), dma(15),
            VMEM((1024, 2048), BF16), VMEM((2048, 256), BF16), VMEM((2048, 256), BF16), VMEM((2048, 256), BF16),
            VMEM((384, 256), BF16), VMEM((384, 256), BF16), VMEM((384, 256), BF16), VMEM((1, 2048), BF16),
            VMEM((4, 6), jnp.int32), VMEM((2, 384), F32), VMEM((2, 384), F32), VMEM((1, 2), F32),
            VMEM((16, 2048), BF16), VMEM((24, 128), F32),
            VMEM((NX, 384, 512), BF16), VMEM((3, 256, 256), BF16), VMEM((6, 128, 128), F32),
            VMEM((6, 128, 128), BF16), VMEM((6, 128, 128), BF16), VMEM((6, 128, 128), BF16), VMEM((6, 128, 128), BF16),
            dma(18), dma(15), dma(15), dma(2, 3), dma(2, 3), dma(2, 6), dma(2, 6), dma(2, 2, 7), dma(2, 2, 7),
            dma(2, 16), dma(2, 16), dma(15), dma(15), dma(12), dma(12), dma(9), dma(9), dma(3), dma(3),
        ],
        1, count=14, limit=LIMITS[0], space=pltpu.HBM,
    )(*[pltpu.with_memory_space_constraint(a, pltpu.HBM) for a in (
        flat_rows, key_weight, value_weight, tokens, query_weight, gate_weight, cotangent.reshape(6, 64, 256),
        mix_query, mix_key, mix_value, passage_ids.T, beta_pre, decay_pre, decay_rate[None, :],
    )])
    kvg, qp = call(
        grads_kernel,
        [shaped((2, 64, 64, 256), BF16), shaped((96, 64, 256), BF16)],
        [VMEM((2, 64, 64, 256), F32), VMEM((96, 64, 256), F32)],
        None, smem=1, count=7, limit=LIMITS[1],
    )(lookup, kv, qa, ca, tl, eg, tot)
    token_grad, passage_grad, key_weight_grad = call(
        finish_kernel,
        [shaped((384, 512), BF16), shaped((1024, 512), BF16), shaped((32, 256), F32)],
        [
            VMEM((2, 8, 128, 256), BF16), VMEM((2, 2, 1024, 256), BF16), VMEM((NZ, 384, 256), BF16),
            VMEM((NZ, 384, 256), BF16), VMEM((2, 4, 384, 256), BF16), VMEM((NX, 2, 1024, 256), BF16),
            VMEM((1024, 512), F32), VMEM((NX, 384, 256), BF16), VMEM((NX, 8, 128), F32),
            VMEM((NZ, 256, 128), F32), VMEM((NZ, 256, 128), F32), VMEM((NZ, 256, 128), BF16),
            VMEM((2, 4, 256, 128), BF16), VMEM((NZ, 256, 256), F32), VMEM((8, 32, 128), F32),
            dma(3, 2, 8), dma(3, 2, 8), dma(2, 4), dma(2, 4), dma(8), dma(8), dma(8, 2, 3), dma(8, 2, 3),
            dma(2, 3), dma(2, 3), dma(3), dma(3), dma(8), dma(8), dma(2, 4), dma(2, 4), dma(7), dma(7),
        ],
        3, count=10, limit=LIMITS[2],
    )(
        kvg.reshape(2, NY, 1024, 256), qp.reshape(16, 384, 256), key_low, flat_rows, query_low,
        wall, gall, own, md, gown,
    )
    return (token_grad, passage_grad.reshape(pass_local, span_rows, 512), key_weight_grad)


def solution(mesh):
    torus = Mesh(mesh.devices.reshape(8, 4, 2, mesh.shape["tp"]), ("st_0", "st_1", "st_2", "tp"))
    return jax.shard_map(
        body,
        mesh=torus,
        in_specs=(
            P(ST, "tp"),
            P(ST, "tp"),
            P(ST, "tp"),
            P(ST, "tp"),
            P(ST, "tp"),
            P("tp", ST),
            P("tp", ST),
            P("tp"),
            P(ST, None, None),
            P(ST, None),
            P(None, "tp"),
            P(None, "tp"),
            P(None, "tp"),
            P("tp", None),
        ),
        out_specs=(P(ST, "tp"), P(ST, None, "tp"), P(ST, "tp")),
        check_vma=False,
    )
```

```python
import functools

import jax
import jax.numpy as jnp
from jax import lax
from jax.experimental import pallas as pl
from jax.experimental.pallas import tpu as pltpu
from jax.sharding import Mesh
from jax.sharding import PartitionSpec as P

SPAN = 64
ST = ("st_0", "st_1", "st_2")
MESH = pl.DeviceIdType.MESH
NZ, NY, NX = 8, 4, 4
VMEM = pltpu.VMEM
F32, BF16 = jnp.float32, jnp.bfloat16
LIMITS = (22, 6, 24)

NORM_FLOOR = 1.0
SCORE_GAIN = 4.0
CONTRACT_LAST = (((1,), (1,)), ((), ()))
CONTRACT_FIRST = (((0,), (0,)), ((), ()))


def place():
    return (lax.axis_index("st_0"), lax.axis_index("st_1"), lax.axis_index("st_2"), lax.axis_index("tp"))


def wrap(value, size):
    return lax.rem(value + size, size)


class Copies:
    def __init__(self):
        self.started = []

    def make(self, src, dst, send, recv, where):
        return pltpu.make_async_remote_copy(
            src_ref=src, dst_ref=dst, send_sem=send, recv_sem=recv, device_id=where, device_id_type=MESH
        )

    def start(self, src, dst, send, recv, where):
        copy = self.make(src, dst, send, recv, where)
        copy.start()
        self.started.append(copy)

    def arrived(self, dst, send, recv, where):
        self.make(dst, dst, send, recv, where).wait_recv()

    def finish(self):
        for copy in self.started:
            copy.wait_send()


def greet(peers):
    barrier = pltpu.get_barrier_semaphore()
    for peer in peers:
        pl.semaphore_signal(barrier, inc=1, device_id=peer, device_id_type=MESH)
    pl.semaphore_wait(barrier, len(peers))


def column_peers(z, c):
    me = z * 2 + c
    peers = []
    for step in range(1, 2 * NZ):
        other = wrap(me + step, 2 * NZ)
        peers.append({"st_0": other // 2, "st_2": lax.rem(other, 2)})
    return peers


def columns_of(rows):
    return jnp.transpose(rows)


def mixer_rows(mx):
    strength = jax.nn.sigmoid(mx[0:8])
    pre = mx[8:16]
    log_decay = -mx[16:17] * (jnp.maximum(pre, 0.0) + jnp.log1p(jnp.exp(-jnp.abs(pre))))
    lane = lax.broadcasted_iota(jnp.int32, (8, 128), 1)
    inner = lax.rem(lane, SPAN)
    total = log_decay
    for shift in (1, 2, 4, 8, 16, 32):
        total = total + jnp.where(inner >= shift, pltpu.roll(total, shift, axis=1), 0.0)
    ends = [
        jnp.sum(jnp.where(lane == at, total, 0.0), axis=1, keepdims=True) for at in (SPAN - 1, 2 * SPAN - 1)
    ]
    last = jnp.where(lane < SPAN, ends[0], ends[1])
    grown = jnp.exp(total)
    stacked = jnp.concatenate([strength, total, strength * grown, grown, jnp.exp(last - total)], axis=0)
    return total, ends, stacked


def low_dot(a, b, dims=(((1,), (0,)), ((), ()))):
    return lax.dot_general(a.astype(BF16), b.astype(BF16), dims, preferred_element_type=F32)


def mixer_prepare(b, mq, mk, mv, total, cols, fresh, corr, att, qdec, kdec):
    at = slice(b * SPAN, (b + 1) * SPAN)

    def both(ref):
        return jnp.concatenate([ref[at, 0:128], ref[at, 128:256]], axis=0).astype(F32)

    def unit(value):
        return value * lax.rsqrt(jnp.sum(value * value, axis=-1, keepdims=True) + NORM_FLOOR)

    def column(k):
        return cols[:, k * 8 + b : k * 8 + b + 1]

    queries, keys, values = unit(both(mq)) * 128 ** (-0.5), unit(both(mk)), both(mv)
    row, col = lax.broadcasted_iota(jnp.int32, (128, 128), 0), lax.broadcasted_iota(jnp.int32, (128, 128), 1)
    same = (row // SPAN) == (col // SPAN)
    spread = jnp.where(same & (row >= col), column(1) - total[b : b + 1, :], -1e30)
    decay = jnp.exp(spread)
    strict = jnp.where(same & (row > col), column(0) * low_dot(keys, keys, CONTRACT_LAST) * decay, 0.0)
    inverse = jnp.where(row == col, 1.0, 0.0) - strict
    power = strict
    for _ in range(SPAN.bit_length() - 2):
        power = low_dot(power, power)
        inverse = inverse + low_dot(inverse, power)
    fresh[b] = low_dot(inverse, values * column(0))
    corr[b] = low_dot(inverse, keys * column(2)).astype(BF16)
    att[b] = (low_dot(queries, keys, CONTRACT_LAST) * decay).astype(BF16)
    qdec[b] = (queries * column(3)).astype(BF16)
    kdec[b] = (keys * column(4)).astype(BF16)


def mixer_advance(b, state, grads, ends, fresh, corr, att, qdec, kdec, sums):
    heads = [slice(0, 64), slice(64, 128)]
    new = jnp.concatenate(
        [fresh[b, h, :] - low_dot(corr[b, h, :], state[i]) for i, h in enumerate(heads)], axis=0
    )
    out = jnp.concatenate([low_dot(qdec[b, h, :], state[i]) for i, h in enumerate(heads)], axis=0)
    out = out + low_dot(att[b], new)
    state = [
        jnp.exp(ends[i][b : b + 1, :]) * state[i] + low_dot(kdec[b, h, :], new[h], CONTRACT_FIRST)
        for i, h in enumerate(heads)
    ]
    grads = jnp.concatenate([grads[:, 0:128], grads[:, 128:256]], axis=0).astype(F32)
    lane = lax.broadcasted_iota(jnp.int32, (128, 128), 1)
    sums = jnp.where(lane == b, jnp.sum(grads * out, axis=-1, keepdims=True), sums)
    return state, sums


def gather_kernel(
    pas_in, wk_in, wv_in, tok_in, wq_in, gw_in, cot_in, mq_in, mk_in, mv_in, ids_in, beta_in, pre_in, rate_in,
    kv, qa, ca, tl, tb, klow, qlow, gown, wall, gall, md, eg, tot, own,
    tbs, sent, parts, total, ss, sr, bs, br,
    pas, wk, wv, wq, mq, mk, mv, gw_row, ids, beta, pre, rate, gw, mx,
    toks, relay, fresh, corr, att, qdec, kdec,
    ins, hs, hr, xs, xr, ys, yr, zs, zr, ps, pr, ts, tr, ws, wr, vs, vr, gs, gr,
):
    z, y, c, x = place()
    me = z * 2 + c
    up, down = {"st_0": wrap(z + 1, NZ)}, {"st_0": wrap(z - 1, NZ)}
    east, west = {"st_1": wrap(y + 1, NY)}, {"st_1": wrap(y - 1, NY)}
    front, back = {"tp": wrap(x + 1, NX)}, {"tp": wrap(x - 1, NX)}
    partner = {"st_2": 1 - c}
    peers = column_peers(z, c)
    across = {"tp": wrap(x + 2, NX)}
    reads = {}

    def fetch(name, src, dst):
        reads[name] = pltpu.make_async_copy(src, dst, ins.at[len(reads)])
        reads[name].start()

    fetch("tok", tok_in, toks.at[x])
    fetch("cot", cot_in, ca.at[pl.ds(me * 6, 6)])
    fetch("wk", wk_in, wk)
    fetch("wv", wv_in, wv)
    for i in range(4):
        fetch(f"pas{i}", pas_in.at[pl.ds(i * 256, 256), :], pas.at[pl.ds(i * 256, 256), :])
    fetch("wq", wq_in, wq)
    for name, src, dst in (
        ("gw", gw_in, gw_row), ("ids", ids_in, ids), ("beta", beta_in, beta), ("pre", pre_in, pre),
        ("rate", rate_in, rate), ("mq", mq_in, mq), ("mk", mk_in, mk), ("mv", mv_in, mv),
    ):
        fetch(name, src, dst)
    greet(peers + [east, west, front, back, across])
    copies = Copies()
    half = 192
    zdirs, ydirs, xdirs = (up, down), (east, west), (front, back)

    def token_rows(slot, h):
        return toks.at[slot, pl.ds(h * half, half), :]

    def rows_of(ref, slot, h):
        return ref.at[pl.ds(slot * 6 + h * 3, 3)]

    def z_send(k, ref, d, h):
        for way in (0, 1):
            if d == 4 and h != way:
                continue
            owner = wrap(z - (d - 1), NZ) if way == 0 else wrap(z + (d - 1), NZ)
            piece = rows_of(ref, owner * 2 + c, h)
            at = (d - 1) * 2 + h if d < 4 else 6
            copies.start(piece, piece, zs.at[k, way, at], zr.at[k, way, at], zdirs[way])

    def z_take(k, ref, d):
        for h in (0, 1):
            for way in (0, 1):
                if d == 4 and h != way:
                    continue
                owner = wrap(z - d, NZ) if way == 0 else wrap(z + d, NZ)
                piece = rows_of(ref, owner * 2 + c, h)
                at = (d - 1) * 2 + h if d < 4 else 6
                copies.arrived(piece, zs.at[k, way, at], zr.at[k, way, at], zdirs[way])
                if d < 3 or (d == 3 and h == way):
                    nxt = d * 2 + h if d < 3 else 6
                    copies.start(piece, piece, zs.at[k, way, nxt], zr.at[k, way, nxt], zdirs[way])
                to = 2 + way * 7 + at
                copies.start(piece, piece, ps.at[k, to], pr.at[k, to], partner)

    def own_send(k, ref):
        for h in (0, 1):
            z_send(k, ref, 1, h)
        for h in (0, 1):
            piece = rows_of(ref, me, h)
            copies.start(piece, piece, ps.at[k, h], pr.at[k, h], partner)

    def partner_take(k, ref):
        theirs = 1 - c
        for h in (0, 1):
            piece = rows_of(ref, z * 2 + theirs, h)
            copies.arrived(piece, ps.at[k, h], pr.at[k, h], partner)
        for d in (1, 2, 3, 4):
            for h in (0, 1):
                for way in (0, 1):
                    if d == 4 and h != way:
                        continue
                    owner = wrap(z - d, NZ) if way == 0 else wrap(z + d, NZ)
                    to = 2 + way * 7 + ((d - 1) * 2 + h if d < 4 else 6)
                    piece = rows_of(ref, owner * 2 + theirs, h)
                    copies.arrived(piece, ps.at[k, to], pr.at[k, to], partner)

    reads["tok"].wait()
    for way, h in ((0, 0), (1, 1), (0, 1), (1, 0)):
        piece = token_rows(x, h)
        copies.start(piece, piece, xs.at[way, h], xr.at[way, h], xdirs[way])
    reads["cot"].wait()
    own_send(0, ca)

    rows = 256

    def kv_rows(i):
        return kv.at[pl.ds(y * 16 + i * 4, 4)]

    reads["wk"].wait()
    reads["wv"].wait()
    for i in range(4):
        reads[f"pas{i}"].wait()
        block = pas[pl.ds(i * rows, rows), :]
        low = jnp.dot(block, wk[...], preferred_element_type=F32).astype(BF16)
        wide = low.astype(F32)
        scale = lax.rsqrt(jnp.mean(wide * wide, axis=-1, keepdims=True) + NORM_FLOOR)
        klow[pl.ds(i * rows, rows), :] = low
        kv[pl.ds(y * 16 + i * 4, 4), :, 0:256] = (wide * scale).astype(BF16).reshape(4, 64, 256)
        value = jnp.dot(block, wv[...], preferred_element_type=F32)
        kv[pl.ds(y * 16 + i * 4, 4), :, 256:512] = value.astype(BF16).reshape(4, 64, 256)
        for way in (0, 1):
            copies.start(kv_rows(i), kv_rows(i), ys.at[way, i], yr.at[way, i], ydirs[way])

    def y_take(i):
        for way in (0, 1):
            owner = wrap(y - 1, NY) if way == 0 else wrap(y + 1, NY)
            piece = kv.at[pl.ds(owner * 16 + i * 4, 4)]
            copies.arrived(piece, ys.at[way, i], yr.at[way, i], ydirs[way])
            if i % 2 == way:
                at = 4 + i // 2
                copies.start(piece, piece, ys.at[way, at], yr.at[way, at], ydirs[way])

    def y_last():
        owner = wrap(y + 2, NY)
        for i in range(4):
            way, at = i % 2, 4 + i // 2
            piece = kv.at[pl.ds(owner * 16 + i * 4, 4)]
            copies.arrived(piece, ys.at[way, at], yr.at[way, at], ydirs[way])

    def x_take(first):
        for way in (0, 1):
            owner = wrap(x - 1, NX) if way == 0 else wrap(x + 1, NX)
            h = way if first else 1 - way
            piece = token_rows(owner, h)
            copies.arrived(piece, xs.at[way, h], xr.at[way, h], xdirs[way])
            if first:
                copies.start(piece, piece, xs.at[way, 2], xr.at[way, 2], xdirs[way])

    def x_last():
        owner = wrap(x + 2, NX)
        for way in (0, 1):
            piece = token_rows(owner, way)
            copies.arrived(piece, xs.at[way, 2], xr.at[way, 2], xdirs[way])

    def project(owner):
        block = toks[owner]
        at = pl.ds(pl.multiple_of(owner * 512, 512), 512)
        return (
            jnp.dot(block, wq[at, :], preferred_element_type=F32),
            lax.dot_general(gw[:, at], block, CONTRACT_LAST, preferred_element_type=F32),
        )

    weights = (wk, wv, wq)
    via, behind = {"tp": wrap(x + 1 - 2 * c, NX)}, wrap(x - 1 + 2 * c, NX)

    def w_rows(owner):
        return pl.ds(pl.multiple_of(owner * 512 + c * 256, 256), 256)

    mine = pl.ds(pl.multiple_of(c * 256, 256), 256)

    def w_send():
        for i, ref in enumerate(weights):
            copies.start(ref.at[w_rows(wrap(x + 2, NX)), :], relay.at[i], ws.at[6 + i], wr.at[6 + i], via)
        for way in (0, 1):
            to = wrap(x + 1 - 2 * way, NX)
            for i, ref in enumerate(weights):
                copies.start(
                    ref.at[w_rows(to), :], wall.at[i, x, mine, :], ws.at[way * 3 + i], wr.at[way * 3 + i], xdirs[way]
                )
        for step, peer in enumerate((front, across, back)):
            at = pl.ds(pl.multiple_of(wrap(x + 1 + step, NX) * 512, 512), 512)
            copies.start(gw.at[:, at], gall.at[x], gs.at[step], gr.at[step], peer)
        own = pl.ds(pl.multiple_of(x * 512, 512), 512)
        for i, ref in enumerate(weights):
            wall[i, x] = ref[own, :]
        gall[x] = gw[:, own]

    def w_forward():
        for i in range(3):
            copies.arrived(relay.at[i], ws.at[6 + i], wr.at[6 + i], via)
            copies.start(relay.at[i], wall.at[i, behind, mine, :], ws.at[9 + i], wr.at[9 + i], via)

    def w_share(n, owner, first):
        for i in range(3):
            piece = wall.at[i, owner, mine, :]
            copies.arrived(piece, ws.at[first + i], wr.at[first + i], via)
            copies.start(piece, piece, vs.at[n * 3 + i], vr.at[n * 3 + i], partner)

    def w_last():
        theirs = pl.ds(pl.multiple_of((1 - c) * 256, 256), 256)
        for n, owner in enumerate((wrap(x - 1, NX), wrap(x + 1, NX), wrap(x + 2, NX))):
            for i in range(3):
                copies.arrived(wall.at[i, owner, theirs, :], vs.at[n * 3 + i], vr.at[n * 3 + i], partner)
        for step, peer in enumerate((front, across, back)):
            copies.arrived(gall.at[wrap(x - 1 - step, NX)], gs.at[step], gr.at[step], peer)

    for name in ("wq", "gw", "ids", "beta", "pre", "rate", "mq", "mk", "mv"):
        reads[name].wait()
    gw[...] = jnp.broadcast_to(gw_row[...].astype(F32), (16, 2048)).astype(BF16)
    lanes = lax.broadcasted_iota(jnp.int32, (1, 128), 1)
    row = jnp.full((1, 128), -1, jnp.int32)
    for b in range(6):
        for p in range(4):
            each = jnp.broadcast_to(ids[p : p + 1, b : b + 1], (1, 128))
            row = jnp.where(lanes == each // 16, (b * 4 + p) * 16 + lax.rem(each, 16), row)
    tb[me] = row
    for step, peer in enumerate(peers):
        copies.start(tb.at[me], tb.at[me], hs.at[step], hr.at[step], peer)
    mx[...] = jnp.zeros((24, 128), F32)
    for b in range(6):
        for h in range(2):
            mx[b : b + 1, h * 64 : h * 64 + 64] = beta[h : h + 1, b * 64 : b * 64 + 64]
            mx[8 + b : 9 + b, h * 64 : h * 64 + 64] = pre[h : h + 1, b * 64 : b * 64 + 64]
    for h in range(2):
        mx[16:17, h * 64 : h * 64 + 64] = jnp.broadcast_to(rate[0:1, h : h + 1], (1, 64))
    decays, ends, stacked = mixer_rows(mx[...])
    cols = columns_of(stacked)
    work = (fresh, corr, att, qdec, kdec)

    def prepare(b):
        mixer_prepare(b, mq, mk, mv, decays, cols, *work)

    z_take(0, ca, 1)
    x_take(True)
    w_send()
    acc = project(x)
    prepare(0)
    y_take(0)
    z_take(0, ca, 2)
    x_take(False)
    for owner in (wrap(x - 1, NX), wrap(x + 1, NX)):
        more = project(owner)
        acc = (acc[0] + more[0], acc[1] + more[1])
    prepare(1)
    x_last()
    more = project(wrap(x + 2, NX))
    low = (acc[0] + more[0]).astype(BF16)
    gate = jax.nn.sigmoid(acc[1] + more[1])
    wide = low.astype(F32)
    scale = lax.rsqrt(jnp.mean(wide * wide, axis=-1, keepdims=True) + NORM_FLOOR)
    qlow[...] = low
    qa[pl.ds(me * 6, 6)] = (wide * scale).astype(BF16).reshape(6, 64, 256)
    own_send(1, qa)
    z_take(0, ca, 3)
    y_take(1)
    tl[me] = jnp.zeros((8, 128), F32)
    for b in range(6):
        tl[me, b : b + 1, 0:64] = gate[0:1, b * 64 : b * 64 + 64]
    gown[...] = tl[me]
    y_take(2)
    prepare(2)
    z_take(1, qa, 1)
    z_take(0, ca, 4)
    prepare(3)
    w_forward()
    y_take(3)
    z_take(1, qa, 2)
    for step, peer in enumerate(peers):
        copies.start(tl.at[me], tl.at[me], ts.at[step], tr.at[step], peer)
    w_share(0, wrap(x - 1, NX), 0)
    w_share(1, wrap(x + 1, NX), 3)
    prepare(4)
    z_take(1, qa, 3)
    w_share(2, wrap(x + 2, NX), 9)
    prepare(5)
    state = [jnp.zeros((128, 128), F32), jnp.zeros((128, 128), F32)]
    sums = jnp.zeros((128, 128), F32)
    for b in range(6):
        state, sums = mixer_advance(b, state, ca[me * 6 + b], ends, *work, sums)
    turned = jnp.transpose(sums)[0:8]
    md[...] = turned[:, 0:64] + turned[:, 64:128]
    w_last()
    z_take(1, qa, 4)
    for step in range(2 * NZ - 1):
        other = wrap(me - (step + 1), 2 * NZ)
        copies.arrived(tl.at[other], ts.at[step], tr.at[step], peers[step])
        copies.arrived(tb.at[other], hs.at[step], hr.at[step], peers[step])
    table = pltpu.make_async_copy(tb, tbs, ins.at[17])
    table.start()
    partner_take(0, ca)
    partner_take(1, qa)
    y_last()
    table.wait()

    gain = SCORE_GAIN * 256 ** (-0.5)
    line = lax.broadcasted_iota(jnp.int32, (8, 128), 0)

    def reader(r):
        tile = tl[r]
        stats = jnp.zeros((8, 128), F32)
        for yy in range(NY):
            entry = tbs[r, 0, (z * NY + yy) * 2 + c]
            used = entry >= 0
            safe = jnp.maximum(entry, 0)
            b, loc = safe // 64, lax.rem(safe, 16)
            keys_values = kv[yy * 16 + loc]
            scores = gain * lax.dot_general(
                keys_values[:, 0:256], qa[r * 6 + b], CONTRACT_LAST, preferred_element_type=F32
            )
            here = (line == b) & used
            gate = jnp.sum(jnp.where(line == b, tile, 0.0), axis=0, keepdims=True)
            grads = gate[:, 0:64] * lax.dot_general(
                keys_values[:, 256:512], ca[r * 6 + b], CONTRACT_LAST, preferred_element_type=F32
            )
            exps = jnp.exp(scores)
            both = jnp.concatenate([exps, grads], axis=1)
            eg[r * NY + yy] = both
            row = jnp.concatenate(
                [jnp.sum(exps, axis=0, keepdims=True), jnp.sum(exps * grads, axis=0, keepdims=True)], axis=1
            )
            stats = stats + jnp.where(here, row, 0.0)
        sent[r] = stats

    def outward(i, carry):
        near = (i + 1) // 2
        step = NZ + near - 2 * near * lax.rem(i, 2) - 1
        r = wrap(me + step + 1, 2 * NZ)
        reader(r)
        copies.make(
            sent.at[r], parts.at[step], ss.at[step], sr.at[step], {"st_0": r // 2, "st_2": lax.rem(r, 2)}
        ).start()
        return carry

    lax.fori_loop(0, 2 * NZ - 1, outward, 0)
    reader(me)
    whole = sent[me]
    for step in range(2 * NZ - 1):
        copies.arrived(parts.at[step], ss.at[step], sr.at[step], peers[step])
        whole = whole + parts[step]
    total[...] = whole
    tot[me] = whole
    own[...] = whole
    for step, peer in enumerate(peers):
        copies.start(total, tot.at[me], bs.at[step], br.at[step], peer)
    for step in range(2 * NZ - 1):
        other = wrap(me - (step + 1), 2 * NZ)
        copies.arrived(tot.at[other], bs.at[step], br.at[step], peers[step])
        copies.make(sent.at[0], parts.at[step], ss.at[step], sr.at[step], peers[step]).wait_send()
    copies.finish()


def grads_kernel(tb, kv, qa, ca, tl, eg, tot, kvg, qp, todo):
    z, c = lax.axis_index("st_0"), lax.axis_index("st_2")
    gain = SCORE_GAIN * 256 ** (-0.5)

    def entry_of(i):
        return tb[i // NY, 0, (z * NY + lax.rem(i, NY)) * 2 + c]

    def pick(i, count):
        todo[count] = i
        return count + (entry_of(i) >= 0).astype(jnp.int32)

    count = lax.fori_loop(0, 64, pick, 0)
    todo[count] = 0

    @pl.loop(0, 32)
    def _(i):
        blank = jnp.zeros((2, 64, 256), BF16)
        kvg[0, pl.ds(i * 2, 2)] = blank
        kvg[1, pl.ds(i * 2, 2)] = blank
        qp[pl.ds(i * 3, 3)] = jnp.zeros((3, 64, 256), BF16)

    @pl.loop(0, (count + 1) // 2)
    def _(pair):
        terms = []
        for u in range(2):
            i = todo[pair * 2 + u]
            live = (pair * 2 + u < count).astype(F32)
            entry = jnp.maximum(entry_of(i), 0)
            r, b = i // NY, entry // 64
            at, slot = r * 6 + b, lax.rem(i, NY) * 16 + lax.rem(entry, 16)
            row = tot[r, pl.ds(b, 1), :]
            gate = tl[r, pl.ds(b, 1), 0:64]
            norm = 1.0 / row[:, 0:64]
            both = eg[i]
            probs = both[:, 0:64] * (norm * live)
            slope = (probs * (both[:, 64:128] - row[:, 64:128] * norm)).astype(BF16)
            gated = (probs * gate).astype(BF16)
            key = gain * jnp.dot(slope, qa[at], preferred_element_type=F32)
            value = jnp.dot(gated, ca[at], preferred_element_type=F32)
            query = gain * lax.dot_general(
                slope, kv[slot, :, 0:256], CONTRACT_FIRST, preferred_element_type=F32
            )
            terms.append((at, slot, key, value, query))
        for at, slot, key, value, query in terms:
            kvg[0, slot] = (kvg[0, slot].astype(F32) + key).astype(BF16)
            kvg[1, slot] = (kvg[1, slot].astype(F32) + value).astype(BF16)
            qp[at] = (qp[at].astype(F32) + query).astype(BF16)


def finish_kernel(
    kvg, qp, klow, pas, qlow, wall, gall, own, md, gown,
    tgrad, pgrad, wgrad,
    ybuf, ysum, px, qs, zbuf, xall, pacc, tacc, xq, ggx, whalf, wget, wz, wbuf, wsum, wlast,
    ys, yr, zs, zr, ps, pr, xs, xr, qxs, qxr, gs, gr, us, ur, vs, vr, ls, lr,
):
    z, y, c, x = place()
    up, down = {"st_0": wrap(z + 1, NZ)}, {"st_0": wrap(z - 1, NZ)}
    east, west = {"st_1": wrap(y + 1, NY)}, {"st_1": wrap(y - 1, NY)}
    front, back, across = {"tp": wrap(x + 1, NX)}, {"tp": wrap(x - 1, NX)}, {"tp": wrap(x + 2, NX)}
    partner = {"st_2": 1 - c}
    spot = y * 2 + c
    plane = []
    for step in range(1, 8):
        other = wrap(spot + step, 8)
        plane.append({"st_1": other // 2, "st_2": lax.rem(other, 2)})
    greet([up, down, front, back, across] + plane)
    copies = Copies()
    zdirs, ydirs, xdirs = (up, down), (east, west), (front, back)

    far, beside = wrap(y + 2, NY), (wrap(y + 1, NY), wrap(y - 1, NY))

    def y_rows(j, part):
        return j // 4, pl.ds((j % 4) * 256 + part * 128, 128)

    def y_far(j):
        for way in (0, 1):
            p, at = y_rows(j, way)
            copies.start(kvg.at[p, far, at, :], ybuf.at[way, j], ys.at[0, way, j], yr.at[0, way, j], ydirs[way])

    def y_near(j):
        for way in (0, 1):
            p, at = y_rows(j, 1 - way)
            copies.start(
                kvg.at[p, beside[way], at, :], ysum.at[way, p, at, :], ys.at[1, way, j], yr.at[1, way, j], ydirs[way]
            )

    def y_add(j):
        for way in (0, 1):
            p, at = y_rows(j, way)
            copies.arrived(ybuf.at[way, j], ys.at[0, way, j], yr.at[0, way, j], ydirs[way])
            ybuf[way, j] = (kvg[p, beside[way], at, :].astype(F32) + ybuf[way, j].astype(F32)).astype(BF16)
            copies.start(ybuf.at[way, j], ysum.at[way, p, at, :], ys.at[2, way, j], yr.at[2, way, j], ydirs[way])
        if j + 1 < 8:
            y_near(j + 1)
        if j + 2 < 8:
            y_far(j + 2)

    def x_pieces(j, h):
        return j // 4, pl.ds((j % 4) * 256 + h * 128, 128)

    def y_done(j):
        for way in (0, 1):
            p, at = y_rows(j, 1 - way)
            copies.arrived(ysum.at[way, p, at, :], ys.at[1, way, j], yr.at[1, way, j], ydirs[way])
            p, at = y_rows(j, way)
            copies.arrived(ysum.at[way, p, at, :], ys.at[2, way, j], yr.at[2, way, j], ydirs[way])
        for h in (0, 1):
            p, at = x_pieces(j, h)
            grad = kvg[p, y, at, :].astype(F32) + ysum[0, p, at, :].astype(F32) + ysum[1, p, at, :].astype(F32)
            if p == 0:
                wide = klow[at, :].astype(F32)
                scale = lax.rsqrt(jnp.mean(wide * wide, axis=-1, keepdims=True) + NORM_FLOOR)
                inner = jnp.mean(wide * grad, axis=-1, keepdims=True)
                grad = scale * grad - (scale * scale * scale * inner) * wide
            xall[x, p, at, :] = grad.astype(BF16)
            for way in (0, 1):
                piece = xall.at[x, p, at, :]
                copies.start(piece, piece, xs.at[j, way, h], xr.at[j, way, h], xdirs[way])

    def x_take(j):
        for way in (0, 1):
            owner = wrap(x - 1 + 2 * way, NX)
            for h in (0, 1):
                p, at = x_pieces(j, h)
                piece = xall.at[owner, p, at, :]
                copies.arrived(piece, xs.at[j, way, h], xr.at[j, way, h], xdirs[way])
                if h == way:
                    copies.start(piece, piece, xs.at[j, way, 2], xr.at[j, way, 2], xdirs[way])

    def head_dot(rows, weight):
        return lax.dot_general(rows, weight, CONTRACT_LAST, preferred_element_type=F32)

    def x_near(j):
        p = j // 4

        @pl.loop(0, 2)
        def _(i):
            at = pl.ds(pl.multiple_of((j % 4) * 256 + i * 128, 128), 128)
            term = head_dot(xall[x, p, at, :], wall[p, x])
            for owner in (wrap(x - 1, NX), wrap(x + 1, NX)):
                term += head_dot(xall[owner, p, at, :], wall[p, owner])
            pacc[at, :] = term if p == 0 else pacc[at, :] + term

    def x_last(j):
        owner = wrap(x + 2, NX)
        for way in (0, 1):
            p, at = x_pieces(j, way)
            copies.arrived(xall.at[owner, p, at, :], xs.at[j, way, 2], xr.at[j, way, 2], xdirs[way])
        p = j // 4

        @pl.loop(0, 2)
        def _(i):
            at = pl.ds(pl.multiple_of((j % 4) * 256 + i * 128, 128), 128)
            term = pacc[at, :] + head_dot(xall[owner, p, at, :], wall[p, owner])
            if p == 0:
                pacc[at, :] = term
            else:
                pgrad[at, :] = term.astype(BF16)

    def ring_step(d, value, slots, send, recv, half):
        for way in (0, 1):
            there = wrap(z + d, NZ) if way == 0 else wrap(z - d, NZ)
            at = pl.ds(way * half, half)
            if d == 3:
                copies.arrived(slots.at[way, 0, at, :], send.at[way, 3], recv.at[way, 3], zdirs[way])
                value[there, at, :] = (value[there, at, :].astype(F32) + slots[way, 0, at, :].astype(F32)).astype(BF16)
            elif d < 3:
                copies.arrived(slots.at[way, 3 - d], send.at[way, d], recv.at[way, d], zdirs[way])
                value[there] = (value[there].astype(F32) + slots[way, 3 - d].astype(F32)).astype(BF16)
            if d == 4:
                copies.start(value.at[there, at, :], slots.at[way, 0, at, :], send.at[way, 3], recv.at[way, 3], zdirs[way])
            else:
                copies.start(value.at[there], slots.at[way, 4 - d], send.at[way, d - 1], recv.at[way, d - 1], zdirs[way])

    def ring_last(value, slots, send, recv):
        result = value[z].astype(F32)
        for way in (0, 1):
            copies.arrived(slots.at[way, 3], send.at[way, 0], recv.at[way, 0], zdirs[way])
            result = result + slots[way, 3].astype(F32)
        return result

    def q_pair(k):
        there = wrap(z + k, NZ)
        copies.arrived(px.at[there], ps.at[k], pr.at[k], partner)
        qs[there] = (qp[there * 2 + c].astype(F32) + px[there].astype(F32)).astype(BF16)

    def q_step(d):
        ring_step(d, qs, zbuf, zs, zr, 192)

    def q_done():
        grad = ring_last(qs, zbuf, zs, zr)
        wide = qlow[...].astype(F32)
        scale = lax.rsqrt(jnp.mean(wide * wide, axis=-1, keepdims=True) + NORM_FLOOR)
        inner = jnp.mean(wide * grad, axis=-1, keepdims=True)
        xq[x] = (scale * grad - (scale * scale * scale * inner) * wide).astype(BF16)
        for way in (0, 1):
            for h in (0, 1):
                piece = xq.at[x, pl.ds(h * 192, 192), :]
                copies.start(piece, piece, qxs.at[way, h], qxr.at[way, h], xdirs[way])

    def gates():
        gate = gown[0:6, 0:64]
        dots = own[0:6, 64:128] / own[0:6, 0:64]
        ggx[x] = jnp.zeros((8, 128), F32)
        ggx[x, 0:6, 0:64] = (1.0 - gate) * (dots - gate * md[0:6, :])
        for step, peer in enumerate((front, across, back)):
            copies.start(ggx.at[x], ggx.at[x], gs.at[step], gr.at[step], peer)

    def q_take():
        for way in (0, 1):
            owner = wrap(x - 1 + 2 * way, NX)
            for h in (0, 1):
                piece = xq.at[owner, pl.ds(h * 192, 192), :]
                copies.arrived(piece, qxs.at[way, h], qxr.at[way, h], xdirs[way])
                if h == way:
                    copies.start(piece, piece, qxs.at[way, 2], qxr.at[way, 2], xdirs[way])

    def q_last():
        owner = wrap(x + 2, NX)
        for way in (0, 1):
            copies.arrived(xq.at[owner, pl.ds(way * 192, 192), :], qxs.at[way, 2], qxr.at[way, 2], xdirs[way])
        for b in range(6):
            at = pl.ds(b * 64, 64)
            tgrad[at, :] = (tacc[at, :] + head_dot(xq[owner, at, :], wall[2, owner])).astype(BF16)

    def q_near():
        for step, peer in enumerate((front, across, back)):
            copies.arrived(ggx.at[wrap(x - 1 - step, NX)], gs.at[step], gr.at[step], peer)
        blank = [jnp.zeros((4, 64), F32)]
        slope = jnp.concatenate(
            [gall[h, 0:1, :].astype(F32) for h in range(NX)] + [jnp.zeros((4, 512), F32)], axis=0
        )
        for b in range(6):
            at = pl.ds(b * 64, 64)
            rows = jnp.concatenate([ggx[h, b : b + 1, 0:64] for h in range(NX)] + blank, axis=0)
            term = lax.dot_general(
                rows, slope, CONTRACT_FIRST, preferred_element_type=F32, precision=lax.Precision.HIGHEST
            )
            for owner in (x, wrap(x - 1, NX), wrap(x + 1, NX)):
                term += head_dot(xq[owner, at, :], wall[2, owner])
            tacc[at, :] = term

    keep = pl.ds(pl.multiple_of(c * 128, 128), 128)
    give = pl.ds(pl.multiple_of((1 - c) * 128, 128), 128)

    def w_tile(k):
        there = wrap(z + k, NZ)
        at = pl.ds(pl.multiple_of(there * 256, 256), 256)
        wsum[there] = lax.dot_general(
            pas[:, at], xall[x, 0], CONTRACT_FIRST, preferred_element_type=F32
        )
        whalf[there] = wsum[there, :, give]
        copies.start(whalf.at[there], wget.at[there], us.at[k], ur.at[k], partner)

    def w_pair(k):
        there = wrap(z + k, NZ)
        copies.arrived(wget.at[there], us.at[k], ur.at[k], partner)
        wz[there] = (wsum[there, :, keep] + wget[there]).astype(BF16)

    def w_step(d):
        ring_step(d, wz, wbuf, vs, vr, 128)

    def w_done():
        wsum[z, :, 0:128] = ring_last(wz, wbuf, vs, vr)
        for step, peer in enumerate(plane):
            other = wrap(spot + step + 1, 8)
            piece = wsum.at[z, pl.ds(pl.multiple_of(other * 32, 32), 32), pl.ds(0, 128)]
            copies.start(piece, wlast.at[spot], ls.at[step], lr.at[step], peer)
        wlast[spot] = wsum[z, pl.ds(pl.multiple_of(spot * 32, 32), 32), 0:128]

    def w_last():
        for step, peer in enumerate(plane):
            copies.arrived(wlast.at[wrap(spot - step - 1, 8)], ls.at[step], lr.at[step], peer)
        for k in (0, 1):
            wgrad[:, k * 128 : k * 128 + 128] = wlast[k] + wlast[2 + k] + wlast[4 + k] + wlast[6 + k]

    y_far(0)
    y_near(0)
    y_far(1)
    for k in (4, 3, 5, 2, 6, 1, 7, 0):
        there = wrap(z + k, NZ)
        copies.start(qp.at[there * 2 + 1 - c], px.at[there], ps.at[k], pr.at[k], partner)
    q_pair(4)
    q_step(4)
    q_pair(3)
    q_pair(5)
    y_add(0)
    for k in (2, 6, 1, 7, 0):
        q_pair(k)
    gates()
    y_add(1)
    q_step(3)
    y_done(0)
    y_add(2)
    y_done(1)
    q_step(2)
    x_take(0)
    y_add(3)
    y_done(2)
    x_take(1)
    y_add(4)
    y_done(3)
    q_step(1)
    x_near(0)
    x_last(0)
    for k in (4, 3, 5):
        w_tile(k)
    x_take(2)
    y_add(5)
    y_done(4)
    x_near(1)
    x_last(1)
    x_take(3)
    for k in (2, 6, 1, 7, 0):
        w_tile(k)
    y_add(6)
    q_done()
    y_done(5)
    w_pair(4)
    w_step(4)
    y_add(7)
    y_done(6)
    x_take(4)
    w_pair(3)
    w_pair(5)
    w_step(3)
    y_done(7)
    x_near(2)
    x_last(2)
    q_take()
    x_take(5)
    for k in (2, 6, 1, 7, 0):
        w_pair(k)
    w_step(2)
    x_near(3)
    x_last(3)
    x_near(4)
    x_take(6)
    w_step(1)
    q_near()
    x_last(4)
    x_near(5)
    x_take(7)
    w_done()
    x_near(6)
    x_near(7)
    q_last()
    x_last(5)
    w_last()
    x_last(6)
    x_last(7)
    copies.finish()


def shaped(shape, dtype):
    return jax.ShapeDtypeStruct(shape, dtype)


def dma(*shape):
    return pltpu.SemaphoreType.DMA(shape)


def call(kernel, outs, scratch, collective, smem=0, limit=48, count=0, space=VMEM, **extra):
    in_specs = [pl.BlockSpec(memory_space=pltpu.SMEM)] * smem + [pl.BlockSpec(memory_space=space)] * (count - smem)
    params = dict(vmem_limit_bytes=limit * 2**20)
    if collective is not None:
        params.update(collective_id=collective, has_side_effects=True)
    return pl.pallas_call(
        kernel,
        out_shape=outs,
        in_specs=in_specs,
        out_specs=[pl.BlockSpec(memory_space=VMEM)] * len(outs),
        scratch_shapes=scratch,
        compiler_params=pltpu.CompilerParams(**params),
        **extra,
    )


def body(
    tokens, cotangent, mix_query, mix_key, mix_value, beta_pre, decay_pre, decay_rate,
    passages, passage_ids, query_weight, key_weight, value_weight, gate_weight,
):
    pass_local, span_rows, model_width = passages.shape
    flat_rows = passages.reshape(pass_local * span_rows, model_width)
    kv, qa, ca, tl, lookup, key_low, query_low, gown, wall, gall, md, eg, tot, own = call(
        gather_kernel,
        [
            shaped((64, 64, 512), BF16), shaped((96, 64, 256), BF16), shaped((96, 64, 256), BF16),
            shaped((16, 8, 128), F32), shaped((16, 1, 128), jnp.int32), shaped((1024, 256), BF16), shaped((384, 256), BF16), shaped((8, 128), F32),
            shaped((3, NX, 512, 256), BF16), shaped((NX, 16, 512), BF16), shaped((8, 64), F32),
            shaped((64, 64, 128), F32), shaped((16, 8, 128), F32), shaped((8, 128), F32),
        ],
        [
            pltpu.SMEM((16, 1, 128), jnp.int32), VMEM((16, 8, 128), F32), VMEM((15, 8, 128), F32), VMEM((8, 128), F32),
            dma(15), dma(15), dma(15), dma(15),
            VMEM((1024, 2048), BF16), VMEM((2048, 256), BF16), VMEM((2048, 256), BF16), VMEM((2048, 256), BF16),
            VMEM((384, 256), BF16), VMEM((384, 256), BF16), VMEM((384, 256), BF16), VMEM((1, 2048), BF16),
            VMEM((4, 6), jnp.int32), VMEM((2, 384), F32), VMEM((2, 384), F32), VMEM((1, 2), F32),
            VMEM((16, 2048), BF16), VMEM((24, 128), F32),
            VMEM((NX, 384, 512), BF16), VMEM((3, 256, 256), BF16), VMEM((6, 128, 128), F32),
            VMEM((6, 128, 128), BF16), VMEM((6, 128, 128), BF16), VMEM((6, 128, 128), BF16), VMEM((6, 128, 128), BF16),
            dma(18), dma(15), dma(15), dma(2, 3), dma(2, 3), dma(2, 6), dma(2, 6), dma(2, 2, 7), dma(2, 2, 7),
            dma(2, 16), dma(2, 16), dma(15), dma(15), dma(12), dma(12), dma(9), dma(9), dma(3), dma(3),
        ],
        1, count=14, limit=LIMITS[0], space=pltpu.HBM,
    )(*[pltpu.with_memory_space_constraint(a, pltpu.HBM) for a in (
        flat_rows, key_weight, value_weight, tokens, query_weight, gate_weight, cotangent.reshape(6, 64, 256),
        mix_query, mix_key, mix_value, passage_ids.T, beta_pre, decay_pre, decay_rate[None, :],
    )])
    kvg, qp = call(
        grads_kernel,
        [shaped((2, 64, 64, 256), BF16), shaped((96, 64, 256), BF16)],
        [pltpu.SMEM((66,), jnp.int32)],
        None, smem=1, count=7, limit=LIMITS[1],
    )(lookup, kv, qa, ca, tl, eg, tot)
    token_grad, passage_grad, key_weight_grad = call(
        finish_kernel,
        [shaped((384, 512), BF16), shaped((1024, 512), BF16), shaped((32, 256), F32)],
        [
            VMEM((2, 8, 128, 256), BF16), VMEM((2, 2, 1024, 256), BF16), VMEM((NZ, 384, 256), BF16),
            VMEM((NZ, 384, 256), BF16), VMEM((2, 4, 384, 256), BF16), VMEM((NX, 2, 1024, 256), BF16),
            VMEM((1024, 512), F32), VMEM((384, 512), F32), VMEM((NX, 384, 256), BF16), VMEM((NX, 8, 128), F32),
            VMEM((NZ, 256, 128), F32), VMEM((NZ, 256, 128), F32), VMEM((NZ, 256, 128), BF16),
            VMEM((2, 4, 256, 128), BF16), VMEM((NZ, 256, 256), F32), VMEM((8, 32, 128), F32),
            dma(3, 2, 8), dma(3, 2, 8), dma(2, 4), dma(2, 4), dma(8), dma(8), dma(8, 2, 3), dma(8, 2, 3),
            dma(2, 3), dma(2, 3), dma(3), dma(3), dma(8), dma(8), dma(2, 4), dma(2, 4), dma(7), dma(7),
        ],
        3, count=10, limit=LIMITS[2],
    )(
        kvg.reshape(2, NY, 1024, 256), qp.reshape(16, 384, 256), key_low, flat_rows, query_low,
        wall, gall, own, md, gown,
    )
    return (token_grad, passage_grad.reshape(pass_local, span_rows, 512), key_weight_grad)


def solution(mesh):
    torus = Mesh(mesh.devices.reshape(8, 4, 2, mesh.shape["tp"]), ("st_0", "st_1", "st_2", "tp"))
    return jax.shard_map(
        body,
        mesh=torus,
        in_specs=(
            P(ST, "tp"),
            P(ST, "tp"),
            P(ST, "tp"),
            P(ST, "tp"),
            P(ST, "tp"),
            P("tp", ST),
            P("tp", ST),
            P("tp"),
            P(ST, None, None),
            P(ST, None),
            P(None, "tp"),
            P(None, "tp"),
            P(None, "tp"),
            P("tp", None),
        ),
        out_specs=(P(ST, "tp"), P(ST, None, "tp"), P(ST, "tp")),
        check_vma=False,
    )
```

```python
import functools

import jax
import jax.numpy as jnp
from jax import lax
from jax.experimental import pallas as pl
from jax.experimental.pallas import tpu as pltpu
from jax.sharding import Mesh
from jax.sharding import PartitionSpec as P

SPAN = 64
ST = ("st_0", "st_1", "st_2")
MESH = pl.DeviceIdType.MESH
NZ, NY, NX = 8, 4, 4
VMEM = pltpu.VMEM
F32, BF16 = jnp.float32, jnp.bfloat16
LIMITS = (22, 6, 24)

NORM_FLOOR = 1.0
SCORE_GAIN = 4.0
CONTRACT_LAST = (((1,), (1,)), ((), ()))
CONTRACT_FIRST = (((0,), (0,)), ((), ()))


def place():
    return (lax.axis_index("st_0"), lax.axis_index("st_1"), lax.axis_index("st_2"), lax.axis_index("tp"))


def wrap(value, size):
    return lax.rem(value + size, size)


class Copies:
    def __init__(self):
        self.started = []

    def make(self, src, dst, send, recv, where):
        return pltpu.make_async_remote_copy(
            src_ref=src, dst_ref=dst, send_sem=send, recv_sem=recv, device_id=where, device_id_type=MESH
        )

    def start(self, src, dst, send, recv, where):
        copy = self.make(src, dst, send, recv, where)
        copy.start()
        self.started.append(copy)

    def arrived(self, dst, send, recv, where):
        self.make(dst, dst, send, recv, where).wait_recv()

    def finish(self):
        for copy in self.started:
            copy.wait_send()


def greet(peers):
    barrier = pltpu.get_barrier_semaphore()
    for peer in peers:
        pl.semaphore_signal(barrier, inc=1, device_id=peer, device_id_type=MESH)
    pl.semaphore_wait(barrier, len(peers))


def column_peers(z, c):
    me = z * 2 + c
    peers = []
    for step in range(1, 2 * NZ):
        other = wrap(me + step, 2 * NZ)
        peers.append({"st_0": other // 2, "st_2": lax.rem(other, 2)})
    return peers


def columns_of(rows):
    return jnp.transpose(rows)


def mixer_rows(mx):
    strength = jax.nn.sigmoid(mx[0:8])
    pre = mx[8:16]
    log_decay = -mx[16:17] * (jnp.maximum(pre, 0.0) + jnp.log1p(jnp.exp(-jnp.abs(pre))))
    lane = lax.broadcasted_iota(jnp.int32, (8, 128), 1)
    inner = lax.rem(lane, SPAN)
    total = log_decay
    for shift in (1, 2, 4, 8, 16, 32):
        total = total + jnp.where(inner >= shift, pltpu.roll(total, shift, axis=1), 0.0)
    ends = [
        jnp.sum(jnp.where(lane == at, total, 0.0), axis=1, keepdims=True) for at in (SPAN - 1, 2 * SPAN - 1)
    ]
    last = jnp.where(lane < SPAN, ends[0], ends[1])
    grown = jnp.exp(total)
    stacked = jnp.concatenate([strength, total, strength * grown, grown, jnp.exp(last - total)], axis=0)
    return total, ends, stacked


def low_dot(a, b, dims=(((1,), (0,)), ((), ()))):
    return lax.dot_general(a.astype(BF16), b.astype(BF16), dims, preferred_element_type=F32)


def mixer_prepare(b, mq, mk, mv, total, cols, fresh, corr, att, qdec, kdec):
    at = slice(b * SPAN, (b + 1) * SPAN)

    def both(ref):
        return jnp.concatenate([ref[at, 0:128], ref[at, 128:256]], axis=0).astype(F32)

    def unit(value):
        return value * lax.rsqrt(jnp.sum(value * value, axis=-1, keepdims=True) + NORM_FLOOR)

    def column(k):
        return cols[:, k * 8 + b : k * 8 + b + 1]

    queries, keys, values = unit(both(mq)) * 128 ** (-0.5), unit(both(mk)), both(mv)
    row, col = lax.broadcasted_iota(jnp.int32, (128, 128), 0), lax.broadcasted_iota(jnp.int32, (128, 128), 1)
    same = (row // SPAN) == (col // SPAN)
    spread = jnp.where(same & (row >= col), column(1) - total[b : b + 1, :], -1e30)
    decay = jnp.exp(spread)
    strict = jnp.where(same & (row > col), column(0) * low_dot(keys, keys, CONTRACT_LAST) * decay, 0.0)
    inverse = jnp.where(row == col, 1.0, 0.0) - strict
    power = strict
    for _ in range(SPAN.bit_length() - 2):
        power = low_dot(power, power)
        inverse = inverse + low_dot(inverse, power)
    fresh[b] = low_dot(inverse, values * column(0))
    corr[b] = low_dot(inverse, keys * column(2)).astype(BF16)
    att[b] = (low_dot(queries, keys, CONTRACT_LAST) * decay).astype(BF16)
    qdec[b] = (queries * column(3)).astype(BF16)
    kdec[b] = (keys * column(4)).astype(BF16)


def mixer_advance(b, state, grads, ends, fresh, corr, att, qdec, kdec, sums):
    heads = [slice(0, 64), slice(64, 128)]
    new = jnp.concatenate(
        [fresh[b, h, :] - low_dot(corr[b, h, :], state[i]) for i, h in enumerate(heads)], axis=0
    )
    out = jnp.concatenate([low_dot(qdec[b, h, :], state[i]) for i, h in enumerate(heads)], axis=0)
    out = out + low_dot(att[b], new)
    state = [
        jnp.exp(ends[i][b : b + 1, :]) * state[i] + low_dot(kdec[b, h, :], new[h], CONTRACT_FIRST)
        for i, h in enumerate(heads)
    ]
    grads = jnp.concatenate([grads[:, 0:128], grads[:, 128:256]], axis=0).astype(F32)
    lane = lax.broadcasted_iota(jnp.int32, (128, 128), 1)
    sums = jnp.where(lane == b, jnp.sum(grads * out, axis=-1, keepdims=True), sums)
    return state, sums


def gather_kernel(
    pas_in, wk_in, wv_in, tok_in, wq_in, gw_in, cot_in, mq_in, mk_in, mv_in, ids_in, beta_in, pre_in, rate_in,
    kv, qa, ca, tl, tb, klow, qlow, gown, wall, gall, md, eg, tot, own,
    tbs, sent, parts, total, ss, sr, bs, br,
    pas, wk, wv, wq, mq, mk, mv, gw_row, ids, beta, pre, rate, gw, mx,
    toks, relay, fresh, corr, att, qdec, kdec,
    ins, hs, hr, xs, xr, ys, yr, zs, zr, ps, pr, ts, tr, ws, wr, vs, vr, gs, gr,
):
    z, y, c, x = place()
    me = z * 2 + c
    up, down = {"st_0": wrap(z + 1, NZ)}, {"st_0": wrap(z - 1, NZ)}
    east, west = {"st_1": wrap(y + 1, NY)}, {"st_1": wrap(y - 1, NY)}
    front, back = {"tp": wrap(x + 1, NX)}, {"tp": wrap(x - 1, NX)}
    partner = {"st_2": 1 - c}
    peers = column_peers(z, c)
    across = {"tp": wrap(x + 2, NX)}
    reads = {}

    def fetch(name, src, dst):
        reads[name] = pltpu.make_async_copy(src, dst, ins.at[len(reads)])
        reads[name].start()

    fetch("tok", tok_in, toks.at[x])
    fetch("cot", cot_in, ca.at[pl.ds(me * 6, 6)])
    fetch("wk", wk_in, wk)
    fetch("wv", wv_in, wv)
    for i in range(4):
        fetch(f"pas{i}", pas_in.at[pl.ds(i * 256, 256), :], pas.at[pl.ds(i * 256, 256), :])
    fetch("wq", wq_in, wq)
    for name, src, dst in (
        ("gw", gw_in, gw_row), ("ids", ids_in, ids), ("beta", beta_in, beta), ("pre", pre_in, pre),
        ("rate", rate_in, rate), ("mq", mq_in, mq), ("mk", mk_in, mk), ("mv", mv_in, mv),
    ):
        fetch(name, src, dst)
    greet(peers + [east, west, front, back, across])
    copies = Copies()
    half = 192
    zdirs, ydirs, xdirs = (up, down), (east, west), (front, back)

    def token_rows(slot, h):
        return toks.at[slot, pl.ds(h * half, half), :]

    def rows_of(ref, slot, h):
        return ref.at[pl.ds(slot * 6 + h * 3, 3)]

    def z_send(k, ref, d, h):
        for way in (0, 1):
            if d == 4 and h != way:
                continue
            owner = wrap(z - (d - 1), NZ) if way == 0 else wrap(z + (d - 1), NZ)
            piece = rows_of(ref, owner * 2 + c, h)
            at = (d - 1) * 2 + h if d < 4 else 6
            copies.start(piece, piece, zs.at[k, way, at], zr.at[k, way, at], zdirs[way])

    def z_take(k, ref, d):
        for h in (0, 1):
            for way in (0, 1):
                if d == 4 and h != way:
                    continue
                owner = wrap(z - d, NZ) if way == 0 else wrap(z + d, NZ)
                piece = rows_of(ref, owner * 2 + c, h)
                at = (d - 1) * 2 + h if d < 4 else 6
                copies.arrived(piece, zs.at[k, way, at], zr.at[k, way, at], zdirs[way])
                if d < 3 or (d == 3 and h == way):
                    nxt = d * 2 + h if d < 3 else 6
                    copies.start(piece, piece, zs.at[k, way, nxt], zr.at[k, way, nxt], zdirs[way])
                to = 2 + way * 7 + at
                copies.start(piece, piece, ps.at[k, to], pr.at[k, to], partner)

    def own_send(k, ref):
        for h in (0, 1):
            z_send(k, ref, 1, h)
        for h in (0, 1):
            piece = rows_of(ref, me, h)
            copies.start(piece, piece, ps.at[k, h], pr.at[k, h], partner)

    def partner_take(k, ref):
        theirs = 1 - c
        for h in (0, 1):
            piece = rows_of(ref, z * 2 + theirs, h)
            copies.arrived(piece, ps.at[k, h], pr.at[k, h], partner)
        for d in (1, 2, 3, 4):
            for h in (0, 1):
                for way in (0, 1):
                    if d == 4 and h != way:
                        continue
                    owner = wrap(z - d, NZ) if way == 0 else wrap(z + d, NZ)
                    to = 2 + way * 7 + ((d - 1) * 2 + h if d < 4 else 6)
                    piece = rows_of(ref, owner * 2 + theirs, h)
                    copies.arrived(piece, ps.at[k, to], pr.at[k, to], partner)

    reads["tok"].wait()
    for way, h in ((0, 0), (1, 1), (0, 1), (1, 0)):
        piece = token_rows(x, h)
        copies.start(piece, piece, xs.at[way, h], xr.at[way, h], xdirs[way])
    reads["cot"].wait()
    own_send(0, ca)

    rows = 256

    def kv_rows(i):
        return kv.at[pl.ds(y * 16 + i * 4, 4)]

    reads["wk"].wait()
    reads["wv"].wait()
    for i in range(4):
        reads[f"pas{i}"].wait()
        block = pas[pl.ds(i * rows, rows), :]
        low = jnp.dot(block, wk[...], preferred_element_type=F32).astype(BF16)
        wide = low.astype(F32)
        scale = lax.rsqrt(jnp.mean(wide * wide, axis=-1, keepdims=True) + NORM_FLOOR)
        klow[pl.ds(i * rows, rows), :] = low
        kv[pl.ds(y * 16 + i * 4, 4), :, 0:256] = (wide * scale).astype(BF16).reshape(4, 64, 256)
        value = jnp.dot(block, wv[...], preferred_element_type=F32)
        kv[pl.ds(y * 16 + i * 4, 4), :, 256:512] = value.astype(BF16).reshape(4, 64, 256)
        for way in (0, 1):
            copies.start(kv_rows(i), kv_rows(i), ys.at[way, i], yr.at[way, i], ydirs[way])

    def y_take(i):
        for way in (0, 1):
            owner = wrap(y - 1, NY) if way == 0 else wrap(y + 1, NY)
            piece = kv.at[pl.ds(owner * 16 + i * 4, 4)]
            copies.arrived(piece, ys.at[way, i], yr.at[way, i], ydirs[way])
            if i % 2 == way:
                at = 4 + i // 2
                copies.start(piece, piece, ys.at[way, at], yr.at[way, at], ydirs[way])

    def y_last():
        owner = wrap(y + 2, NY)
        for i in range(4):
            way, at = i % 2, 4 + i // 2
            piece = kv.at[pl.ds(owner * 16 + i * 4, 4)]
            copies.arrived(piece, ys.at[way, at], yr.at[way, at], ydirs[way])

    def x_take(first):
        for way in (0, 1):
            owner = wrap(x - 1, NX) if way == 0 else wrap(x + 1, NX)
            h = way if first else 1 - way
            piece = token_rows(owner, h)
            copies.arrived(piece, xs.at[way, h], xr.at[way, h], xdirs[way])
            if first:
                copies.start(piece, piece, xs.at[way, 2], xr.at[way, 2], xdirs[way])

    def x_last():
        owner = wrap(x + 2, NX)
        for way in (0, 1):
            piece = token_rows(owner, way)
            copies.arrived(piece, xs.at[way, 2], xr.at[way, 2], xdirs[way])

    def project(owner):
        block = toks[owner]
        at = pl.ds(pl.multiple_of(owner * 512, 512), 512)
        return (
            jnp.dot(block, wq[at, :], preferred_element_type=F32),
            lax.dot_general(gw[:, at], block, CONTRACT_LAST, preferred_element_type=F32),
        )

    weights = (wk, wv, wq)
    via, behind = {"tp": wrap(x + 1 - 2 * c, NX)}, wrap(x - 1 + 2 * c, NX)

    def w_rows(owner):
        return pl.ds(pl.multiple_of(owner * 512 + c * 256, 256), 256)

    mine = pl.ds(pl.multiple_of(c * 256, 256), 256)

    def w_send():
        for i, ref in enumerate(weights):
            copies.start(ref.at[w_rows(wrap(x + 2, NX)), :], relay.at[i], ws.at[6 + i], wr.at[6 + i], via)
        for way in (0, 1):
            to = wrap(x + 1 - 2 * way, NX)
            for i, ref in enumerate(weights):
                copies.start(
                    ref.at[w_rows(to), :], wall.at[i, x, mine, :], ws.at[way * 3 + i], wr.at[way * 3 + i], xdirs[way]
                )
        for step, peer in enumerate((front, across, back)):
            at = pl.ds(pl.multiple_of(wrap(x + 1 + step, NX) * 512, 512), 512)
            copies.start(gw.at[:, at], gall.at[x], gs.at[step], gr.at[step], peer)
        own = pl.ds(pl.multiple_of(x * 512, 512), 512)
        for i, ref in enumerate(weights):
            wall[i, x] = ref[own, :]
        gall[x] = gw[:, own]

    def w_forward():
        for i in range(3):
            copies.arrived(relay.at[i], ws.at[6 + i], wr.at[6 + i], via)
            copies.start(relay.at[i], wall.at[i, behind, mine, :], ws.at[9 + i], wr.at[9 + i], via)

    def w_share(n, owner, first):
        for i in range(3):
            piece = wall.at[i, owner, mine, :]
            copies.arrived(piece, ws.at[first + i], wr.at[first + i], via)
            copies.start(piece, piece, vs.at[n * 3 + i], vr.at[n * 3 + i], partner)

    def w_last():
        theirs = pl.ds(pl.multiple_of((1 - c) * 256, 256), 256)
        for n, owner in enumerate((wrap(x - 1, NX), wrap(x + 1, NX), wrap(x + 2, NX))):
            for i in range(3):
                copies.arrived(wall.at[i, owner, theirs, :], vs.at[n * 3 + i], vr.at[n * 3 + i], partner)
        for step, peer in enumerate((front, across, back)):
            copies.arrived(gall.at[wrap(x - 1 - step, NX)], gs.at[step], gr.at[step], peer)

    for name in ("wq", "gw", "ids", "beta", "pre", "rate", "mq", "mk", "mv"):
        reads[name].wait()
    gw[...] = jnp.broadcast_to(gw_row[...].astype(F32), (16, 2048)).astype(BF16)
    lanes = lax.broadcasted_iota(jnp.int32, (1, 128), 1)
    row = jnp.full((1, 128), -1, jnp.int32)
    for b in range(6):
        for p in range(4):
            each = jnp.broadcast_to(ids[p : p + 1, b : b + 1], (1, 128))
            row = jnp.where(lanes == each // 16, (b * 4 + p) * 16 + lax.rem(each, 16), row)
    tb[me] = row
    for step, peer in enumerate(peers):
        copies.start(tb.at[me], tb.at[me], hs.at[step], hr.at[step], peer)
    mx[...] = jnp.zeros((24, 128), F32)
    for b in range(6):
        for h in range(2):
            mx[b : b + 1, h * 64 : h * 64 + 64] = beta[h : h + 1, b * 64 : b * 64 + 64]
            mx[8 + b : 9 + b, h * 64 : h * 64 + 64] = pre[h : h + 1, b * 64 : b * 64 + 64]
    for h in range(2):
        mx[16:17, h * 64 : h * 64 + 64] = jnp.broadcast_to(rate[0:1, h : h + 1], (1, 64))
    decays, ends, stacked = mixer_rows(mx[...])
    cols = columns_of(stacked)
    work = (fresh, corr, att, qdec, kdec)

    def prepare(b):
        mixer_prepare(b, mq, mk, mv, decays, cols, *work)

    z_take(0, ca, 1)
    x_take(True)
    w_send()
    acc = project(x)
    prepare(0)
    y_take(0)
    z_take(0, ca, 2)
    x_take(False)
    for owner in (wrap(x - 1, NX), wrap(x + 1, NX)):
        more = project(owner)
        acc = (acc[0] + more[0], acc[1] + more[1])
    prepare(1)
    x_last()
    more = project(wrap(x + 2, NX))
    low = (acc[0] + more[0]).astype(BF16)
    gate = jax.nn.sigmoid(acc[1] + more[1])
    wide = low.astype(F32)
    scale = lax.rsqrt(jnp.mean(wide * wide, axis=-1, keepdims=True) + NORM_FLOOR)
    qlow[...] = low
    qa[pl.ds(me * 6, 6)] = (wide * scale).astype(BF16).reshape(6, 64, 256)
    own_send(1, qa)
    z_take(0, ca, 3)
    y_take(1)
    tl[me] = jnp.zeros((8, 128), F32)
    for b in range(6):
        tl[me, b : b + 1, 0:64] = gate[0:1, b * 64 : b * 64 + 64]
    gown[...] = tl[me]
    prepare(2)
    prepare(3)
    y_take(2)
    z_take(1, qa, 1)
    z_take(0, ca, 4)
    w_forward()
    y_take(3)
    z_take(1, qa, 2)
    for step, peer in enumerate(peers):
        copies.start(tl.at[me], tl.at[me], ts.at[step], tr.at[step], peer)
    w_share(0, wrap(x - 1, NX), 0)
    w_share(1, wrap(x + 1, NX), 3)
    prepare(4)
    z_take(1, qa, 3)
    w_share(2, wrap(x + 2, NX), 9)
    prepare(5)
    state = [jnp.zeros((128, 128), F32), jnp.zeros((128, 128), F32)]
    sums = jnp.zeros((128, 128), F32)
    for b in range(6):
        state, sums = mixer_advance(b, state, ca[me * 6 + b], ends, *work, sums)
    turned = jnp.transpose(sums)[0:8]
    md[...] = turned[:, 0:64] + turned[:, 64:128]
    w_last()
    z_take(1, qa, 4)
    for step in range(2 * NZ - 1):
        other = wrap(me - (step + 1), 2 * NZ)
        copies.arrived(tl.at[other], ts.at[step], tr.at[step], peers[step])
        copies.arrived(tb.at[other], hs.at[step], hr.at[step], peers[step])
    table = pltpu.make_async_copy(tb, tbs, ins.at[17])
    table.start()
    partner_take(0, ca)
    partner_take(1, qa)
    y_last()
    table.wait()

    gain = SCORE_GAIN * 256 ** (-0.5)
    line = lax.broadcasted_iota(jnp.int32, (8, 128), 0)

    def reader(r):
        tile = tl[r]
        stats = jnp.zeros((8, 128), F32)
        for yy in range(NY):
            entry = tbs[r, 0, (z * NY + yy) * 2 + c]
            used = entry >= 0
            safe = jnp.maximum(entry, 0)
            b, loc = safe // 64, lax.rem(safe, 16)
            keys_values = kv[yy * 16 + loc]
            scores = gain * lax.dot_general(
                keys_values[:, 0:256], qa[r * 6 + b], CONTRACT_LAST, preferred_element_type=F32
            )
            here = (line == b) & used
            gate = jnp.sum(jnp.where(line == b, tile, 0.0), axis=0, keepdims=True)
            grads = gate[:, 0:64] * lax.dot_general(
                keys_values[:, 256:512], ca[r * 6 + b], CONTRACT_LAST, preferred_element_type=F32
            )
            exps = jnp.exp(scores)
            both = jnp.concatenate([exps, grads], axis=1)
            eg[r * NY + yy] = both
            row = jnp.concatenate(
                [jnp.sum(exps, axis=0, keepdims=True), jnp.sum(exps * grads, axis=0, keepdims=True)], axis=1
            )
            stats = stats + jnp.where(here, row, 0.0)
        sent[r] = stats

    def outward(i, carry):
        near = (i + 1) // 2
        step = NZ + near - 2 * near * lax.rem(i, 2) - 1
        r = wrap(me + step + 1, 2 * NZ)
        reader(r)
        copies.make(
            sent.at[r], parts.at[step], ss.at[step], sr.at[step], {"st_0": r // 2, "st_2": lax.rem(r, 2)}
        ).start()
        return carry

    lax.fori_loop(0, 2 * NZ - 1, outward, 0)
    reader(me)
    whole = sent[me]
    for step in range(2 * NZ - 1):
        copies.arrived(parts.at[step], ss.at[step], sr.at[step], peers[step])
        whole = whole + parts[step]
    total[...] = whole
    tot[me] = whole
    own[...] = whole
    for step, peer in enumerate(peers):
        copies.start(total, tot.at[me], bs.at[step], br.at[step], peer)
    for step in range(2 * NZ - 1):
        other = wrap(me - (step + 1), 2 * NZ)
        copies.arrived(tot.at[other], bs.at[step], br.at[step], peers[step])
        copies.make(sent.at[0], parts.at[step], ss.at[step], sr.at[step], peers[step]).wait_send()
    copies.finish()


def grads_kernel(tb, kv, qa, ca, tl, eg, tot, kvg, qp, todo):
    z, c = lax.axis_index("st_0"), lax.axis_index("st_2")
    gain = SCORE_GAIN * 256 ** (-0.5)

    def entry_of(i):
        return tb[i // NY, 0, (z * NY + lax.rem(i, NY)) * 2 + c]

    def pick(i, count):
        todo[count] = i
        return count + (entry_of(i) >= 0).astype(jnp.int32)

    count = lax.fori_loop(0, 64, pick, 0, unroll=8)
    todo[count] = 0

    @pl.loop(0, 32)
    def _(i):
        blank = jnp.zeros((2, 64, 256), BF16)
        kvg[0, pl.ds(i * 2, 2)] = blank
        kvg[1, pl.ds(i * 2, 2)] = blank
        qp[pl.ds(i * 3, 3)] = jnp.zeros((3, 64, 256), BF16)

    @pl.loop(0, (count + 1) // 2)
    def _(pair):
        terms = []
        for u in range(2):
            i = todo[pair * 2 + u]
            live = (pair * 2 + u < count).astype(F32)
            entry = jnp.maximum(entry_of(i), 0)
            r, b = i // NY, entry // 64
            at, slot = r * 6 + b, lax.rem(i, NY) * 16 + lax.rem(entry, 16)
            row = tot[r, pl.ds(b, 1), :]
            gate = tl[r, pl.ds(b, 1), 0:64]
            norm = 1.0 / row[:, 0:64]
            both = eg[i]
            probs = both[:, 0:64] * (norm * live)
            slope = (probs * (both[:, 64:128] - row[:, 64:128] * norm)).astype(BF16)
            gated = (probs * gate).astype(BF16)
            key = gain * jnp.dot(slope, qa[at], preferred_element_type=F32)
            value = jnp.dot(gated, ca[at], preferred_element_type=F32)
            query = gain * lax.dot_general(
                slope, kv[slot, :, 0:256], CONTRACT_FIRST, preferred_element_type=F32
            )
            terms.append((at, slot, key, value, query))
        for at, slot, key, value, query in terms:
            kvg[0, slot] = (kvg[0, slot].astype(F32) + key).astype(BF16)
            kvg[1, slot] = (kvg[1, slot].astype(F32) + value).astype(BF16)
            qp[at] = (qp[at].astype(F32) + query).astype(BF16)


def finish_kernel(
    kvg, qp, klow, pas, qlow, wall, gall, own, md, gown,
    tgrad, pgrad, wgrad,
    ybuf, ysum, px, qs, zbuf, xall, pacc, tacc, xq, ggx, whalf, wget, wz, wbuf, wsum, wlast,
    ys, yr, zs, zr, ps, pr, xs, xr, qxs, qxr, gs, gr, us, ur, vs, vr, ls, lr,
):
    z, y, c, x = place()
    up, down = {"st_0": wrap(z + 1, NZ)}, {"st_0": wrap(z - 1, NZ)}
    east, west = {"st_1": wrap(y + 1, NY)}, {"st_1": wrap(y - 1, NY)}
    front, back, across = {"tp": wrap(x + 1, NX)}, {"tp": wrap(x - 1, NX)}, {"tp": wrap(x + 2, NX)}
    partner = {"st_2": 1 - c}
    spot = y * 2 + c
    plane = []
    for step in range(1, 8):
        other = wrap(spot + step, 8)
        plane.append({"st_1": other // 2, "st_2": lax.rem(other, 2)})
    greet([up, down, front, back, across] + plane)
    copies = Copies()
    zdirs, ydirs, xdirs = (up, down), (east, west), (front, back)

    far, beside = wrap(y + 2, NY), (wrap(y + 1, NY), wrap(y - 1, NY))

    def y_rows(j, part):
        return j // 4, pl.ds((j % 4) * 256 + part * 128, 128)

    def y_far(j):
        for way in (0, 1):
            p, at = y_rows(j, way)
            copies.start(kvg.at[p, far, at, :], ybuf.at[way, j], ys.at[0, way, j], yr.at[0, way, j], ydirs[way])

    def y_near(j):
        for way in (0, 1):
            p, at = y_rows(j, 1 - way)
            copies.start(
                kvg.at[p, beside[way], at, :], ysum.at[way, p, at, :], ys.at[1, way, j], yr.at[1, way, j], ydirs[way]
            )

    def y_add(j):
        for way in (0, 1):
            p, at = y_rows(j, way)
            copies.arrived(ybuf.at[way, j], ys.at[0, way, j], yr.at[0, way, j], ydirs[way])
            ybuf[way, j] = (kvg[p, beside[way], at, :].astype(F32) + ybuf[way, j].astype(F32)).astype(BF16)
            copies.start(ybuf.at[way, j], ysum.at[way, p, at, :], ys.at[2, way, j], yr.at[2, way, j], ydirs[way])
        if j + 1 < 8:
            y_near(j + 1)
        if j + 2 < 8:
            y_far(j + 2)

    def x_pieces(j, h):
        return j // 4, pl.ds((j % 4) * 256 + h * 128, 128)

    def y_done(j):
        for way in (0, 1):
            p, at = y_rows(j, 1 - way)
            copies.arrived(ysum.at[way, p, at, :], ys.at[1, way, j], yr.at[1, way, j], ydirs[way])
            p, at = y_rows(j, way)
            copies.arrived(ysum.at[way, p, at, :], ys.at[2, way, j], yr.at[2, way, j], ydirs[way])
        for h in (0, 1):
            p, at = x_pieces(j, h)
            grad = kvg[p, y, at, :].astype(F32) + ysum[0, p, at, :].astype(F32) + ysum[1, p, at, :].astype(F32)
            if p == 0:
                wide = klow[at, :].astype(F32)
                scale = lax.rsqrt(jnp.mean(wide * wide, axis=-1, keepdims=True) + NORM_FLOOR)
                inner = jnp.mean(wide * grad, axis=-1, keepdims=True)
                grad = scale * grad - (scale * scale * scale * inner) * wide
            xall[x, p, at, :] = grad.astype(BF16)
            for way in (0, 1):
                piece = xall.at[x, p, at, :]
                copies.start(piece, piece, xs.at[j, way, h], xr.at[j, way, h], xdirs[way])

    def x_take(j):
        for way in (0, 1):
            owner = wrap(x - 1 + 2 * way, NX)
            for h in (0, 1):
                p, at = x_pieces(j, h)
                piece = xall.at[owner, p, at, :]
                copies.arrived(piece, xs.at[j, way, h], xr.at[j, way, h], xdirs[way])
                if h == way:
                    copies.start(piece, piece, xs.at[j, way, 2], xr.at[j, way, 2], xdirs[way])

    def head_dot(rows, weight):
        return lax.dot_general(rows, weight, CONTRACT_LAST, preferred_element_type=F32)

    def x_near(j):
        p = j // 4

        @pl.loop(0, 2)
        def _(i):
            at = pl.ds(pl.multiple_of((j % 4) * 256 + i * 128, 128), 128)
            term = head_dot(xall[x, p, at, :], wall[p, x])
            for owner in (wrap(x - 1, NX), wrap(x + 1, NX)):
                term += head_dot(xall[owner, p, at, :], wall[p, owner])
            pacc[at, :] = term if p == 0 else pacc[at, :] + term

    def x_last(j):
        owner = wrap(x + 2, NX)
        for way in (0, 1):
            p, at = x_pieces(j, way)
            copies.arrived(xall.at[owner, p, at, :], xs.at[j, way, 2], xr.at[j, way, 2], xdirs[way])
        p = j // 4

        @pl.loop(0, 2)
        def _(i):
            at = pl.ds(pl.multiple_of((j % 4) * 256 + i * 128, 128), 128)
            term = pacc[at, :] + head_dot(xall[owner, p, at, :], wall[p, owner])
            if p == 0:
                pacc[at, :] = term
            else:
                pgrad[at, :] = term.astype(BF16)

    def ring_step(d, value, slots, send, recv, half):
        for way in (0, 1):
            there = wrap(z + d, NZ) if way == 0 else wrap(z - d, NZ)
            at = pl.ds(way * half, half)
            if d == 3:
                copies.arrived(slots.at[way, 0, at, :], send.at[way, 3], recv.at[way, 3], zdirs[way])
                value[there, at, :] = (value[there, at, :].astype(F32) + slots[way, 0, at, :].astype(F32)).astype(BF16)
            elif d < 3:
                copies.arrived(slots.at[way, 3 - d], send.at[way, d], recv.at[way, d], zdirs[way])
                value[there] = (value[there].astype(F32) + slots[way, 3 - d].astype(F32)).astype(BF16)
            if d == 4:
                copies.start(value.at[there, at, :], slots.at[way, 0, at, :], send.at[way, 3], recv.at[way, 3], zdirs[way])
            else:
                copies.start(value.at[there], slots.at[way, 4 - d], send.at[way, d - 1], recv.at[way, d - 1], zdirs[way])

    def ring_last(value, slots, send, recv):
        result = value[z].astype(F32)
        for way in (0, 1):
            copies.arrived(slots.at[way, 3], send.at[way, 0], recv.at[way, 0], zdirs[way])
            result = result + slots[way, 3].astype(F32)
        return result

    def q_pair(k):
        there = wrap(z + k, NZ)
        copies.arrived(px.at[there], ps.at[k], pr.at[k], partner)
        qs[there] = (qp[there * 2 + c].astype(F32) + px[there].astype(F32)).astype(BF16)

    def q_step(d):
        ring_step(d, qs, zbuf, zs, zr, 192)

    def q_done():
        grad = ring_last(qs, zbuf, zs, zr)
        wide = qlow[...].astype(F32)
        scale = lax.rsqrt(jnp.mean(wide * wide, axis=-1, keepdims=True) + NORM_FLOOR)
        inner = jnp.mean(wide * grad, axis=-1, keepdims=True)
        xq[x] = (scale * grad - (scale * scale * scale * inner) * wide).astype(BF16)
        for way in (0, 1):
            for h in (0, 1):
                piece = xq.at[x, pl.ds(h * 192, 192), :]
                copies.start(piece, piece, qxs.at[way, h], qxr.at[way, h], xdirs[way])

    def gates():
        gate = gown[0:6, 0:64]
        dots = own[0:6, 64:128] / own[0:6, 0:64]
        ggx[x] = jnp.zeros((8, 128), F32)
        ggx[x, 0:6, 0:64] = (1.0 - gate) * (dots - gate * md[0:6, :])
        for step, peer in enumerate((front, across, back)):
            copies.start(ggx.at[x], ggx.at[x], gs.at[step], gr.at[step], peer)

    def q_take():
        for way in (0, 1):
            owner = wrap(x - 1 + 2 * way, NX)
            for h in (0, 1):
                piece = xq.at[owner, pl.ds(h * 192, 192), :]
                copies.arrived(piece, qxs.at[way, h], qxr.at[way, h], xdirs[way])
                if h == way:
                    copies.start(piece, piece, qxs.at[way, 2], qxr.at[way, 2], xdirs[way])

    def q_last():
        owner = wrap(x + 2, NX)
        for way in (0, 1):
            copies.arrived(xq.at[owner, pl.ds(way * 192, 192), :], qxs.at[way, 2], qxr.at[way, 2], xdirs[way])
        for b in range(6):
            at = pl.ds(b * 64, 64)
            tgrad[at, :] = (tacc[at, :] + head_dot(xq[owner, at, :], wall[2, owner])).astype(BF16)

    def q_near():
        for step, peer in enumerate((front, across, back)):
            copies.arrived(ggx.at[wrap(x - 1 - step, NX)], gs.at[step], gr.at[step], peer)
        blank = [jnp.zeros((4, 64), F32)]
        slope = jnp.concatenate(
            [gall[h, 0:1, :].astype(F32) for h in range(NX)] + [jnp.zeros((4, 512), F32)], axis=0
        )
        for b in range(6):
            at = pl.ds(b * 64, 64)
            rows = jnp.concatenate([ggx[h, b : b + 1, 0:64] for h in range(NX)] + blank, axis=0)
            term = lax.dot_general(
                rows, slope, CONTRACT_FIRST, preferred_element_type=F32, precision=lax.Precision.HIGHEST
            )
            for owner in (x, wrap(x - 1, NX), wrap(x + 1, NX)):
                term += head_dot(xq[owner, at, :], wall[2, owner])
            tacc[at, :] = term

    keep = pl.ds(pl.multiple_of(c * 128, 128), 128)
    give = pl.ds(pl.multiple_of((1 - c) * 128, 128), 128)

    def w_tile(k):
        there = wrap(z + k, NZ)
        at = pl.ds(pl.multiple_of(there * 256, 256), 256)
        wsum[there] = lax.dot_general(
            pas[:, at], xall[x, 0], CONTRACT_FIRST, preferred_element_type=F32
        )
        whalf[there] = wsum[there, :, give]
        copies.start(whalf.at[there], wget.at[there], us.at[k], ur.at[k], partner)

    def w_pair(k):
        there = wrap(z + k, NZ)
        copies.arrived(wget.at[there], us.at[k], ur.at[k], partner)
        wz[there] = (wsum[there, :, keep] + wget[there]).astype(BF16)

    def w_step(d):
        ring_step(d, wz, wbuf, vs, vr, 128)

    def w_done():
        wsum[z, :, 0:128] = ring_last(wz, wbuf, vs, vr)
        for step, peer in enumerate(plane):
            other = wrap(spot + step + 1, 8)
            piece = wsum.at[z, pl.ds(pl.multiple_of(other * 32, 32), 32), pl.ds(0, 128)]
            copies.start(piece, wlast.at[spot], ls.at[step], lr.at[step], peer)
        wlast[spot] = wsum[z, pl.ds(pl.multiple_of(spot * 32, 32), 32), 0:128]

    def w_last():
        for step, peer in enumerate(plane):
            copies.arrived(wlast.at[wrap(spot - step - 1, 8)], ls.at[step], lr.at[step], peer)
        for k in (0, 1):
            wgrad[:, k * 128 : k * 128 + 128] = wlast[k] + wlast[2 + k] + wlast[4 + k] + wlast[6 + k]

    y_far(0)
    y_near(0)
    y_far(1)
    for k in (4, 3, 5, 2, 6, 1, 7, 0):
        there = wrap(z + k, NZ)
        copies.start(qp.at[there * 2 + 1 - c], px.at[there], ps.at[k], pr.at[k], partner)
    q_pair(4)
    q_step(4)
    q_pair(3)
    q_pair(5)
    y_add(0)
    for k in (2, 6, 1, 7, 0):
        q_pair(k)
    gates()
    y_add(1)
    q_step(3)
    y_done(0)
    y_add(2)
    y_done(1)
    q_step(2)
    x_take(0)
    y_add(3)
    y_done(2)
    x_take(1)
    y_add(4)
    y_done(3)
    q_step(1)
    x_near(0)
    x_last(0)
    for k in (4, 3, 5):
        w_tile(k)
    x_take(2)
    y_add(5)
    y_done(4)
    x_near(1)
    x_last(1)
    x_take(3)
    for k in (2, 6, 1, 7, 0):
        w_tile(k)
    y_add(6)
    q_done()
    y_done(5)
    w_pair(4)
    w_step(4)
    y_add(7)
    y_done(6)
    x_take(4)
    w_pair(3)
    w_pair(5)
    w_step(3)
    y_done(7)
    x_near(2)
    x_last(2)
    q_take()
    x_take(5)
    for k in (2, 6, 1, 7, 0):
        w_pair(k)
    w_step(2)
    x_near(3)
    x_last(3)
    x_near(4)
    x_take(6)
    w_step(1)
    q_near()
    x_last(4)
    x_near(5)
    x_take(7)
    w_done()
    x_near(6)
    x_near(7)
    q_last()
    x_last(5)
    w_last()
    x_last(6)
    x_last(7)
    copies.finish()


def store_kernel(tgrad, pgrad, wgrad, tokens, rows, weights, sems):
    pairs = ((pgrad, rows), (tgrad, tokens), (wgrad, weights))
    copies = [pltpu.make_async_copy(src, dst, sems.at[i]) for i, (src, dst) in enumerate(pairs)]
    for copy in copies:
        copy.start()
    for copy in copies:
        copy.wait()


def shaped(shape, dtype):
    return jax.ShapeDtypeStruct(shape, dtype)


def dma(*shape):
    return pltpu.SemaphoreType.DMA(shape)


def call(kernel, outs, scratch, collective, smem=0, limit=48, count=0, space=VMEM, out_space=VMEM, **extra):
    in_specs = [pl.BlockSpec(memory_space=pltpu.SMEM)] * smem + [pl.BlockSpec(memory_space=space)] * (count - smem)
    params = dict(vmem_limit_bytes=limit * 2**20)
    if collective is not None:
        params.update(collective_id=collective, has_side_effects=True)
    return pl.pallas_call(
        kernel,
        out_shape=outs,
        in_specs=in_specs,
        out_specs=[pl.BlockSpec(memory_space=out_space)] * len(outs),
        scratch_shapes=scratch,
        compiler_params=pltpu.CompilerParams(**params),
        **extra,
    )


def body(
    tokens, cotangent, mix_query, mix_key, mix_value, beta_pre, decay_pre, decay_rate,
    passages, passage_ids, query_weight, key_weight, value_weight, gate_weight,
):
    pass_local, span_rows, model_width = passages.shape
    flat_rows = passages.reshape(pass_local * span_rows, model_width)
    kv, qa, ca, tl, lookup, key_low, query_low, gown, wall, gall, md, eg, tot, own = call(
        gather_kernel,
        [
            shaped((64, 64, 512), BF16), shaped((96, 64, 256), BF16), shaped((96, 64, 256), BF16),
            shaped((16, 8, 128), F32), shaped((16, 1, 128), jnp.int32), shaped((1024, 256), BF16), shaped((384, 256), BF16), shaped((8, 128), F32),
            shaped((3, NX, 512, 256), BF16), shaped((NX, 16, 512), BF16), shaped((8, 64), F32),
            shaped((64, 64, 128), F32), shaped((16, 8, 128), F32), shaped((8, 128), F32),
        ],
        [
            pltpu.SMEM((16, 1, 128), jnp.int32), VMEM((16, 8, 128), F32), VMEM((15, 8, 128), F32), VMEM((8, 128), F32),
            dma(15), dma(15), dma(15), dma(15),
            VMEM((1024, 2048), BF16), VMEM((2048, 256), BF16), VMEM((2048, 256), BF16), VMEM((2048, 256), BF16),
            VMEM((384, 256), BF16), VMEM((384, 256), BF16), VMEM((384, 256), BF16), VMEM((1, 2048), BF16),
            VMEM((4, 6), jnp.int32), VMEM((2, 384), F32), VMEM((2, 384), F32), VMEM((1, 2), F32),
            VMEM((16, 2048), BF16), VMEM((24, 128), F32),
            VMEM((NX, 384, 512), BF16), VMEM((3, 256, 256), BF16), VMEM((6, 128, 128), F32),
            VMEM((6, 128, 128), BF16), VMEM((6, 128, 128), BF16), VMEM((6, 128, 128), BF16), VMEM((6, 128, 128), BF16),
            dma(18), dma(15), dma(15), dma(2, 3), dma(2, 3), dma(2, 6), dma(2, 6), dma(2, 2, 7), dma(2, 2, 7),
            dma(2, 16), dma(2, 16), dma(15), dma(15), dma(12), dma(12), dma(9), dma(9), dma(3), dma(3),
        ],
        1, count=14, limit=LIMITS[0], space=pltpu.HBM,
    )(*[pltpu.with_memory_space_constraint(a, pltpu.HBM) for a in (
        flat_rows, key_weight, value_weight, tokens, query_weight, gate_weight, cotangent.reshape(6, 64, 256),
        mix_query, mix_key, mix_value, passage_ids.T, beta_pre, decay_pre, decay_rate[None, :],
    )])
    kvg, qp = call(
        grads_kernel,
        [shaped((2, 64, 64, 256), BF16), shaped((96, 64, 256), BF16)],
        [pltpu.SMEM((66,), jnp.int32)],
        None, smem=1, count=7, limit=LIMITS[1],
    )(lookup, kv, qa, ca, tl, eg, tot)
    token_grad, passage_grad, key_weight_grad = call(
        finish_kernel,
        [shaped((384, 512), BF16), shaped((1024, 512), BF16), shaped((32, 256), F32)],
        [
            VMEM((2, 8, 128, 256), BF16), VMEM((2, 2, 1024, 256), BF16), VMEM((NZ, 384, 256), BF16),
            VMEM((NZ, 384, 256), BF16), VMEM((2, 4, 384, 256), BF16), VMEM((NX, 2, 1024, 256), BF16),
            VMEM((1024, 512), F32), VMEM((384, 512), F32), VMEM((NX, 384, 256), BF16), VMEM((NX, 8, 128), F32),
            VMEM((NZ, 256, 128), F32), VMEM((NZ, 256, 128), F32), VMEM((NZ, 256, 128), BF16),
            VMEM((2, 4, 256, 128), BF16), VMEM((NZ, 256, 256), F32), VMEM((8, 32, 128), F32),
            dma(3, 2, 8), dma(3, 2, 8), dma(2, 4), dma(2, 4), dma(8), dma(8), dma(8, 2, 3), dma(8, 2, 3),
            dma(2, 3), dma(2, 3), dma(3), dma(3), dma(8), dma(8), dma(2, 4), dma(2, 4), dma(7), dma(7),
        ],
        3, count=10, limit=LIMITS[2],
    )(
        kvg.reshape(2, NY, 1024, 256), qp.reshape(16, 384, 256), key_low, flat_rows, query_low,
        wall, gall, own, md, gown,
    )
    token_grad, passage_grad, key_weight_grad = call(
        store_kernel,
        [shaped((384, 512), BF16), shaped((1024, 512), BF16), shaped((32, 256), F32)],
        [dma(3)],
        None, count=3, limit=4, out_space=pltpu.HBM,
    )(token_grad, passage_grad, key_weight_grad)
    return (token_grad, passage_grad.reshape(pass_local, span_rows, 512), key_weight_grad)


def solution(mesh):
    torus = Mesh(mesh.devices.reshape(8, 4, 2, mesh.shape["tp"]), ("st_0", "st_1", "st_2", "tp"))
    return jax.shard_map(
        body,
        mesh=torus,
        in_specs=(
            P(ST, "tp"),
            P(ST, "tp"),
            P(ST, "tp"),
            P(ST, "tp"),
            P(ST, "tp"),
            P("tp", ST),
            P("tp", ST),
            P("tp"),
            P(ST, None, None),
            P(ST, None),
            P(None, "tp"),
            P(None, "tp"),
            P(None, "tp"),
            P("tp", None),
        ),
        out_specs=(P(ST, "tp"), P(ST, None, "tp"), P(ST, "tp")),
        check_vma=False,
    )
```

```python
import functools

import jax
import jax.numpy as jnp
from jax import lax
from jax.experimental import pallas as pl
from jax.experimental.pallas import tpu as pltpu
from jax.sharding import Mesh
from jax.sharding import PartitionSpec as P

SPAN = 64
ST = ("st_0", "st_1", "st_2")
MESH = pl.DeviceIdType.MESH
NZ, NY, NX = 8, 4, 4
VMEM = pltpu.VMEM
F32, BF16 = jnp.float32, jnp.bfloat16
LIMITS = (22, 6, 24)

NORM_FLOOR = 1.0
SCORE_GAIN = 4.0
CONTRACT_LAST = (((1,), (1,)), ((), ()))
CONTRACT_FIRST = (((0,), (0,)), ((), ()))


def place():
    return (lax.axis_index("st_0"), lax.axis_index("st_1"), lax.axis_index("st_2"), lax.axis_index("tp"))


def wrap(value, size):
    return lax.rem(value + size, size)


class Copies:
    def __init__(self):
        self.started = []

    def make(self, src, dst, send, recv, where):
        return pltpu.make_async_remote_copy(
            src_ref=src, dst_ref=dst, send_sem=send, recv_sem=recv, device_id=where, device_id_type=MESH
        )

    def start(self, src, dst, send, recv, where):
        copy = self.make(src, dst, send, recv, where)
        copy.start()
        self.started.append(copy)

    def arrived(self, dst, send, recv, where):
        self.make(dst, dst, send, recv, where).wait_recv()

    def finish(self):
        for copy in self.started:
            copy.wait_send()


def greet(peers, meanwhile=None):
    barrier = pltpu.get_barrier_semaphore()
    for peer in peers:
        pl.semaphore_signal(barrier, inc=1, device_id=peer, device_id_type=MESH)
    if meanwhile is not None:
        meanwhile()
    pl.semaphore_wait(barrier, len(peers))


def column_peers(z, c):
    me = z * 2 + c
    peers = []
    for step in range(1, 2 * NZ):
        other = wrap(me + step, 2 * NZ)
        peers.append({"st_0": other // 2, "st_2": lax.rem(other, 2)})
    return peers


def columns_of(rows):
    return jnp.transpose(rows)


def mixer_rows(mx):
    strength = jax.nn.sigmoid(mx[0:8])
    pre = mx[8:16]
    log_decay = -mx[16:17] * (jnp.maximum(pre, 0.0) + jnp.log1p(jnp.exp(-jnp.abs(pre))))
    lane = lax.broadcasted_iota(jnp.int32, (8, 128), 1)
    inner = lax.rem(lane, SPAN)
    total = log_decay
    for shift in (1, 2, 4, 8, 16, 32):
        total = total + jnp.where(inner >= shift, pltpu.roll(total, shift, axis=1), 0.0)
    ends = [
        jnp.sum(jnp.where(lane == at, total, 0.0), axis=1, keepdims=True) for at in (SPAN - 1, 2 * SPAN - 1)
    ]
    last = jnp.where(lane < SPAN, ends[0], ends[1])
    grown = jnp.exp(total)
    stacked = jnp.concatenate([strength, total, strength * grown, grown, jnp.exp(last - total)], axis=0)
    return total, ends, stacked


def low_dot(a, b, dims=(((1,), (0,)), ((), ()))):
    return lax.dot_general(a.astype(BF16), b.astype(BF16), dims, preferred_element_type=F32)


def mixer_prepare(b, mq, mk, mv, total, cols, fresh, corr, att, qdec, kdec):
    at = slice(b * SPAN, (b + 1) * SPAN)

    def both(ref):
        return jnp.concatenate([ref[at, 0:128], ref[at, 128:256]], axis=0).astype(F32)

    def unit(value):
        return value * lax.rsqrt(jnp.sum(value * value, axis=-1, keepdims=True) + NORM_FLOOR)

    def column(k):
        return cols[:, k * 8 + b : k * 8 + b + 1]

    queries, keys, values = unit(both(mq)) * 128 ** (-0.5), unit(both(mk)), both(mv)
    row, col = lax.broadcasted_iota(jnp.int32, (128, 128), 0), lax.broadcasted_iota(jnp.int32, (128, 128), 1)
    same = (row // SPAN) == (col // SPAN)
    spread = jnp.where(same & (row >= col), column(1) - total[b : b + 1, :], -1e30)
    decay = jnp.exp(spread)
    strict = jnp.where(same & (row > col), column(0) * low_dot(keys, keys, CONTRACT_LAST) * decay, 0.0)
    inverse = jnp.where(row == col, 1.0, 0.0) - strict
    power = strict
    for _ in range(SPAN.bit_length() - 2):
        power = low_dot(power, power)
        inverse = inverse + low_dot(inverse, power)
    fresh[b] = low_dot(inverse, values * column(0))
    corr[b] = low_dot(inverse, keys * column(2)).astype(BF16)
    att[b] = (low_dot(queries, keys, CONTRACT_LAST) * decay).astype(BF16)
    qdec[b] = (queries * column(3)).astype(BF16)
    kdec[b] = (keys * column(4)).astype(BF16)


def mixer_advance(b, state, grads, ends, fresh, corr, att, qdec, kdec, sums):
    heads = [slice(0, 64), slice(64, 128)]
    new = jnp.concatenate(
        [fresh[b, h, :] - low_dot(corr[b, h, :], state[i]) for i, h in enumerate(heads)], axis=0
    )
    out = jnp.concatenate([low_dot(qdec[b, h, :], state[i]) for i, h in enumerate(heads)], axis=0)
    out = out + low_dot(att[b], new)
    state = [
        jnp.exp(ends[i][b : b + 1, :]) * state[i] + low_dot(kdec[b, h, :], new[h], CONTRACT_FIRST)
        for i, h in enumerate(heads)
    ]
    grads = jnp.concatenate([grads[:, 0:128], grads[:, 128:256]], axis=0).astype(F32)
    lane = lax.broadcasted_iota(jnp.int32, (128, 128), 1)
    sums = jnp.where(lane == b, jnp.sum(grads * out, axis=-1, keepdims=True), sums)
    return state, sums


def gather_kernel(
    pas_in, wk_in, wv_in, tok_in, wq_in, gw_in, cot_in, mq_in, mk_in, mv_in, ids_in, beta_in, pre_in, rate_in,
    kv, qa, ca, tl, tb, klow, qlow, gown, wall, gall, md, eg, tot, own,
    tbs, sent, parts, total, ss, sr, bs, br,
    pas, wk, wv, wq, mq, mk, mv, gw_row, ids, beta, pre, rate, gw, mx,
    toks, relay, fresh, corr, att, qdec, kdec,
    ins, hs, hr, xs, xr, ys, yr, zs, zr, ps, pr, ts, tr, ws, wr, vs, vr, gs, gr,
):
    z, y, c, x = place()
    me = z * 2 + c
    up, down = {"st_0": wrap(z + 1, NZ)}, {"st_0": wrap(z - 1, NZ)}
    east, west = {"st_1": wrap(y + 1, NY)}, {"st_1": wrap(y - 1, NY)}
    front, back = {"tp": wrap(x + 1, NX)}, {"tp": wrap(x - 1, NX)}
    partner = {"st_2": 1 - c}
    peers = column_peers(z, c)
    across = {"tp": wrap(x + 2, NX)}
    reads = {}

    def fetch(name, src, dst):
        reads[name] = pltpu.make_async_copy(src, dst, ins.at[len(reads)])
        reads[name].start()

    fetch("tok", tok_in, toks.at[x])
    fetch("cot", cot_in, ca.at[pl.ds(me * 6, 6)])
    fetch("wk", wk_in, wk)
    fetch("wv", wv_in, wv)
    for i in range(4):
        fetch(f"pas{i}", pas_in.at[pl.ds(i * 256, 256), :], pas.at[pl.ds(i * 256, 256), :])
    fetch("wq", wq_in, wq)
    for name, src, dst in (
        ("gw", gw_in, gw_row), ("ids", ids_in, ids), ("beta", beta_in, beta), ("pre", pre_in, pre),
        ("rate", rate_in, rate), ("mq", mq_in, mq), ("mk", mk_in, mk), ("mv", mv_in, mv),
    ):
        fetch(name, src, dst)
    rows = 256

    def project_passages():
        reads["wk"].wait()
        reads["wv"].wait()
        for i in range(4):
            reads[f"pas{i}"].wait()
            block = pas[pl.ds(i * rows, rows), :]
            low = jnp.dot(block, wk[...], preferred_element_type=F32).astype(BF16)
            wide = low.astype(F32)
            scale = lax.rsqrt(jnp.mean(wide * wide, axis=-1, keepdims=True) + NORM_FLOOR)
            klow[pl.ds(i * rows, rows), :] = low
            kv[pl.ds(y * 16 + i * 4, 4), :, 0:256] = (wide * scale).astype(BF16).reshape(4, 64, 256)
            value = jnp.dot(block, wv[...], preferred_element_type=F32)
            kv[pl.ds(y * 16 + i * 4, 4), :, 256:512] = value.astype(BF16).reshape(4, 64, 256)

    greet(peers + [east, west, front, back, across], project_passages)
    copies = Copies()
    half = 192
    zdirs, ydirs, xdirs = (up, down), (east, west), (front, back)

    def token_rows(slot, h):
        return toks.at[slot, pl.ds(h * half, half), :]

    def rows_of(ref, slot, h):
        return ref.at[pl.ds(slot * 6 + h * 3, 3)]

    def z_send(k, ref, d, h):
        for way in (0, 1):
            if d == 4 and h != way:
                continue
            owner = wrap(z - (d - 1), NZ) if way == 0 else wrap(z + (d - 1), NZ)
            piece = rows_of(ref, owner * 2 + c, h)
            at = (d - 1) * 2 + h if d < 4 else 6
            copies.start(piece, piece, zs.at[k, way, at], zr.at[k, way, at], zdirs[way])

    def z_take(k, ref, d):
        for h in (0, 1):
            for way in (0, 1):
                if d == 4 and h != way:
                    continue
                owner = wrap(z - d, NZ) if way == 0 else wrap(z + d, NZ)
                piece = rows_of(ref, owner * 2 + c, h)
                at = (d - 1) * 2 + h if d < 4 else 6
                copies.arrived(piece, zs.at[k, way, at], zr.at[k, way, at], zdirs[way])
                if d < 3 or (d == 3 and h == way):
                    nxt = d * 2 + h if d < 3 else 6
                    copies.start(piece, piece, zs.at[k, way, nxt], zr.at[k, way, nxt], zdirs[way])
                to = 2 + way * 7 + at
                copies.start(piece, piece, ps.at[k, to], pr.at[k, to], partner)

    def own_send(k, ref):
        for h in (0, 1):
            z_send(k, ref, 1, h)
        for h in (0, 1):
            piece = rows_of(ref, me, h)
            copies.start(piece, piece, ps.at[k, h], pr.at[k, h], partner)

    def partner_take(k, ref):
        theirs = 1 - c
        for h in (0, 1):
            piece = rows_of(ref, z * 2 + theirs, h)
            copies.arrived(piece, ps.at[k, h], pr.at[k, h], partner)
        for d in (1, 2, 3, 4):
            for h in (0, 1):
                for way in (0, 1):
                    if d == 4 and h != way:
                        continue
                    owner = wrap(z - d, NZ) if way == 0 else wrap(z + d, NZ)
                    to = 2 + way * 7 + ((d - 1) * 2 + h if d < 4 else 6)
                    piece = rows_of(ref, owner * 2 + theirs, h)
                    copies.arrived(piece, ps.at[k, to], pr.at[k, to], partner)

    reads["tok"].wait()
    for way, h in ((0, 0), (1, 1), (0, 1), (1, 0)):
        piece = token_rows(x, h)
        copies.start(piece, piece, xs.at[way, h], xr.at[way, h], xdirs[way])
    reads["cot"].wait()
    own_send(0, ca)

    def kv_rows(i):
        return kv.at[pl.ds(y * 16 + i * 4, 4)]

    for i in range(4):
        for way in (0, 1):
            copies.start(kv_rows(i), kv_rows(i), ys.at[way, i], yr.at[way, i], ydirs[way])

    def y_take(i):
        for way in (0, 1):
            owner = wrap(y - 1, NY) if way == 0 else wrap(y + 1, NY)
            piece = kv.at[pl.ds(owner * 16 + i * 4, 4)]
            copies.arrived(piece, ys.at[way, i], yr.at[way, i], ydirs[way])
            if i % 2 == way:
                at = 4 + i // 2
                copies.start(piece, piece, ys.at[way, at], yr.at[way, at], ydirs[way])

    def y_last():
        owner = wrap(y + 2, NY)
        for i in range(4):
            way, at = i % 2, 4 + i // 2
            piece = kv.at[pl.ds(owner * 16 + i * 4, 4)]
            copies.arrived(piece, ys.at[way, at], yr.at[way, at], ydirs[way])

    def x_take(first):
        for way in (0, 1):
            owner = wrap(x - 1, NX) if way == 0 else wrap(x + 1, NX)
            h = way if first else 1 - way
            piece = token_rows(owner, h)
            copies.arrived(piece, xs.at[way, h], xr.at[way, h], xdirs[way])
            if first:
                copies.start(piece, piece, xs.at[way, 2], xr.at[way, 2], xdirs[way])

    def x_last():
        owner = wrap(x + 2, NX)
        for way in (0, 1):
            piece = token_rows(owner, way)
            copies.arrived(piece, xs.at[way, 2], xr.at[way, 2], xdirs[way])

    def project(owner):
        block = toks[owner]
        at = pl.ds(pl.multiple_of(owner * 512, 512), 512)
        return (
            jnp.dot(block, wq[at, :], preferred_element_type=F32),
            lax.dot_general(gw[:, at], block, CONTRACT_LAST, preferred_element_type=F32),
        )

    weights = (wk, wv, wq)
    via, behind = {"tp": wrap(x + 1 - 2 * c, NX)}, wrap(x - 1 + 2 * c, NX)

    def w_rows(owner):
        return pl.ds(pl.multiple_of(owner * 512 + c * 256, 256), 256)

    mine = pl.ds(pl.multiple_of(c * 256, 256), 256)

    def w_send():
        for i, ref in enumerate(weights):
            copies.start(ref.at[w_rows(wrap(x + 2, NX)), :], relay.at[i], ws.at[6 + i], wr.at[6 + i], via)
        for way in (0, 1):
            to = wrap(x + 1 - 2 * way, NX)
            for i, ref in enumerate(weights):
                copies.start(
                    ref.at[w_rows(to), :], wall.at[i, x, mine, :], ws.at[way * 3 + i], wr.at[way * 3 + i], xdirs[way]
                )
        for step, peer in enumerate((front, across, back)):
            at = pl.ds(pl.multiple_of(wrap(x + 1 + step, NX) * 512, 512), 512)
            copies.start(gw.at[:, at], gall.at[x], gs.at[step], gr.at[step], peer)
        own = pl.ds(pl.multiple_of(x * 512, 512), 512)
        for i, ref in enumerate(weights):
            wall[i, x] = ref[own, :]
        gall[x] = gw[:, own]

    def w_forward():
        for i in range(3):
            copies.arrived(relay.at[i], ws.at[6 + i], wr.at[6 + i], via)
            copies.start(relay.at[i], wall.at[i, behind, mine, :], ws.at[9 + i], wr.at[9 + i], via)

    def w_share(n, owner, first):
        for i in range(3):
            piece = wall.at[i, owner, mine, :]
            copies.arrived(piece, ws.at[first + i], wr.at[first + i], via)
            copies.start(piece, piece, vs.at[n * 3 + i], vr.at[n * 3 + i], partner)

    def w_last():
        theirs = pl.ds(pl.multiple_of((1 - c) * 256, 256), 256)
        for n, owner in enumerate((wrap(x - 1, NX), wrap(x + 1, NX), wrap(x + 2, NX))):
            for i in range(3):
                copies.arrived(wall.at[i, owner, theirs, :], vs.at[n * 3 + i], vr.at[n * 3 + i], partner)
        for step, peer in enumerate((front, across, back)):
            copies.arrived(gall.at[wrap(x - 1 - step, NX)], gs.at[step], gr.at[step], peer)

    for name in ("wq", "gw", "ids", "beta", "pre", "rate", "mq", "mk", "mv"):
        reads[name].wait()
    gw[...] = jnp.broadcast_to(gw_row[...].astype(F32), (16, 2048)).astype(BF16)
    lanes = lax.broadcasted_iota(jnp.int32, (1, 128), 1)
    row = jnp.full((1, 128), -1, jnp.int32)
    for b in range(6):
        for p in range(4):
            each = jnp.broadcast_to(ids[p : p + 1, b : b + 1], (1, 128))
            row = jnp.where(lanes == each // 16, (b * 4 + p) * 16 + lax.rem(each, 16), row)
    tb[me] = row
    for step, peer in enumerate(peers):
        copies.start(tb.at[me], tb.at[me], hs.at[step], hr.at[step], peer)
    mx[...] = jnp.zeros((24, 128), F32)
    for b in range(6):
        for h in range(2):
            mx[b : b + 1, h * 64 : h * 64 + 64] = beta[h : h + 1, b * 64 : b * 64 + 64]
            mx[8 + b : 9 + b, h * 64 : h * 64 + 64] = pre[h : h + 1, b * 64 : b * 64 + 64]
    for h in range(2):
        mx[16:17, h * 64 : h * 64 + 64] = jnp.broadcast_to(rate[0:1, h : h + 1], (1, 64))
    decays, ends, stacked = mixer_rows(mx[...])
    cols = columns_of(stacked)
    work = (fresh, corr, att, qdec, kdec)

    def prepare(b):
        mixer_prepare(b, mq, mk, mv, decays, cols, *work)

    z_take(0, ca, 1)
    x_take(True)
    w_send()
    acc = project(x)
    prepare(0)
    y_take(0)
    z_take(0, ca, 2)
    x_take(False)
    for owner in (wrap(x - 1, NX), wrap(x + 1, NX)):
        more = project(owner)
        acc = (acc[0] + more[0], acc[1] + more[1])
    prepare(1)
    x_last()
    more = project(wrap(x + 2, NX))
    low = (acc[0] + more[0]).astype(BF16)
    gate = jax.nn.sigmoid(acc[1] + more[1])
    wide = low.astype(F32)
    scale = lax.rsqrt(jnp.mean(wide * wide, axis=-1, keepdims=True) + NORM_FLOOR)
    qlow[...] = low
    qa[pl.ds(me * 6, 6)] = (wide * scale).astype(BF16).reshape(6, 64, 256)
    own_send(1, qa)
    z_take(0, ca, 3)
    y_take(1)
    tl[me] = jnp.zeros((8, 128), F32)
    for b in range(6):
        tl[me, b : b + 1, 0:64] = gate[0:1, b * 64 : b * 64 + 64]
    gown[...] = tl[me]
    prepare(2)
    prepare(3)
    y_take(2)
    z_take(1, qa, 1)
    z_take(0, ca, 4)
    w_forward()
    y_take(3)
    z_take(1, qa, 2)
    for step, peer in enumerate(peers):
        copies.start(tl.at[me], tl.at[me], ts.at[step], tr.at[step], peer)
    w_share(0, wrap(x - 1, NX), 0)
    w_share(1, wrap(x + 1, NX), 3)
    prepare(4)
    z_take(1, qa, 3)
    w_share(2, wrap(x + 2, NX), 9)
    prepare(5)
    state = [jnp.zeros((128, 128), F32), jnp.zeros((128, 128), F32)]
    sums = jnp.zeros((128, 128), F32)
    for b in range(6):
        state, sums = mixer_advance(b, state, ca[me * 6 + b], ends, *work, sums)
    turned = jnp.transpose(sums)[0:8]
    md[...] = turned[:, 0:64] + turned[:, 64:128]
    w_last()
    z_take(1, qa, 4)
    for step in range(2 * NZ - 1):
        other = wrap(me - (step + 1), 2 * NZ)
        copies.arrived(tl.at[other], ts.at[step], tr.at[step], peers[step])
        copies.arrived(tb.at[other], hs.at[step], hr.at[step], peers[step])
    table = pltpu.make_async_copy(tb, tbs, ins.at[17])
    table.start()
    partner_take(0, ca)
    partner_take(1, qa)
    y_last()
    table.wait()

    gain = SCORE_GAIN * 256 ** (-0.5)
    line = lax.broadcasted_iota(jnp.int32, (8, 128), 0)

    def reader(r):
        tile = tl[r]
        stats = jnp.zeros((8, 128), F32)
        for yy in range(NY):
            entry = tbs[r, 0, (z * NY + yy) * 2 + c]
            used = entry >= 0
            safe = jnp.maximum(entry, 0)
            b, loc = safe // 64, lax.rem(safe, 16)
            keys_values = kv[yy * 16 + loc]
            scores = gain * lax.dot_general(
                keys_values[:, 0:256], qa[r * 6 + b], CONTRACT_LAST, preferred_element_type=F32
            )
            here = (line == b) & used
            gate = jnp.sum(jnp.where(line == b, tile, 0.0), axis=0, keepdims=True)
            grads = gate[:, 0:64] * lax.dot_general(
                keys_values[:, 256:512], ca[r * 6 + b], CONTRACT_LAST, preferred_element_type=F32
            )
            exps = jnp.exp(scores)
            both = jnp.concatenate([exps, grads], axis=1)
            eg[r * NY + yy] = both
            row = jnp.concatenate(
                [jnp.sum(exps, axis=0, keepdims=True), jnp.sum(exps * grads, axis=0, keepdims=True)], axis=1
            )
            stats = stats + jnp.where(here, row, 0.0)
        sent[r] = stats

    def outward(i, carry):
        near = (i + 1) // 2
        step = NZ + near - 2 * near * lax.rem(i, 2) - 1
        r = wrap(me + step + 1, 2 * NZ)
        reader(r)
        copies.make(
            sent.at[r], parts.at[step], ss.at[step], sr.at[step], {"st_0": r // 2, "st_2": lax.rem(r, 2)}
        ).start()
        return carry

    lax.fori_loop(0, 2 * NZ - 1, outward, 0)
    reader(me)
    whole = sent[me]
    for step in range(2 * NZ - 1):
        copies.arrived(parts.at[step], ss.at[step], sr.at[step], peers[step])
        whole = whole + parts[step]
    total[...] = whole
    tot[me] = whole
    own[...] = whole
    for step, peer in enumerate(peers):
        copies.start(total, tot.at[me], bs.at[step], br.at[step], peer)
    for step in range(2 * NZ - 1):
        other = wrap(me - (step + 1), 2 * NZ)
        copies.arrived(tot.at[other], bs.at[step], br.at[step], peers[step])
        copies.make(sent.at[0], parts.at[step], ss.at[step], sr.at[step], peers[step]).wait_send()
    copies.finish()


def grads_kernel(tb, kv, qa, ca, tl, eg, tot, kvg, qp, todo):
    z, c = lax.axis_index("st_0"), lax.axis_index("st_2")
    gain = SCORE_GAIN * 256 ** (-0.5)

    def entry_of(i):
        return tb[i // NY, 0, (z * NY + lax.rem(i, NY)) * 2 + c]

    def pick(i, count):
        todo[count] = i
        return count + (entry_of(i) >= 0).astype(jnp.int32)

    count = lax.fori_loop(0, 64, pick, 0, unroll=8)
    todo[count] = 0

    @pl.loop(0, 32)
    def _(i):
        blank = jnp.zeros((2, 64, 256), BF16)
        kvg[0, pl.ds(i * 2, 2)] = blank
        kvg[1, pl.ds(i * 2, 2)] = blank
        qp[pl.ds(i * 3, 3)] = jnp.zeros((3, 64, 256), BF16)

    @pl.loop(0, (count + 1) // 2)
    def _(pair):
        terms = []
        for u in range(2):
            i = todo[pair * 2 + u]
            live = (pair * 2 + u < count).astype(F32)
            entry = jnp.maximum(entry_of(i), 0)
            r, b = i // NY, entry // 64
            at, slot = r * 6 + b, lax.rem(i, NY) * 16 + lax.rem(entry, 16)
            row = tot[r, pl.ds(b, 1), :]
            gate = tl[r, pl.ds(b, 1), 0:64]
            norm = 1.0 / row[:, 0:64]
            both = eg[i]
            probs = both[:, 0:64] * (norm * live)
            slope = (probs * (both[:, 64:128] - row[:, 64:128] * norm)).astype(BF16)
            gated = (probs * gate).astype(BF16)
            key = gain * jnp.dot(slope, qa[at], preferred_element_type=F32)
            value = jnp.dot(gated, ca[at], preferred_element_type=F32)
            query = gain * lax.dot_general(
                slope, kv[slot, :, 0:256], CONTRACT_FIRST, preferred_element_type=F32
            )
            terms.append((at, slot, key, value, query))
        for at, slot, key, value, query in terms:
            kvg[0, slot] = (kvg[0, slot].astype(F32) + key).astype(BF16)
            kvg[1, slot] = (kvg[1, slot].astype(F32) + value).astype(BF16)
            qp[at] = (qp[at].astype(F32) + query).astype(BF16)


def finish_kernel(
    kvg, qp, klow, pas, qlow, wall, gall, own, md, gown,
    tgrad, pgrad, wgrad,
    ybuf, ysum, px, qs, zbuf, xall, pacc, tacc, xq, ggx, whalf, wget, wz, wbuf, wsum, wlast,
    ys, yr, zs, zr, ps, pr, xs, xr, qxs, qxr, gs, gr, us, ur, vs, vr, ls, lr,
):
    z, y, c, x = place()
    up, down = {"st_0": wrap(z + 1, NZ)}, {"st_0": wrap(z - 1, NZ)}
    east, west = {"st_1": wrap(y + 1, NY)}, {"st_1": wrap(y - 1, NY)}
    front, back, across = {"tp": wrap(x + 1, NX)}, {"tp": wrap(x - 1, NX)}, {"tp": wrap(x + 2, NX)}
    partner = {"st_2": 1 - c}
    spot = y * 2 + c
    plane = []
    for step in range(1, 8):
        other = wrap(spot + step, 8)
        plane.append({"st_1": other // 2, "st_2": lax.rem(other, 2)})
    greet([up, down, front, back, across] + plane)
    copies = Copies()
    zdirs, ydirs, xdirs = (up, down), (east, west), (front, back)

    far, beside = wrap(y + 2, NY), (wrap(y + 1, NY), wrap(y - 1, NY))

    def y_rows(j, part):
        return j // 4, pl.ds((j % 4) * 256 + part * 128, 128)

    def y_far(j):
        for way in (0, 1):
            p, at = y_rows(j, way)
            copies.start(kvg.at[p, far, at, :], ybuf.at[way, j], ys.at[0, way, j], yr.at[0, way, j], ydirs[way])

    def y_near(j):
        for way in (0, 1):
            p, at = y_rows(j, 1 - way)
            copies.start(
                kvg.at[p, beside[way], at, :], ysum.at[way, p, at, :], ys.at[1, way, j], yr.at[1, way, j], ydirs[way]
            )

    def y_add(j):
        for way in (0, 1):
            p, at = y_rows(j, way)
            copies.arrived(ybuf.at[way, j], ys.at[0, way, j], yr.at[0, way, j], ydirs[way])
            ybuf[way, j] = (kvg[p, beside[way], at, :].astype(F32) + ybuf[way, j].astype(F32)).astype(BF16)
            copies.start(ybuf.at[way, j], ysum.at[way, p, at, :], ys.at[2, way, j], yr.at[2, way, j], ydirs[way])
        if j + 1 < 8:
            y_near(j + 1)
        if j + 2 < 8:
            y_far(j + 2)

    def x_pieces(j, h):
        return j // 4, pl.ds((j % 4) * 256 + h * 128, 128)

    def y_done(j):
        for way in (0, 1):
            p, at = y_rows(j, 1 - way)
            copies.arrived(ysum.at[way, p, at, :], ys.at[1, way, j], yr.at[1, way, j], ydirs[way])
            p, at = y_rows(j, way)
            copies.arrived(ysum.at[way, p, at, :], ys.at[2, way, j], yr.at[2, way, j], ydirs[way])
        for h in (0, 1):
            p, at = x_pieces(j, h)
            grad = kvg[p, y, at, :].astype(F32) + ysum[0, p, at, :].astype(F32) + ysum[1, p, at, :].astype(F32)
            if p == 0:
                wide = klow[at, :].astype(F32)
                scale = lax.rsqrt(jnp.mean(wide * wide, axis=-1, keepdims=True) + NORM_FLOOR)
                inner = jnp.mean(wide * grad, axis=-1, keepdims=True)
                grad = scale * grad - (scale * scale * scale * inner) * wide
            xall[x, p, at, :] = grad.astype(BF16)
            for way in (0, 1):
                piece = xall.at[x, p, at, :]
                copies.start(piece, piece, xs.at[j, way, h], xr.at[j, way, h], xdirs[way])

    def x_take(j):
        for way in (0, 1):
            owner = wrap(x - 1 + 2 * way, NX)
            for h in (0, 1):
                p, at = x_pieces(j, h)
                piece = xall.at[owner, p, at, :]
                copies.arrived(piece, xs.at[j, way, h], xr.at[j, way, h], xdirs[way])
                if h == way:
                    copies.start(piece, piece, xs.at[j, way, 2], xr.at[j, way, 2], xdirs[way])

    def head_dot(rows, weight):
        return lax.dot_general(rows, weight, CONTRACT_LAST, preferred_element_type=F32)

    def x_near(j):
        p = j // 4

        @pl.loop(0, 2)
        def _(i):
            at = pl.ds(pl.multiple_of((j % 4) * 256 + i * 128, 128), 128)
            term = head_dot(xall[x, p, at, :], wall[p, x])
            for owner in (wrap(x - 1, NX), wrap(x + 1, NX)):
                term += head_dot(xall[owner, p, at, :], wall[p, owner])
            pacc[at, :] = term if p == 0 else pacc[at, :] + term

    def x_last(j):
        owner = wrap(x + 2, NX)
        for way in (0, 1):
            p, at = x_pieces(j, way)
            copies.arrived(xall.at[owner, p, at, :], xs.at[j, way, 2], xr.at[j, way, 2], xdirs[way])
        p = j // 4

        @pl.loop(0, 2)
        def _(i):
            at = pl.ds(pl.multiple_of((j % 4) * 256 + i * 128, 128), 128)
            term = pacc[at, :] + head_dot(xall[owner, p, at, :], wall[p, owner])
            if p == 0:
                pacc[at, :] = term
            else:
                pgrad[at, :] = term.astype(BF16)

    def ring_step(d, value, slots, send, recv, half):
        for way in (0, 1):
            there = wrap(z + d, NZ) if way == 0 else wrap(z - d, NZ)
            at = pl.ds(way * half, half)
            if d == 3:
                copies.arrived(slots.at[way, 0, at, :], send.at[way, 3], recv.at[way, 3], zdirs[way])
                value[there, at, :] = (value[there, at, :].astype(F32) + slots[way, 0, at, :].astype(F32)).astype(BF16)
            elif d < 3:
                copies.arrived(slots.at[way, 3 - d], send.at[way, d], recv.at[way, d], zdirs[way])
                value[there] = (value[there].astype(F32) + slots[way, 3 - d].astype(F32)).astype(BF16)
            if d == 4:
                copies.start(value.at[there, at, :], slots.at[way, 0, at, :], send.at[way, 3], recv.at[way, 3], zdirs[way])
            else:
                copies.start(value.at[there], slots.at[way, 4 - d], send.at[way, d - 1], recv.at[way, d - 1], zdirs[way])

    def ring_last(value, slots, send, recv):
        result = value[z].astype(F32)
        for way in (0, 1):
            copies.arrived(slots.at[way, 3], send.at[way, 0], recv.at[way, 0], zdirs[way])
            result = result + slots[way, 3].astype(F32)
        return result

    def q_pair(k):
        there = wrap(z + k, NZ)
        copies.arrived(px.at[there], ps.at[k], pr.at[k], partner)
        qs[there] = (qp[there * 2 + c].astype(F32) + px[there].astype(F32)).astype(BF16)

    def q_step(d):
        ring_step(d, qs, zbuf, zs, zr, 192)

    def q_done():
        grad = ring_last(qs, zbuf, zs, zr)
        wide = qlow[...].astype(F32)
        scale = lax.rsqrt(jnp.mean(wide * wide, axis=-1, keepdims=True) + NORM_FLOOR)
        inner = jnp.mean(wide * grad, axis=-1, keepdims=True)
        xq[x] = (scale * grad - (scale * scale * scale * inner) * wide).astype(BF16)
        for way in (0, 1):
            for h in (0, 1):
                piece = xq.at[x, pl.ds(h * 192, 192), :]
                copies.start(piece, piece, qxs.at[way, h], qxr.at[way, h], xdirs[way])

    def gates():
        gate = gown[0:6, 0:64]
        dots = own[0:6, 64:128] / own[0:6, 0:64]
        ggx[x] = jnp.zeros((8, 128), F32)
        ggx[x, 0:6, 0:64] = (1.0 - gate) * (dots - gate * md[0:6, :])
        for step, peer in enumerate((front, across, back)):
            copies.start(ggx.at[x], ggx.at[x], gs.at[step], gr.at[step], peer)

    def q_take():
        for way in (0, 1):
            owner = wrap(x - 1 + 2 * way, NX)
            for h in (0, 1):
                piece = xq.at[owner, pl.ds(h * 192, 192), :]
                copies.arrived(piece, qxs.at[way, h], qxr.at[way, h], xdirs[way])
                if h == way:
                    copies.start(piece, piece, qxs.at[way, 2], qxr.at[way, 2], xdirs[way])

    def q_last():
        owner = wrap(x + 2, NX)
        for way in (0, 1):
            copies.arrived(xq.at[owner, pl.ds(way * 192, 192), :], qxs.at[way, 2], qxr.at[way, 2], xdirs[way])
        for b in range(6):
            at = pl.ds(b * 64, 64)
            tgrad[at, :] = (tacc[at, :] + head_dot(xq[owner, at, :], wall[2, owner])).astype(BF16)

    def q_near():
        for step, peer in enumerate((front, across, back)):
            copies.arrived(ggx.at[wrap(x - 1 - step, NX)], gs.at[step], gr.at[step], peer)
        blank = [jnp.zeros((4, 64), F32)]
        slope = jnp.concatenate(
            [gall[h, 0:1, :].astype(F32) for h in range(NX)] + [jnp.zeros((4, 512), F32)], axis=0
        )
        for b in range(6):
            at = pl.ds(b * 64, 64)
            rows = jnp.concatenate([ggx[h, b : b + 1, 0:64] for h in range(NX)] + blank, axis=0)
            term = lax.dot_general(
                rows, slope, CONTRACT_FIRST, preferred_element_type=F32, precision=lax.Precision.HIGHEST
            )
            for owner in (x, wrap(x - 1, NX), wrap(x + 1, NX)):
                term += head_dot(xq[owner, at, :], wall[2, owner])
            tacc[at, :] = term

    keep = pl.ds(pl.multiple_of(c * 128, 128), 128)
    give = pl.ds(pl.multiple_of((1 - c) * 128, 128), 128)

    def w_tile(k):
        there = wrap(z + k, NZ)
        at = pl.ds(pl.multiple_of(there * 256, 256), 256)
        wsum[there] = lax.dot_general(
            pas[:, at], xall[x, 0], CONTRACT_FIRST, preferred_element_type=F32
        )
        whalf[there] = wsum[there, :, give]
        copies.start(whalf.at[there], wget.at[there], us.at[k], ur.at[k], partner)

    def w_pair(k):
        there = wrap(z + k, NZ)
        copies.arrived(wget.at[there], us.at[k], ur.at[k], partner)
        wz[there] = (wsum[there, :, keep] + wget[there]).astype(BF16)

    def w_step(d):
        ring_step(d, wz, wbuf, vs, vr, 128)

    def w_done():
        wsum[z, :, 0:128] = ring_last(wz, wbuf, vs, vr)
        for step, peer in enumerate(plane):
            other = wrap(spot + step + 1, 8)
            piece = wsum.at[z, pl.ds(pl.multiple_of(other * 32, 32), 32), pl.ds(0, 128)]
            copies.start(piece, wlast.at[spot], ls.at[step], lr.at[step], peer)
        wlast[spot] = wsum[z, pl.ds(pl.multiple_of(spot * 32, 32), 32), 0:128]

    def w_last():
        for step, peer in enumerate(plane):
            copies.arrived(wlast.at[wrap(spot - step - 1, 8)], ls.at[step], lr.at[step], peer)
        for k in (0, 1):
            wgrad[:, k * 128 : k * 128 + 128] = wlast[k] + wlast[2 + k] + wlast[4 + k] + wlast[6 + k]

    y_far(0)
    y_near(0)
    y_far(1)
    for k in (4, 3, 5, 2, 6, 1, 7, 0):
        there = wrap(z + k, NZ)
        copies.start(qp.at[there * 2 + 1 - c], px.at[there], ps.at[k], pr.at[k], partner)
    q_pair(4)
    q_step(4)
    q_pair(3)
    q_pair(5)
    y_add(0)
    for k in (2, 6, 1, 7, 0):
        q_pair(k)
    gates()
    y_add(1)
    q_step(3)
    y_done(0)
    y_add(2)
    y_done(1)
    q_step(2)
    x_take(0)
    y_add(3)
    y_done(2)
    x_take(1)
    y_add(4)
    y_done(3)
    q_step(1)
    x_near(0)
    x_last(0)
    for k in (4, 3, 5):
        w_tile(k)
    x_take(2)
    y_add(5)
    y_done(4)
    x_near(1)
    x_last(1)
    x_take(3)
    for k in (2, 6, 1, 7, 0):
        w_tile(k)
    y_add(6)
    q_done()
    y_done(5)
    w_pair(4)
    w_step(4)
    y_add(7)
    y_done(6)
    x_take(4)
    w_pair(3)
    w_pair(5)
    w_step(3)
    y_done(7)
    x_near(2)
    x_last(2)
    q_take()
    x_take(5)
    for k in (2, 6, 1, 7, 0):
        w_pair(k)
    w_step(2)
    x_near(3)
    x_last(3)
    x_near(4)
    x_take(6)
    w_step(1)
    q_near()
    x_last(4)
    x_near(5)
    x_take(7)
    w_done()
    x_near(6)
    x_near(7)
    q_last()
    x_last(5)
    w_last()
    x_last(6)
    x_last(7)
    copies.finish()


def store_kernel(tgrad, pgrad, wgrad, tokens, rows, weights, sems):
    pairs = ((pgrad, rows), (tgrad, tokens), (wgrad, weights))
    copies = [pltpu.make_async_copy(src, dst, sems.at[i]) for i, (src, dst) in enumerate(pairs)]
    for copy in copies:
        copy.start()
    for copy in copies:
        copy.wait()


def shaped(shape, dtype):
    return jax.ShapeDtypeStruct(shape, dtype)


def dma(*shape):
    return pltpu.SemaphoreType.DMA(shape)


def call(kernel, outs, scratch, collective, smem=0, limit=48, count=0, space=VMEM, out_space=VMEM, **extra):
    in_specs = [pl.BlockSpec(memory_space=pltpu.SMEM)] * smem + [pl.BlockSpec(memory_space=space)] * (count - smem)
    params = dict(vmem_limit_bytes=limit * 2**20)
    if collective is not None:
        params.update(collective_id=collective, has_side_effects=True)
    return pl.pallas_call(
        kernel,
        out_shape=outs,
        in_specs=in_specs,
        out_specs=[pl.BlockSpec(memory_space=out_space)] * len(outs),
        scratch_shapes=scratch,
        compiler_params=pltpu.CompilerParams(**params),
        **extra,
    )


def body(
    tokens, cotangent, mix_query, mix_key, mix_value, beta_pre, decay_pre, decay_rate,
    passages, passage_ids, query_weight, key_weight, value_weight, gate_weight,
):
    pass_local, span_rows, model_width = passages.shape
    flat_rows = passages.reshape(pass_local * span_rows, model_width)
    kv, qa, ca, tl, lookup, key_low, query_low, gown, wall, gall, md, eg, tot, own = call(
        gather_kernel,
        [
            shaped((64, 64, 512), BF16), shaped((96, 64, 256), BF16), shaped((96, 64, 256), BF16),
            shaped((16, 8, 128), F32), shaped((16, 1, 128), jnp.int32), shaped((1024, 256), BF16), shaped((384, 256), BF16), shaped((8, 128), F32),
            shaped((3, NX, 512, 256), BF16), shaped((NX, 16, 512), BF16), shaped((8, 64), F32),
            shaped((64, 64, 128), F32), shaped((16, 8, 128), F32), shaped((8, 128), F32),
        ],
        [
            pltpu.SMEM((16, 1, 128), jnp.int32), VMEM((16, 8, 128), F32), VMEM((15, 8, 128), F32), VMEM((8, 128), F32),
            dma(15), dma(15), dma(15), dma(15),
            VMEM((1024, 2048), BF16), VMEM((2048, 256), BF16), VMEM((2048, 256), BF16), VMEM((2048, 256), BF16),
            VMEM((384, 256), BF16), VMEM((384, 256), BF16), VMEM((384, 256), BF16), VMEM((1, 2048), BF16),
            VMEM((4, 6), jnp.int32), VMEM((2, 384), F32), VMEM((2, 384), F32), VMEM((1, 2), F32),
            VMEM((16, 2048), BF16), VMEM((24, 128), F32),
            VMEM((NX, 384, 512), BF16), VMEM((3, 256, 256), BF16), VMEM((6, 128, 128), F32),
            VMEM((6, 128, 128), BF16), VMEM((6, 128, 128), BF16), VMEM((6, 128, 128), BF16), VMEM((6, 128, 128), BF16),
            dma(18), dma(15), dma(15), dma(2, 3), dma(2, 3), dma(2, 6), dma(2, 6), dma(2, 2, 7), dma(2, 2, 7),
            dma(2, 16), dma(2, 16), dma(15), dma(15), dma(12), dma(12), dma(9), dma(9), dma(3), dma(3),
        ],
        1, count=14, limit=LIMITS[0], space=pltpu.HBM,
    )(*[pltpu.with_memory_space_constraint(a, pltpu.HBM) for a in (
        flat_rows, key_weight, value_weight, tokens, query_weight, gate_weight, cotangent.reshape(6, 64, 256),
        mix_query, mix_key, mix_value, passage_ids.T, beta_pre, decay_pre, decay_rate[None, :],
    )])
    kvg, qp = call(
        grads_kernel,
        [shaped((2, 64, 64, 256), BF16), shaped((96, 64, 256), BF16)],
        [pltpu.SMEM((66,), jnp.int32)],
        None, smem=1, count=7, limit=LIMITS[1],
    )(lookup, kv, qa, ca, tl, eg, tot)
    token_grad, passage_grad, key_weight_grad = call(
        finish_kernel,
        [shaped((384, 512), BF16), shaped((1024, 512), BF16), shaped((32, 256), F32)],
        [
            VMEM((2, 8, 128, 256), BF16), VMEM((2, 2, 1024, 256), BF16), VMEM((NZ, 384, 256), BF16),
            VMEM((NZ, 384, 256), BF16), VMEM((2, 4, 384, 256), BF16), VMEM((NX, 2, 1024, 256), BF16),
            VMEM((1024, 512), F32), VMEM((384, 512), F32), VMEM((NX, 384, 256), BF16), VMEM((NX, 8, 128), F32),
            VMEM((NZ, 256, 128), F32), VMEM((NZ, 256, 128), F32), VMEM((NZ, 256, 128), BF16),
            VMEM((2, 4, 256, 128), BF16), VMEM((NZ, 256, 256), F32), VMEM((8, 32, 128), F32),
            dma(3, 2, 8), dma(3, 2, 8), dma(2, 4), dma(2, 4), dma(8), dma(8), dma(8, 2, 3), dma(8, 2, 3),
            dma(2, 3), dma(2, 3), dma(3), dma(3), dma(8), dma(8), dma(2, 4), dma(2, 4), dma(7), dma(7),
        ],
        3, count=10, limit=LIMITS[2],
    )(
        kvg.reshape(2, NY, 1024, 256), qp.reshape(16, 384, 256), key_low, flat_rows, query_low,
        wall, gall, own, md, gown,
    )
    token_grad, passage_grad, key_weight_grad = call(
        store_kernel,
        [shaped((384, 512), BF16), shaped((1024, 512), BF16), shaped((32, 256), F32)],
        [dma(3)],
        None, count=3, limit=4, out_space=pltpu.HBM,
    )(token_grad, passage_grad, key_weight_grad)
    return (token_grad, passage_grad.reshape(pass_local, span_rows, 512), key_weight_grad)


def solution(mesh):
    torus = Mesh(mesh.devices.reshape(8, 4, 2, mesh.shape["tp"]), ("st_0", "st_1", "st_2", "tp"))
    return jax.shard_map(
        body,
        mesh=torus,
        in_specs=(
            P(ST, "tp"),
            P(ST, "tp"),
            P(ST, "tp"),
            P(ST, "tp"),
            P(ST, "tp"),
            P("tp", ST),
            P("tp", ST),
            P("tp"),
            P(ST, None, None),
            P(ST, None),
            P(None, "tp"),
            P(None, "tp"),
            P(None, "tp"),
            P("tp", None),
        ),
        out_specs=(P(ST, "tp"), P(ST, None, "tp"), P(ST, "tp")),
        check_vma=False,
    )
```
